32 devices in a mesh: sp: 16 (over z, y, core), tp: 2 (over x).
Axes of the slice: x: 2, y: 2, z: 4, core: 2. Of those that a mesh axis runs over, the one named last changes fastest.
Arguments:
- tokens: bfloat16 [4096, 2048], P('sp'), may hold values from -28 to 28
- query_weight: bfloat16 [2048, 1536], P(None, 'tp'), may hold values from -0.125 to 0.125
- key_weight: bfloat16 [2048, 1536], P(None, 'tp'), may hold values from -0.125 to 0.125
- value_weight: bfloat16 [2048, 1536], P(None, 'tp'), may hold values from -0.125 to 0.125
- out_weight: bfloat16 [512, 2048], P(None, 'tp'), may hold values from -1 to 1
Outputs:
- mixed: bfloat16 [4096, 2048], P('sp', 'tp')
- total_log: float32 [4, 4096], P('tp', 'sp')
The draws below stay inside these ranges and needn't reach their ends.
All inputs are finite; a program needn't handle non-finite values.
Results may differ from the reference program's by a relative error of at most 0.012.
The reference program's roundings to bfloat16 on the way (of `queries`, `probs` and `merged`) count: a program that leaves them out, or rounds other values in their place, can miss the bound.
Values may be sent and summed in bfloat16 or wider, within the bound.
A program may use at most 64 MiB of HBM per device.

```python
import jax
import jax.numpy as jnp
from jax import lax

D = 2048
HEADS = 4
HEAD_DIM = 128
NEAR_WINDOW = 128
MIDDLE_WINDOW = 512
MIDDLE_DILATION = 4
FAR_WINDOW = 2048
FAR_DILATION = 16
TOK_DEV = 256
TOKENS = 4096
N_SP = 16


def draw_tokens(key, part):
    first_key, second_key, third_key = jax.random.split(key, 3)
    return jnp.clip(jax.random.normal(first_key, (TOKENS, D), jnp.float32), -6.0, 6.0).astype(jnp.bfloat16)


def block_scale(key, extent, cuts, low, largest):
    loudness = 1.0
    for axis_at, shards_of in cuts:
        steps = jax.random.uniform(jax.random.fold_in(jax.random.fold_in(key, 6), axis_at), (shards_of,), jnp.float32, low / len(cuts), largest / len(cuts))
        loudness = loudness * jnp.repeat(jnp.exp(steps), extent[axis_at] // shards_of).reshape((-1,) + (1,) * (len(extent) - 1 - axis_at))
    return loudness


def gaussian(own_key, dims, deviation, limit, cuts=(), kind=jnp.bfloat16):
    level = block_scale(own_key, dims, cuts, -0.22, 0.18) if cuts else 1.0
    array = jax.random.normal(own_key, dims, jnp.float32) * deviation * level
    return jnp.minimum(jnp.maximum(array, -limit), limit).astype(kind)


def setup_inputs(seed: int = 0) -> dict:
    splits = jax.random.split(jax.random.key(seed), 6)
    tokens = draw_tokens(jax.random.fold_in(splits[5], 71), 0)
    query_weight = gaussian(splits[1], (D, HEADS * 3 * HEAD_DIM), D ** -0.5, 0.125, ((1, 2),))
    key_weight = gaussian(splits[2], (D, HEADS * 3 * HEAD_DIM), D ** -0.5, 0.125, ((1, 2),))
    value_weight = gaussian(splits[3], (D, HEADS * 3 * HEAD_DIM), D ** -0.5, 0.125, ((1, 2),))
    out_weight = gaussian(splits[4], (HEADS * HEAD_DIM, D), (HEADS * HEAD_DIM // 16) ** -0.5, 1.0, ((1, 2),))
    return dict(tokens=tokens, query_weight=query_weight, key_weight=key_weight, value_weight=value_weight, out_weight=out_weight)


def window_table():
    return ((NEAR_WINDOW, 1), (MIDDLE_WINDOW, MIDDLE_DILATION), (FAR_WINDOW, FAR_DILATION))


def attend_group(group_queries, buffer, window, dilation, first_key, slopes_here):
    row_count = group_queries.shape[0]
    head_count = group_queries.shape[1]
    head_size = group_queries.shape[2]
    query_split = group_queries.reshape(row_count // dilation, dilation, head_count, head_size)
    key_split = buffer[0].reshape(-1, dilation, head_count, head_size)
    value_split = buffer[1].reshape(-1, dilation, head_count, head_size)
    scores = jnp.einsum("mrhe,nrhe->rhmn", query_split.astype(jnp.float32), key_split.astype(jnp.float32)) * head_size ** -0.5
    grid_shape = (row_count // dilation, key_split.shape[0])
    query_slot = lax.broadcasted_iota(jnp.int32, grid_shape, 0)
    key_slot = lax.broadcasted_iota(jnp.int32, grid_shape, 1)
    spacing = query_slot + window // dilation - key_slot
    residue = lax.broadcasted_iota(jnp.int32, (dilation, 1, 1), 0)
    key_place = first_key + residue + dilation * key_slot[None]
    valid = (spacing[None] >= 0) & (spacing[None] <= window // dilation) & (key_place >= 0)
    scores = scores - slopes_here[None, :, None, None] * (dilation * spacing).astype(scores.dtype)[None, None]
    masked = jnp.where(valid[:, None], scores, -jnp.inf)
    highest = jnp.max(masked, axis=-1, keepdims=True)
    log_sum = highest + jnp.log(jnp.sum(jnp.exp(masked - highest), axis=-1, keepdims=True))
    probs = jnp.exp(masked - log_sum).astype(jnp.bfloat16)
    attended = jnp.einsum("rhmn,nrhe->mrhe", probs.astype(jnp.float32), value_split.astype(jnp.float32))
    attended = attended.reshape(row_count, head_count, head_size)
    log_rows = jnp.transpose(log_sum[..., 0], (1, 2, 0)).reshape(head_count, row_count)
    return attended, log_rows


def reference(tokens, query_weight, key_weight, value_weight, out_weight):
    def project(weight_matrix):
        product = jnp.dot(tokens, weight_matrix, preferred_element_type=jnp.float32)
        return product.astype(jnp.bfloat16).reshape(TOKENS, HEADS, 3, HEAD_DIM)

    queries = project(query_weight)
    keys_all = project(key_weight)
    values_all = project(value_weight)
    stacked = jnp.stack((keys_all, values_all))
    padding = jnp.zeros((2, FAR_WINDOW, HEADS, 3, HEAD_DIM), stacked.dtype)
    padded = jnp.concatenate((padding, stacked), axis=1)
    head_ids = jnp.arange(HEADS).astype(jnp.float32)

    def block_step(block_index):
        first_row = block_index * TOK_DEV
        query_block = lax.dynamic_slice_in_dim(queries, first_row, TOK_DEV, 0)
        outputs = []
        logs = []
        for group_index, (window, dilation) in enumerate(window_table()):
            begin = (first_row + FAR_WINDOW - window).astype(jnp.int32)
            buffer = lax.dynamic_slice_in_dim(padded, begin, window + TOK_DEV, 1)[:, :, :, group_index]
            slopes_here = 2.0 ** (3.0 - 8.0 * (head_ids + 1.0) / HEADS) / window
            attended, log_rows = attend_group(query_block[:, :, group_index], buffer, window, dilation, first_row - window, slopes_here)
            outputs.append(attended)
            logs.append(log_rows)
        stacked_logs = jnp.stack(logs)
        highest = jnp.max(stacked_logs, axis=0)
        total_block = highest + jnp.log(jnp.sum(jnp.exp(stacked_logs - highest), axis=0))
        mixing = jnp.exp(stacked_logs - total_block)
        merged_block = outputs[0] * jnp.transpose(mixing[0])[:, :, None]
        merged_block = merged_block + outputs[1] * jnp.transpose(mixing[1])[:, :, None]
        merged_block = merged_block + outputs[2] * jnp.transpose(mixing[2])[:, :, None]
        return merged_block.astype(jnp.bfloat16), total_block

    merged_blocks, totals = lax.map(block_step, jnp.arange(N_SP, dtype=jnp.int32))
    merged = merged_blocks.reshape(TOKENS, HEADS * HEAD_DIM)
    mixed = jnp.dot(merged, out_weight, preferred_element_type=jnp.float32).astype(jnp.bfloat16)
    total_log = jnp.transpose(totals, (1, 0, 2)).reshape(HEADS, TOKENS)
    return mixed, total_log
```

```python
import functools
import jax
import jax.numpy as jnp
from jax import lax
from jax.experimental import pallas as pl
from jax.experimental.pallas import tpu as pltpu
from jax.sharding import PartitionSpec as P

HEADS = 4
HEAD_DIM = 128
NEAR_WINDOW = 128
MIDDLE_WINDOW = 512
MIDDLE_DILATION = 4
FAR_WINDOW = 2048
FAR_DILATION = 16


def from_behind(block, axis, distance):
    devices = range(lax.axis_size(axis))
    route = [(i - distance, i) for i in devices if i - distance in devices]
    return lax.ppermute(block, axis, route)


def window_table():
    return ((NEAR_WINDOW, 1), (MIDDLE_WINDOW, MIDDLE_DILATION), (FAR_WINDOW, FAR_DILATION))


def tail_counts(row_count, distance, held_rows):
    counts = []
    for entry, available in zip(window_table(), held_rows):
        counts.append(max(0, min(available, entry[0] - (distance - 1) * row_count)))
    return counts


def pack_tails(sources, counts):
    selected = [
        source[:, source.shape[1] - amount :]
        for source, amount in zip(sources, counts)
        if amount > 0
    ]
    return jnp.concatenate(selected, axis=1)


def unpack_rows(packed, counts):
    result = []
    cursor = 0
    for amount in counts:
        result.append(packed[:, cursor : cursor + amount])
        cursor = cursor + amount
    return result


def attend_group(group_queries, buffer, window, dilation, first_key, slopes_here):
    row_count = group_queries.shape[0]
    head_count = group_queries.shape[1]
    head_size = group_queries.shape[2]
    query_split = group_queries.reshape(row_count // dilation, dilation, head_count, head_size)
    key_split = buffer[0].reshape(-1, dilation, head_count, head_size)
    value_split = buffer[1].reshape(-1, dilation, head_count, head_size)
    scores = jnp.einsum(
        "mrhe,nrhe->rhmn", query_split, key_split, preferred_element_type=jnp.float32
    ) * head_size ** (-0.5)
    grid_shape = (row_count // dilation, key_split.shape[0])
    query_slot = lax.broadcasted_iota(jnp.int32, grid_shape, 0)
    key_slot = lax.broadcasted_iota(jnp.int32, grid_shape, 1)
    spacing = query_slot + window // dilation - key_slot
    residue = lax.broadcasted_iota(jnp.int32, (dilation, 1, 1), 0)
    key_place = first_key + residue + dilation * key_slot[None]
    valid = (spacing[None] >= 0) & (spacing[None] <= window // dilation) & (key_place >= 0)
    scores = (
        scores
        - slopes_here[None, :, None, None] * (dilation * spacing).astype(jnp.float32)[None, None]
    )
    masked = jnp.where(valid[:, None], scores, -jnp.inf)
    highest = jnp.max(masked, axis=-1, keepdims=True)
    log_sum = highest + jnp.log(jnp.sum(jnp.exp(masked - highest), axis=-1, keepdims=True))
    probs = jnp.exp(masked - log_sum).astype(jnp.bfloat16)
    attended = jnp.einsum("rhmn,nrhe->mrhe", probs, value_split, preferred_element_type=jnp.float32)
    attended = attended.reshape(row_count, head_count, head_size)
    log_rows = jnp.transpose(log_sum[..., 0], (1, 2, 0)).reshape(head_count, row_count)
    return (attended, log_rows)


def local(tokens, query_weight, key_weight, value_weight, out_weight):
    rows_here = tokens.shape[0]
    local_heads = query_weight.shape[1] // (3 * HEAD_DIM)

    def project(weight_matrix):
        product = jnp.dot(tokens, weight_matrix, preferred_element_type=jnp.float32)
        return product.astype(jnp.bfloat16).reshape(rows_here, local_heads, 3, HEAD_DIM)

    queries = project(query_weight)
    keys_all = project(key_weight)
    values_all = project(value_weight)
    table = window_table()
    own = [jnp.stack((keys_all[:, :, index], values_all[:, :, index])) for index in range(3)]
    held = list(own)
    span_now = 1
    while span_now * rows_here < FAR_WINDOW + rows_here:
        counts = tail_counts(rows_here, span_now, [item.shape[1] for item in held])
        packed = pack_tails(held, counts)
        arrived = from_behind(packed, "sp", span_now)
        pieces_in = unpack_rows(arrived, counts)
        for index in range(3):
            if counts[index] > 0:
                joined = jnp.concatenate((pieces_in[index], held[index]), axis=1)
                held[index] = joined
        span_now = span_now * 2
    priors = [held[index][:, : table[index][0]] for index in range(3)]
    position_start = lax.axis_index("sp") * rows_here
    head_ids = (
        lax.axis_index("tp") * local_heads + jnp.arange(local_heads, dtype=jnp.int32)
    ).astype(jnp.float32)
    outputs = []
    logs = []
    for index, (window, dilation) in enumerate(table):
        buffer = jnp.concatenate((priors[index], own[index]), axis=1)
        slopes_here = 2.0 ** (3.0 - 8.0 * (head_ids + 1.0) / HEADS) / window
        attended, log_rows = attend_group(
            queries[:, :, index], buffer, window, dilation, position_start - window, slopes_here
        )
        outputs.append(attended)
        logs.append(log_rows)
    stacked_logs = jnp.stack(logs)
    highest = jnp.max(stacked_logs, axis=0)
    total_log = highest + jnp.log(jnp.sum(jnp.exp(stacked_logs - highest), axis=0))
    mixing = jnp.exp(stacked_logs - total_log)
    merged = outputs[0] * jnp.transpose(mixing[0])[:, :, None]
    merged = merged + outputs[1] * jnp.transpose(mixing[1])[:, :, None]
    merged = merged + outputs[2] * jnp.transpose(mixing[2])[:, :, None]
    merged = merged.astype(jnp.bfloat16).reshape(rows_here, local_heads * HEAD_DIM)
    mixed = jnp.dot(
        lax.all_gather(merged, "tp", axis=1, tiled=True),
        out_weight,
        preferred_element_type=jnp.float32,
    ).astype(jnp.bfloat16)
    return (mixed, total_log)


MESH = pl.DeviceIdType.MESH
MASKED = -1e30


def weigh(query, key, slope, distance, valid):
    scores = lax.dot_general(
        query, key, (((1,), (1,)), ((), ())), preferred_element_type=jnp.float32
    ) * HEAD_DIM ** (-0.5)
    scores = jnp.where(valid, scores - slope * distance, MASKED)
    highest = jnp.max(scores, axis=-1, keepdims=True)
    weights = jnp.exp(scores - highest)
    total = jnp.sum(weights, axis=-1, keepdims=True)
    probs = (weights * (1.0 / total)).astype(jnp.bfloat16)
    return probs, highest + jnp.log(total)


def attend(query, key, value, slope, distance, valid):
    probs, log_sum = weigh(query, key, slope, distance, valid)
    return jnp.dot(probs, value, preferred_element_type=jnp.float32), log_sum


def swap_matrix(rows, width):
    shift = width.bit_length() - 1
    row = lax.broadcasted_iota(jnp.int32, (rows, rows), 0)
    column = lax.broadcasted_iota(jnp.int32, (rows, rows), 1)
    source = ((row & (width - 1)) << shift) + (row >> shift)
    return jnp.where(column == source, 1.0, 0.0).astype(jnp.bfloat16)


def kernel(
    n, local_heads,
    tok_hbm, wq_hbm, wk_hbm, wv_hbm, wo_hbm,
    partial_ref, peer_ref, totals_ref,
    tok, weight, wo, far_send, far_held, back_send, back_held, log_send, log_held,
    mid_query, mid_own, mid_held, via_held, near_query, near_own, near_held, via_near,
    base, factor, merged_own, merged_held,
    load_sem, far_ssem, far_rsem, back_ssem, back_rsem, log_ssem, log_rsem,
    mid_ssem, mid_rsem, via_ssem, via_rsem, near_ssem, near_rsem, merged_ssem, merged_rsem,
):
    me = lax.axis_index("sp")
    tp = lax.axis_index("tp")
    rows = tok.shape[0]
    width = local_heads * HEAD_DIM
    chunk = rows // n
    shift = n.bit_length() - 1
    peer = 1 - tp
    sources = (wq_hbm, wk_hbm, wv_hbm)

    tok_load = pltpu.make_async_copy(tok_hbm, tok, load_sem.at[0])
    tok_load.start()
    wo_load = pltpu.make_async_copy(wo_hbm, wo, load_sem.at[1])
    loads = {}
    count = 2
    for group in (2, 1, 0):
        loads[group] = []
        if group == 2:
            order = [(part, head) for head in range(local_heads) for part in range(3)]
        else:
            order = [(part, head) for part in (1, 2, 0) for head in range(local_heads)]
        for place, (part, head) in enumerate(order):
            loads[group].append(pltpu.make_async_copy(
                sources[part].at[:, pl.ds((head * 3 + group) * HEAD_DIM, HEAD_DIM)],
                weight.at[group, :, pl.ds(place * HEAD_DIM, HEAD_DIM)],
                load_sem.at[count],
            ))
            count += 1
    for copy in loads[2]:
        copy.start()

    barrier = pltpu.get_barrier_semaphore()

    def greet(k, carry):
        pl.semaphore_signal(barrier, inc=1, device_id=(lax.rem(me + k, n), tp), device_id_type=MESH)
        return carry

    lax.fori_loop(1, n, greet, 0)
    pl.semaphore_signal(barrier, inc=1, device_id=(me, peer), device_id_type=MESH)

    @pl.when(me < 2)
    def _():
        mid_held[0] = jnp.zeros((2, rows, width), jnp.bfloat16)

    @pl.when(me < 1)
    def _():
        mid_held[1] = jnp.zeros((2, rows, width), jnp.bfloat16)
        near_held[...] = jnp.zeros((2, NEAR_WINDOW, width), jnp.bfloat16)

    def project(group, block):
        for copy in loads[group][block * local_heads : (block + 1) * local_heads]:
            copy.wait()
        return jnp.dot(
            tok[...], weight[group, :, block * width : (block + 1) * width],
            preferred_element_type=jnp.float32,
        ).astype(jnp.bfloat16)

    def at_rows(index):
        return pl.ds(pl.multiple_of(index * chunk, chunk), chunk)

    swap = swap_matrix(rows, n)

    def swapped(block):
        return jnp.dot(swap, block, preferred_element_type=jnp.float32).astype(jnp.bfloat16)

    def each(action):
        def step(k, carry):
            action(k)
            return carry

        lax.fori_loop(1, n, step, 0)

    def exchange(source, target, ssem, rsem, k, outgoing):
        to = lax.rem(me + k, n)
        come = lax.rem(me + n - k, n)
        place = at_rows(me if outgoing else come)
        return pltpu.make_async_remote_copy(
            src_ref=source.at[at_rows(to)],
            dst_ref=target.at[place],
            send_sem=ssem.at[k],
            recv_sem=rsem.at[k],
            device_id=(to, tp),
            device_id_type=MESH,
        )

    def far_copy(block, k, outgoing):
        return exchange(
            far_send.at[block], far_held.at[block], far_ssem.at[block], far_rsem.at[block], k, outgoing
        )

    def back_copy(head, k, outgoing):
        return exchange(
            back_send.at[head], back_held.at[head], back_ssem.at[head], back_rsem.at[head], k, outgoing
        )

    def log_copy(k, outgoing):
        to = lax.rem(me + k, n)
        come = lax.rem(me + n - k, n)
        return pltpu.make_async_remote_copy(
            src_ref=log_send.at[to],
            dst_ref=log_held.at[me if outgoing else come],
            send_sem=log_ssem.at[k],
            recv_sem=log_rsem.at[k],
            device_id=(to, tp),
            device_id_type=MESH,
        )

    tok_load.wait()
    for block in range(3):
        far_send[block] = swapped(project(2, block))
        if block == 0:
            for copy in loads[1]:
                copy.start()
            pl.semaphore_wait(barrier, n)
        each(lambda k: far_copy(block, k, True).start())
        far_held[block, at_rows(me), :] = far_send[block, at_rows(me), :]
    for copy in loads[0]:
        copy.start()
    wo_load.start()

    def mid_copy(slot, hop, source, part, sem):
        return pltpu.make_async_remote_copy(
            src_ref=source,
            dst_ref=mid_held.at[slot, part],
            send_sem=mid_ssem.at[sem, part],
            recv_sem=mid_rsem.at[slot, part],
            device_id=(lax.rem(me + hop + n, n), tp),
            device_id_type=MESH,
        )

    def near_copy(hop, source, part, sem):
        return pltpu.make_async_remote_copy(
            src_ref=source,
            dst_ref=near_held.at[part],
            send_sem=near_ssem.at[sem],
            recv_sem=near_rsem.at[part],
            device_id=(lax.rem(me + hop, n), tp),
            device_id_type=MESH,
        )

    def via_copy(which, source, target):
        return pltpu.make_async_remote_copy(
            src_ref=source,
            dst_ref=target,
            send_sem=via_ssem.at[which],
            recv_sem=via_rsem.at[which],
            device_id=(lax.rem(me + -2 + n, n), tp),
            device_id_type=MESH,
        )

    near_tail = pl.ds(rows - NEAR_WINDOW, NEAR_WINDOW)
    key_two = mid_copy(0, 2, mid_own.at[0], 0, 0)
    key_one = mid_copy(1, 1, mid_own.at[0], 0, 1)
    value_two = mid_copy(0, 2, mid_own.at[1], 1, 0)
    value_one = mid_copy(1, 1, mid_own.at[1], 1, 1)
    near_key = near_copy(1, near_own.at[0, near_tail], 0, 0)
    near_value = near_copy(1, near_own.at[1, near_tail], 1, 1)
    via_mid = via_copy(0, mid_own.at[1], via_held)
    via_last = via_copy(1, near_own.at[1, near_tail], via_near)
    onward_even = mid_copy(0, 4, via_held, 1, 3)
    onward_odd = mid_copy(1, 3, via_held, 1, 3)
    onward_near = near_copy(3, via_near, 1, 2)
    relay_key = mid_copy(0, 1, mid_held.at[1, 0], 0, 2)
    relay_value = mid_copy(0, 1, mid_held.at[1, 1], 1, 2)

    even = lax.rem(me, 2) == 0
    odd = jnp.logical_not(even)
    sends_one = me + 1 < n
    sends_two = even & (me + 2 < n)
    relays = even & (me >= 1)
    above = me + 4 - lax.rem(me, 4) < n
    crosses = (lax.rem(me, 4) >= 2) & above
    stays = jnp.logical_not(crosses)
    forwards = (lax.rem(me, 4) < 2) & above
    direct = sends_one & jnp.logical_not(crosses & odd)

    mid_own[0] = project(1, 0)
    mid_own[1] = project(1, 1)

    @pl.when(crosses)
    def _():
        via_mid.start()

    @pl.when(sends_two & stays)
    def _():
        key_two.start()
        value_two.start()

    @pl.when(direct)
    def _():
        key_one.start()
        value_one.start()

    near_own[0] = project(0, 0)
    near_own[1] = project(0, 1)

    @pl.when(crosses & odd)
    def _():
        via_last.start()

    @pl.when(direct)
    def _():
        near_key.start()
        near_value.start()

    mid_query[...] = swapped(project(1, 2))
    near_query[...] = swapped(project(0, 2))

    def slope_of(head, window):
        number = tp * local_heads + head
        slope = jnp.float32(0.0)
        for index in range(HEADS):
            value = 2.0 ** (3.0 - 8.0 * (index + 1.0) / HEADS) / window
            slope = jnp.where(number == index, jnp.float32(value), slope)
        return slope

    def spacing(row_count, key_count, offset, scattered):
        row = lax.broadcasted_iota(jnp.int32, (row_count, key_count), 0)
        column = lax.broadcasted_iota(jnp.int32, (row_count, key_count), 1)
        if scattered:
            row = ((row & (n - 1)) << shift) + (row >> shift)
        return row + offset - column, column

    each(lambda k: far_copy(0, k, False).wait_recv())
    each(lambda k: far_copy(1, k, False).wait_recv())

    @pl.when(crosses & even)
    def _():
        key_two.start()

    @pl.when(crosses & odd)
    def _():
        key_one.start()
        near_key.start()

    @pl.when(forwards)
    def _():
        via_mid.wait_recv()

    @pl.when(forwards & even)
    def _():
        onward_even.start()

    @pl.when(forwards & odd)
    def _():
        onward_odd.start()
        via_last.wait_recv()
        onward_near.start()

    reach = FAR_WINDOW // FAR_DILATION
    apart, _ = spacing(rows, rows, 0, False)
    valid = (apart >= 0) & (apart <= reach)
    distance = (apart * FAR_DILATION).astype(jnp.float32)
    lane = lax.broadcasted_iota(jnp.int32, (rows, HEAD_DIM), 1)
    slot = lax.broadcasted_iota(jnp.int32, (rows, HEAD_DIM), 0) & (chunk - 1)
    packed = jnp.zeros((rows, HEAD_DIM), jnp.float32)

    def far_part(head, part):
        block, half = divmod(head * 3 + part, local_heads)
        return far_held[block, :, half * HEAD_DIM : (half + 1) * HEAD_DIM]

    for head in range(local_heads):
        if head == local_heads - 1:
            each(lambda k: far_copy(2, k, False).wait_recv())
        probs, log_sum = weigh(
            far_part(head, 0), far_part(head, 1), slope_of(head, FAR_WINDOW), distance, valid
        )
        packed = jnp.where(lane == head * chunk + slot, log_sum, packed)
        if head == local_heads - 1:
            log_send[...] = jnp.sum(packed.reshape(n, chunk, HEAD_DIM), axis=1, keepdims=True)
            each(lambda k: log_copy(k, True).start())
            log_held[me] = log_send[me]
        back_send[head] = jnp.dot(
            probs, far_part(head, 2), preferred_element_type=jnp.float32
        ).astype(jnp.bfloat16)
        each(lambda k: back_copy(head, k, True).start())
        back_held[head, at_rows(me), :] = back_send[head, at_rows(me), :]

    @pl.when(me >= 1)
    def _():
        near_key.wait_recv()
        near_value.wait_recv()
        key_one.wait_recv()
        value_one.wait_recv()

    @pl.when(relays)
    def _():
        relay_key.start()
        relay_value.start()

    apart, column = spacing(rows, NEAR_WINDOW + rows, NEAR_WINDOW, True)
    valid = (apart >= 0) & (apart <= NEAR_WINDOW) & (column + me * rows >= NEAR_WINDOW)
    distance = apart.astype(jnp.float32)
    near = []
    for head in range(local_heads):
        at = pl.ds(head * HEAD_DIM, HEAD_DIM)
        key = jnp.concatenate((near_held[0, :, at], near_own[0, :, at]), axis=0)
        value = jnp.concatenate((near_held[1, :, at], near_own[1, :, at]), axis=0)
        near.append(attend(near_query[:, at], key, value, slope_of(head, NEAR_WINDOW), distance, valid))

    @pl.when(me >= 2)
    def _():
        key_two.wait_recv()
        value_two.wait_recv()

    apart, column = spacing(rows, MIDDLE_WINDOW + rows, MIDDLE_WINDOW, True)
    valid = (apart >= 0) & (apart <= MIDDLE_WINDOW) & ((apart & (MIDDLE_DILATION - 1)) == 0)
    valid = valid & (column + me * rows >= MIDDLE_WINDOW)
    distance = apart.astype(jnp.float32)
    pairs = []
    for head in range(local_heads):
        at = pl.ds(head * HEAD_DIM, HEAD_DIM)
        key = jnp.concatenate((mid_held[0, 0, :, at], mid_held[1, 0, :, at], mid_own[0, :, at]), axis=0)
        value = jnp.concatenate((mid_held[0, 1, :, at], mid_held[1, 1, :, at], mid_own[1, :, at]), axis=0)
        middle, middle_log = attend(
            mid_query[:, at], key, value, slope_of(head, MIDDLE_WINDOW), distance, valid
        )
        near_log = near[head][1]
        highest = jnp.maximum(near_log, middle_log)
        near_share, middle_share = jnp.exp(near_log - highest), jnp.exp(middle_log - highest)
        base[head] = near[head][0] * near_share + middle * middle_share
        pairs.append((highest, near_share + middle_share))

    each(lambda k: log_copy(k, False).wait_recv())

    spread = jnp.broadcast_to(log_held[...], (n, chunk, HEAD_DIM)).reshape(rows, HEAD_DIM)
    terms = jnp.zeros((rows, HEAD_DIM), jnp.float32)
    for head in range(local_heads):
        far_log = jnp.sum(
            jnp.where(lane == head * chunk + slot, spread, 0.0), axis=-1, keepdims=True
        )
        pair_log, pair_sum = pairs[head]
        highest = jnp.maximum(pair_log, far_log)
        total = highest + jnp.log(pair_sum * jnp.exp(pair_log - highest) + jnp.exp(far_log - highest))
        base[head] = base[head] * jnp.exp(pair_log - total)
        factor[head] = jnp.broadcast_to(jnp.exp(far_log - total), (rows, HEAD_DIM))
        rest = total
        for term in range(3):
            piece = rest.astype(jnp.bfloat16).astype(jnp.float32)
            terms = jnp.where(lane == 3 * head + term, piece, terms)
            rest = rest - piece

    def merged_copy(k, outgoing):
        place = at_rows(lax.rem(me + n - k, n))
        return pltpu.make_async_remote_copy(
            src_ref=merged_own.at[place],
            dst_ref=merged_held.at[place],
            send_sem=merged_ssem.at[k],
            recv_sem=merged_rsem.at[k],
            device_id=(me, peer),
            device_id_type=MESH,
        )

    def merge(k):
        place = at_rows(lax.rem(me + n - k, n))
        for head in range(local_heads):
            mixed = base[head, place, :] + back_held[head, place, :].astype(jnp.float32) * factor[head, place, :]
            merged_own[place, head * HEAD_DIM : (head + 1) * HEAD_DIM] = mixed.astype(jnp.bfloat16)
        merged_copy(k, True).start()

    merge(0)

    def arrive(k):
        for head in range(local_heads):
            back_copy(head, k, False).wait_recv()
        merge(k)

    each(arrive)

    totals = jnp.dot(swap, terms.astype(jnp.bfloat16), preferred_element_type=jnp.float32)
    summed = jnp.zeros((rows, HEAD_DIM), jnp.float32)
    for head in range(local_heads):
        total = jnp.sum(
            jnp.where((lane >= 3 * head) & (lane < 3 * head + 3), totals, 0.0), axis=-1, keepdims=True
        )
        summed = jnp.where(lane == head, total, summed)
    totals_ref[...] = summed
    wo_load.wait()
    partial_ref[...] = jnp.dot(
        swapped(merged_own[...]), wo[pl.ds(pl.multiple_of(tp * width, width), width), :],
        preferred_element_type=jnp.float32,
    )

    merged_copy(0, False).wait_recv()
    each(lambda k: merged_copy(k, False).wait_recv())
    peer_ref[...] = swapped(merged_held[...])

    merged_copy(0, True).wait_send()
    each(lambda k: merged_copy(k, True).wait_send())
    for block in range(3):
        each(lambda k: far_copy(block, k, True).wait_send())
    each(lambda k: log_copy(k, True).wait_send())
    for head in range(local_heads):
        each(lambda k: back_copy(head, k, True).wait_send())

    @pl.when(crosses)
    def _():
        via_mid.wait_send()

    @pl.when(crosses & odd)
    def _():
        via_last.wait_send()

    @pl.when(sends_two)
    def _():
        key_two.wait_send()

    @pl.when(sends_two & stays)
    def _():
        value_two.wait_send()

    @pl.when(sends_one)
    def _():
        key_one.wait_send()
        near_key.wait_send()

    @pl.when(direct)
    def _():
        value_one.wait_send()
        near_value.wait_send()

    @pl.when(forwards & even)
    def _():
        onward_even.wait_send()

    @pl.when(forwards & odd)
    def _():
        onward_odd.wait_send()
        onward_near.wait_send()

    @pl.when(relays)
    def _():
        relay_key.wait_send()
        relay_value.wait_send()


def mix(partial_ref, peer_ref, totals_ref, wo_ref, mixed_hbm, log_ref, out, sem):
    width = peer_ref.shape[1]
    steps = out.shape[0]
    piece = out.shape[2]
    at = pl.ds(pl.multiple_of((1 - lax.axis_index("tp")) * width, width), width)
    copies = []
    for step in range(steps):
        columns = pl.ds(step * piece, piece)
        product = jnp.dot(peer_ref[...], wo_ref[at, columns], preferred_element_type=jnp.float32)
        out[step] = (partial_ref[:, columns] + product).astype(jnp.bfloat16)
        copies.append(pltpu.make_async_copy(out.at[step], mixed_hbm.at[:, columns], sem.at[step]))
        copies[-1].start()
    log_ref[...] = jnp.transpose(totals_ref[...])[: log_ref.shape[0]]
    for copy in copies:
        copy.wait()


def fused(n, tokens, query_weight, key_weight, value_weight, out_weight):
    rows, depth = tokens.shape
    columns = query_weight.shape[1]
    out_columns = out_weight.shape[1]
    local_heads = columns // (3 * HEAD_DIM)
    width = local_heads * HEAD_DIM
    dma = pltpu.SemaphoreType.DMA
    half = jnp.bfloat16
    full = jnp.float32
    whole = pl.BlockSpec(memory_space=pltpu.VMEM)
    anywhere = pl.BlockSpec(memory_space=pl.ANY)
    partial, peer, totals = pl.pallas_call(
        functools.partial(kernel, n, local_heads),
        out_shape=(
            jax.ShapeDtypeStruct((rows, out_columns), full),
            jax.ShapeDtypeStruct((rows, width), half),
            jax.ShapeDtypeStruct((rows, HEAD_DIM), full),
        ),
        in_specs=[anywhere] * 5,
        out_specs=(whole, whole, whole),
        scratch_shapes=[
            pltpu.VMEM((rows, depth), half),
            pltpu.VMEM((3, depth, columns), half),
            pltpu.VMEM(out_weight.shape, half),
            pltpu.VMEM((3, rows, width), half),
            pltpu.VMEM((3, rows, width), half),
            pltpu.VMEM((local_heads, rows, HEAD_DIM), half),
            pltpu.VMEM((local_heads, rows, HEAD_DIM), half),
            pltpu.VMEM((n, 1, HEAD_DIM), full),
            pltpu.VMEM((n, 1, HEAD_DIM), full),
            pltpu.VMEM((rows, width), half),
            pltpu.VMEM((2, rows, width), half),
            pltpu.VMEM((2, 2, rows, width), half),
            pltpu.VMEM((rows, width), half),
            pltpu.VMEM((rows, width), half),
            pltpu.VMEM((2, rows, width), half),
            pltpu.VMEM((2, NEAR_WINDOW, width), half),
            pltpu.VMEM((NEAR_WINDOW, width), half),
            pltpu.VMEM((local_heads, rows, HEAD_DIM), full),
            pltpu.VMEM((local_heads, rows, HEAD_DIM), full),
            pltpu.VMEM((rows, width), half),
            pltpu.VMEM((rows, width), half),
            dma((2 + 9 * local_heads,)),
            dma((3, n)), dma((3, n)), dma((local_heads, n)), dma((local_heads, n)), dma((n,)), dma((n,)),
            dma((4, 2)), dma((2, 2)), dma((2,)), dma((2,)), dma((3,)), dma((2,)), dma((n,)), dma((n,)),
        ],
        compiler_params=pltpu.CompilerParams(
            collective_id=0, has_side_effects=True, vmem_limit_bytes=54000 * 1024
        ),
    )(tokens, query_weight, key_weight, value_weight, out_weight)
    pieces = out_columns // width
    return pl.pallas_call(
        mix,
        out_shape=(
            jax.ShapeDtypeStruct((rows, out_columns), half),
            jax.ShapeDtypeStruct((local_heads, rows), full),
        ),
        in_specs=[whole] * 4,
        out_specs=(anywhere, whole),
        scratch_shapes=[pltpu.VMEM((pieces, rows, width), half), dma((pieces,))],
        compiler_params=pltpu.CompilerParams(vmem_limit_bytes=16000 * 1024),
    )(partial, peer, totals, out_weight)


def solution(mesh):
    n, n_tp = mesh.shape["sp"], mesh.shape["tp"]
    if n == FAR_DILATION and n_tp == 2:
        body = functools.partial(fused, n)
    else:
        body = local
    return jax.shard_map(
        body,
        mesh=mesh,
        in_specs=(P("sp", None), P(None, "tp"), P(None, "tp"), P(None, "tp"), P(None, "tp")),
        out_specs=(P("sp", "tp"), P("tp", "sp")),
        check_vma=False,
    )
```

```python
import functools
import jax
import jax.numpy as jnp
from jax import lax
from jax.experimental import pallas as pl
from jax.experimental.pallas import tpu as pltpu
from jax.sharding import PartitionSpec as P

HEADS = 4
HEAD_DIM = 128
NEAR_WINDOW = 128
MIDDLE_WINDOW = 512
MIDDLE_DILATION = 4
FAR_WINDOW = 2048
FAR_DILATION = 16


def from_behind(block, axis, distance):
    devices = range(lax.axis_size(axis))
    route = [(i - distance, i) for i in devices if i - distance in devices]
    return lax.ppermute(block, axis, route)


def window_table():
    return ((NEAR_WINDOW, 1), (MIDDLE_WINDOW, MIDDLE_DILATION), (FAR_WINDOW, FAR_DILATION))


def tail_counts(row_count, distance, held_rows):
    counts = []
    for entry, available in zip(window_table(), held_rows):
        counts.append(max(0, min(available, entry[0] - (distance - 1) * row_count)))
    return counts


def pack_tails(sources, counts):
    selected = [
        source[:, source.shape[1] - amount :]
        for source, amount in zip(sources, counts)
        if amount > 0
    ]
    return jnp.concatenate(selected, axis=1)


def unpack_rows(packed, counts):
    result = []
    cursor = 0
    for amount in counts:
        result.append(packed[:, cursor : cursor + amount])
        cursor = cursor + amount
    return result


def attend_group(group_queries, buffer, window, dilation, first_key, slopes_here):
    row_count = group_queries.shape[0]
    head_count = group_queries.shape[1]
    head_size = group_queries.shape[2]
    query_split = group_queries.reshape(row_count // dilation, dilation, head_count, head_size)
    key_split = buffer[0].reshape(-1, dilation, head_count, head_size)
    value_split = buffer[1].reshape(-1, dilation, head_count, head_size)
    scores = jnp.einsum(
        "mrhe,nrhe->rhmn", query_split, key_split, preferred_element_type=jnp.float32
    ) * head_size ** (-0.5)
    grid_shape = (row_count // dilation, key_split.shape[0])
    query_slot = lax.broadcasted_iota(jnp.int32, grid_shape, 0)
    key_slot = lax.broadcasted_iota(jnp.int32, grid_shape, 1)
    spacing = query_slot + window // dilation - key_slot
    residue = lax.broadcasted_iota(jnp.int32, (dilation, 1, 1), 0)
    key_place = first_key + residue + dilation * key_slot[None]
    valid = (spacing[None] >= 0) & (spacing[None] <= window // dilation) & (key_place >= 0)
    scores = (
        scores
        - slopes_here[None, :, None, None] * (dilation * spacing).astype(jnp.float32)[None, None]
    )
    masked = jnp.where(valid[:, None], scores, -jnp.inf)
    highest = jnp.max(masked, axis=-1, keepdims=True)
    log_sum = highest + jnp.log(jnp.sum(jnp.exp(masked - highest), axis=-1, keepdims=True))
    probs = jnp.exp(masked - log_sum).astype(jnp.bfloat16)
    attended = jnp.einsum("rhmn,nrhe->mrhe", probs, value_split, preferred_element_type=jnp.float32)
    attended = attended.reshape(row_count, head_count, head_size)
    log_rows = jnp.transpose(log_sum[..., 0], (1, 2, 0)).reshape(head_count, row_count)
    return (attended, log_rows)


def local(tokens, query_weight, key_weight, value_weight, out_weight):
    rows_here = tokens.shape[0]
    local_heads = query_weight.shape[1] // (3 * HEAD_DIM)

    def project(weight_matrix):
        product = jnp.dot(tokens, weight_matrix, preferred_element_type=jnp.float32)
        return product.astype(jnp.bfloat16).reshape(rows_here, local_heads, 3, HEAD_DIM)

    queries = project(query_weight)
    keys_all = project(key_weight)
    values_all = project(value_weight)
    table = window_table()
    own = [jnp.stack((keys_all[:, :, index], values_all[:, :, index])) for index in range(3)]
    held = list(own)
    span_now = 1
    while span_now * rows_here < FAR_WINDOW + rows_here:
        counts = tail_counts(rows_here, span_now, [item.shape[1] for item in held])
        packed = pack_tails(held, counts)
        arrived = from_behind(packed, "sp", span_now)
        pieces_in = unpack_rows(arrived, counts)
        for index in range(3):
            if counts[index] > 0:
                joined = jnp.concatenate((pieces_in[index], held[index]), axis=1)
                held[index] = joined
        span_now = span_now * 2
    priors = [held[index][:, : table[index][0]] for index in range(3)]
    position_start = lax.axis_index("sp") * rows_here
    head_ids = (
        lax.axis_index("tp") * local_heads + jnp.arange(local_heads, dtype=jnp.int32)
    ).astype(jnp.float32)
    outputs = []
    logs = []
    for index, (window, dilation) in enumerate(table):
        buffer = jnp.concatenate((priors[index], own[index]), axis=1)
        slopes_here = 2.0 ** (3.0 - 8.0 * (head_ids + 1.0) / HEADS) / window
        attended, log_rows = attend_group(
            queries[:, :, index], buffer, window, dilation, position_start - window, slopes_here
        )
        outputs.append(attended)
        logs.append(log_rows)
    stacked_logs = jnp.stack(logs)
    highest = jnp.max(stacked_logs, axis=0)
    total_log = highest + jnp.log(jnp.sum(jnp.exp(stacked_logs - highest), axis=0))
    mixing = jnp.exp(stacked_logs - total_log)
    merged = outputs[0] * jnp.transpose(mixing[0])[:, :, None]
    merged = merged + outputs[1] * jnp.transpose(mixing[1])[:, :, None]
    merged = merged + outputs[2] * jnp.transpose(mixing[2])[:, :, None]
    merged = merged.astype(jnp.bfloat16).reshape(rows_here, local_heads * HEAD_DIM)
    mixed = jnp.dot(
        lax.all_gather(merged, "tp", axis=1, tiled=True),
        out_weight,
        preferred_element_type=jnp.float32,
    ).astype(jnp.bfloat16)
    return (mixed, total_log)


MESH = pl.DeviceIdType.MESH
MASKED = -1e30


def scores_of(query, key):
    return lax.dot_general(
        query, key, (((1,), (1,)), ((), ())), preferred_element_type=jnp.float32
    ) * HEAD_DIM ** (-0.5)


def weigh(scores, slope, distance, valid):
    scores = jnp.where(valid, scores - slope * distance, MASKED)
    highest = jnp.max(scores, axis=-1, keepdims=True)
    weights = jnp.exp(scores - highest)
    return highest, weights, jnp.sum(weights, axis=-1, keepdims=True)


def apply(weights, value):
    return jnp.dot(weights.astype(jnp.bfloat16), value, preferred_element_type=jnp.float32)


def one_hot(rows, token_of_row):
    row = lax.broadcasted_iota(jnp.int32, (rows, rows), 0)
    column = lax.broadcasted_iota(jnp.int32, (rows, rows), 1)
    return jnp.where(column == token_of_row(row), 1.0, 0.0).astype(jnp.bfloat16)


def kernel(
    n, local_heads,
    tok_hbm, wq_hbm, wk_hbm, wv_hbm, wo_hbm,
    partial_ref, peer_ref, totals_ref,
    tok, weight, wo, first_send, first_held, second_send, second_held, back_send, back_held, log_send, log_held,
    mid_query, mid_own, mid_held, via_held, near_query, near_own, near_held,
    base, stats, terms, merged_own, merged_held, near_sum,
    load_sem, first_sem, second_sem, back_ssem, back_rsem, log_ssem, log_rsem,
    mid_ssem, mid_rsem, via_ssem, via_rsem, near_ssem, near_rsem, merged_ssem, merged_rsem,
):
    me = lax.axis_index("sp")
    tp = lax.axis_index("tp")
    rows = tok.shape[0]
    width = local_heads * HEAD_DIM
    chunk = rows // n
    classes = MIDDLE_DILATION
    members = n // classes
    stretch = rows // classes
    peer = 1 - tp
    sources = (wq_hbm, wk_hbm, wv_hbm)

    tok_load = pltpu.make_async_copy(tok_hbm, tok, load_sem.at[0])
    tok_load.start()
    wo_load = pltpu.make_async_copy(wo_hbm, wo, load_sem.at[1])
    loads = []
    order = [(2, part, head) for head in range(local_heads) for part in range(3)]
    for group, part in ((0, 0), (0, 1), (0, 2), (1, 0)):
        order += [(group, part, head) for head in range(local_heads)]
    middle = [(1, part, head) for part in (1, 2) for head in range(local_heads)]
    order[2 * local_heads : 2 * local_heads] = middle
    for place, (group, part, head) in enumerate(order):
        loads.append(pltpu.make_async_copy(
            sources[part].at[:, pl.ds((head * 3 + group) * HEAD_DIM, HEAD_DIM)],
            weight.at[:, pl.ds(place * HEAD_DIM, HEAD_DIM)],
            load_sem.at[2 + place],
        ))
    early = 4 * local_heads
    for copy in loads[:early]:
        copy.start()

    barrier = pltpu.get_barrier_semaphore()

    def greet(k, carry):
        pl.semaphore_signal(barrier, inc=1, device_id=(lax.rem(me + k, n), tp), device_id_type=MESH)
        return carry

    lax.fori_loop(1, n, greet, 0)
    pl.semaphore_signal(barrier, inc=1, device_id=(me, peer), device_id_type=MESH)

    @pl.when(me < 2)
    def _():
        mid_held[0] = jnp.zeros((2, rows, width), jnp.bfloat16)

    @pl.when(me < 1)
    def _():
        mid_held[1] = jnp.zeros((2, rows, width), jnp.bfloat16)
        near_held[...] = jnp.zeros((2, NEAR_WINDOW, width), jnp.bfloat16)

    def project(first, last):
        for copy in loads[first * local_heads : last * local_heads]:
            copy.wait()
        return jnp.dot(
            tok[...], weight[:, first * width : last * width], preferred_element_type=jnp.float32
        ).astype(jnp.bfloat16)

    def at_rows(index):
        return pl.ds(pl.multiple_of(index * chunk, chunk), chunk)

    def scatter_token(row):
        group, index = row // chunk, row % chunk
        return index * n + (group % members) * classes + group // members

    def gather_row(token):
        index, residue = token // n, token % n
        return ((residue % classes) * members + residue // classes) * chunk + index

    def class_token(row):
        return (row % stretch) * classes + row // stretch

    to_scattered = one_hot(rows, scatter_token)
    to_tokens = one_hot(rows, gather_row)
    to_classes = one_hot(rows, class_token)

    def moved(matrix, block):
        return jnp.dot(matrix, block, preferred_element_type=jnp.float32).astype(jnp.bfloat16)

    def each(action):
        def step(k, carry):
            action(k)
            return carry

        lax.fori_loop(1, n, step, 0)

    plane = me // members
    upper = me // (n // 2)

    def target_of(k):
        rising = k - 1 + jnp.where(k - 1 >= me, 1, 0)
        falling = n - k - jnp.where(n - k <= me, 1, 0)
        return jnp.where(upper == 1, rising, falling)


    def far_copy(source, target, sem, k):
        to = target_of(k)
        return pltpu.make_async_remote_copy(
            src_ref=source.at[at_rows(to)],
            dst_ref=target.at[at_rows(me)],
            send_sem=sem.at[0],
            recv_sem=sem.at[1],
            device_id=(to, tp),
            device_id_type=MESH,
        )

    def far_whole(source, target, sem):
        others = pl.ds(0, rows - chunk)
        return pltpu.make_async_remote_copy(
            src_ref=source.at[others],
            dst_ref=target.at[others],
            send_sem=sem.at[0],
            recv_sem=sem.at[1],
            device_id=(lax.rem(me + 1, n), tp),
            device_id_type=MESH,
        )

    def back_copy(k):
        to = target_of(k)
        return pltpu.make_async_remote_copy(
            src_ref=back_send.at[at_rows(to)],
            dst_ref=back_held.at[at_rows(me)],
            send_sem=back_ssem,
            recv_sem=back_rsem.at[plane],
            device_id=(to, tp),
            device_id_type=MESH,
        )

    def back_whole(count, group):
        some = pl.ds(0, count * chunk)
        return pltpu.make_async_remote_copy(
            src_ref=back_send.at[some],
            dst_ref=back_held.at[some],
            send_sem=back_ssem,
            recv_sem=back_rsem.at[group],
            device_id=(lax.rem(me + 1, n), tp),
            device_id_type=MESH,
        )

    def log_copy(k):
        to = target_of(k)
        return pltpu.make_async_remote_copy(
            src_ref=log_send.at[to],
            dst_ref=log_held.at[me],
            send_sem=log_ssem,
            recv_sem=log_rsem.at[plane],
            device_id=(to, tp),
            device_id_type=MESH,
        )

    def log_whole(count, group):
        some = pl.ds(0, count)
        return pltpu.make_async_remote_copy(
            src_ref=log_send.at[some],
            dst_ref=log_held.at[some],
            send_sem=log_ssem,
            recv_sem=log_rsem.at[group],
            device_id=(lax.rem(me + 1, n), tp),
            device_id_type=MESH,
        )

    tok_load.wait()
    first_send[...] = moved(to_scattered, project(0, 2))
    for copy in loads[early:]:
        copy.start()
    pl.semaphore_wait(barrier, n)
    each(lambda k: far_copy(first_send, first_held, first_sem, k).start())
    first_held[at_rows(me), :] = first_send[at_rows(me), :]

    def mid_copy(slot, hop, source, part, sem):
        return pltpu.make_async_remote_copy(
            src_ref=source,
            dst_ref=mid_held.at[slot, part],
            send_sem=mid_ssem.at[sem, part],
            recv_sem=mid_rsem.at[slot, part],
            device_id=(lax.rem(me + hop + n, n), tp),
            device_id_type=MESH,
        )

    def near_copy(hop, source, part, sem):
        return pltpu.make_async_remote_copy(
            src_ref=source,
            dst_ref=near_held.at[part],
            send_sem=near_ssem.at[sem],
            recv_sem=near_rsem.at[part],
            device_id=(lax.rem(me + hop, n), tp),
            device_id_type=MESH,
        )

    def via_copy(which, source, target):
        return pltpu.make_async_remote_copy(
            src_ref=source,
            dst_ref=target,
            send_sem=via_ssem.at[which],
            recv_sem=via_rsem.at[which],
            device_id=(lax.rem(me + -2 + n, n), tp),
            device_id_type=MESH,
        )

    near_tail = pl.ds(rows - NEAR_WINDOW, NEAR_WINDOW)
    key_two = mid_copy(0, 2, mid_own.at[0], 0, 0)
    key_one = mid_copy(1, 1, mid_own.at[0], 0, 1)
    value_two = mid_copy(0, 2, mid_own.at[1], 1, 0)
    value_one = mid_copy(1, 1, mid_own.at[1], 1, 1)
    near_key = near_copy(1, near_own.at[0, near_tail], 0, 0)
    near_value = near_copy(1, near_own.at[1, near_tail], 1, 1)
    via_mid = via_copy(0, mid_own.at[1], via_held)
    onward_even = mid_copy(0, 4, via_held, 1, 3)
    onward_odd = mid_copy(1, 3, via_held, 1, 3)
    relay_key = mid_copy(0, 1, mid_held.at[1, 0], 0, 2)
    relay_value = mid_copy(0, 1, mid_held.at[1, 1], 1, 2)

    even = lax.rem(me, 2) == 0
    odd = jnp.logical_not(even)
    sends_one = me + 1 < n
    sends_two = even & (me + 2 < n)
    relays = even & (me >= 1)
    above = me + 4 - lax.rem(me, 4) < n
    crosses = (lax.rem(me, 4) >= 2) & above
    stays = jnp.logical_not(crosses)
    forwards = (lax.rem(me, 4) < 2) & above
    direct = sends_one & jnp.logical_not(crosses & odd)

    pair = moved(to_classes, project(2, 4))
    mid_own[0] = pair[:, :width]
    mid_own[1] = pair[:, width:]

    @pl.when(crosses)
    def _():
        via_mid.start()

    pair = moved(to_scattered, project(4, 6))
    second_send[...] = pair[:, :width]
    near_query[...] = pair[:, width:]
    each(lambda k: far_copy(second_send, second_held, second_sem, k).start())
    second_held[at_rows(me), :] = second_send[at_rows(me), :]
    wo_load.start()

    @pl.when(sends_two & stays)
    def _():
        key_two.start()
        value_two.start()

    @pl.when(direct)
    def _():
        key_one.start()
        value_one.start()

    pair = project(6, 8)
    near_own[0] = pair[:, :width]
    near_own[1] = pair[:, width:]

    @pl.when(direct)
    def _():
        near_key.start()
        near_value.start()

    @pl.when(crosses & even)
    def _():
        key_two.start()

    @pl.when(crosses & odd)
    def _():
        near_key.start()
        near_value.start()
        key_one.start()

    mid_query[...] = moved(to_scattered, project(8, 9))

    def slope_of(head, window):
        number = tp * local_heads + head
        slope = jnp.float32(0.0)
        for index in range(HEADS):
            value = 2.0 ** (3.0 - 8.0 * (index + 1.0) / HEADS) / window
            slope = jnp.where(number == index, jnp.float32(value), slope)
        return slope

    def grid(row_count, key_count):
        row = lax.broadcasted_iota(jnp.int32, (row_count, key_count), 0)
        column = lax.broadcasted_iota(jnp.int32, (row_count, key_count), 1)
        return row, column

    row, column = grid(rows, rows)
    apart = scatter_token(row) - column
    valid = (apart >= 0) & (apart <= NEAR_WINDOW)
    distance = apart.astype(jnp.float32)
    near = []
    for head in range(local_heads):
        at = pl.ds(head * HEAD_DIM, HEAD_DIM)
        highest, weights, total = weigh(
            scores_of(near_query[:, at], near_own[0, :, at]), slope_of(head, NEAR_WINDOW), distance, valid
        )
        near_sum[head] = apply(weights, near_own[1, :, at])
        near.append((highest, total))

    @pl.when(forwards)
    def _():
        via_mid.wait_recv()

    @pl.when(forwards & even)
    def _():
        onward_even.start()

    @pl.when(forwards & odd)
    def _():
        onward_odd.start()

    far_whole(first_send, first_held, first_sem).wait_recv()
    far_whole(second_send, second_held, second_sem).wait_recv()

    row, column = grid(rows, rows)
    apart = row - column
    valid = (apart >= 0) & (apart <= FAR_WINDOW // FAR_DILATION)
    distance = (apart * FAR_DILATION).astype(jnp.float32)
    lane = lax.broadcasted_iota(jnp.int32, (rows, HEAD_DIM), 1)
    slot = lax.broadcasted_iota(jnp.int32, (rows, HEAD_DIM), 0) & (chunk - 1)
    packed = jnp.zeros((rows, HEAD_DIM), jnp.float32)

    def far_part(head, part):
        place = head * 3 + part
        if place < 2 * local_heads:
            return first_held[:, place * HEAD_DIM : (place + 1) * HEAD_DIM]
        place -= 2 * local_heads
        return second_held[:, place * HEAD_DIM : (place + 1) * HEAD_DIM]

    for head in range(local_heads):
        highest, weights, total = weigh(
            scores_of(far_part(head, 0), far_part(head, 1)), slope_of(head, FAR_WINDOW), distance, valid
        )
        packed = jnp.where(lane == head * chunk + slot, highest + jnp.log(total), packed)
        back_send[:, head * HEAD_DIM : (head + 1) * HEAD_DIM] = apply(
            weights * (1.0 / total), far_part(head, 2)
        ).astype(jnp.bfloat16)
    log_send[...] = jnp.sum(packed.reshape(n, chunk, HEAD_DIM), axis=1, keepdims=True)

    def send_back(k):
        log_copy(k).start()
        back_copy(k).start()

    each(send_back)
    log_held[me] = log_send[me]
    back_held[at_rows(me), :] = back_send[at_rows(me), :]

    @pl.when(me >= 1)
    def _():
        near_key.wait_recv()
        near_value.wait_recv()
        key_one.wait_recv()
        value_one.wait_recv()

    @pl.when(relays)
    def _():
        relay_key.start()
        relay_value.start()

    row, column = grid(rows, NEAR_WINDOW)
    apart = scatter_token(row) + NEAR_WINDOW - column
    valid = (apart >= 0) & (apart <= NEAR_WINDOW) & (column + me * rows >= NEAR_WINDOW)
    distance = apart.astype(jnp.float32)
    for head in range(local_heads):
        at = pl.ds(head * HEAD_DIM, HEAD_DIM)
        own_high, own_total = near[head]
        high, weights, total = weigh(
            scores_of(near_query[:, at], near_held[0, :, at]), slope_of(head, NEAR_WINDOW), distance, valid
        )
        highest = jnp.maximum(own_high, high)
        own_share, share = jnp.exp(own_high - highest), jnp.exp(high - highest)
        near_sum[head] = near_sum[head] * own_share + apply(weights, near_held[1, :, at]) * share
        near[head] = (highest, own_total * own_share + total * share)

    @pl.when(me >= 2)
    def _():
        key_two.wait_recv()
        value_two.wait_recv()

    keys = MIDDLE_WINDOW // classes + stretch
    row, column = grid(rows, keys)
    apart = (row % chunk) * members + (row // chunk) % members + MIDDLE_WINDOW // classes - column
    valid = (apart >= 0) & (apart <= MIDDLE_WINDOW // classes)
    valid = valid & (column + me * stretch >= MIDDLE_WINDOW // classes)
    distance = (apart * classes).astype(jnp.float32)

    def class_rows(part, group, at):
        of_class = pl.ds(group * stretch, stretch)
        return jnp.concatenate(
            (mid_held[0, part, of_class, at], mid_held[1, part, of_class, at], mid_own[part, of_class, at]), axis=0
        )

    for head in range(local_heads):
        at = pl.ds(head * HEAD_DIM, HEAD_DIM)
        scores = jnp.concatenate([
            scores_of(mid_query[group * stretch : (group + 1) * stretch, at], class_rows(0, group, at))
            for group in range(classes)
        ], axis=0)
        high, weights, total = weigh(scores, slope_of(head, MIDDLE_WINDOW), distance, valid)
        middle = jnp.concatenate([
            apply(weights[group * stretch : (group + 1) * stretch], class_rows(1, group, at))
            for group in range(classes)
        ], axis=0)
        near_high, near_total = near[head]
        highest = jnp.maximum(near_high, high)
        near_share, share = jnp.exp(near_high - highest), jnp.exp(high - highest)
        base[head] = near_sum[head] * near_share + middle * share
        stats[2 * head] = highest
        stats[2 * head + 1] = near_total * near_share + total * share

    def merged_copy(group):
        place = pl.ds(pl.multiple_of(group * members * chunk, members * chunk), members * chunk)
        return pltpu.make_async_remote_copy(
            src_ref=merged_own.at[place],
            dst_ref=merged_held.at[place],
            send_sem=merged_ssem.at[group],
            recv_sem=merged_rsem.at[group],
            device_id=(me, peer),
            device_id_type=MESH,
        )

    block = members * chunk
    lane = lax.broadcasted_iota(jnp.int32, (block, HEAD_DIM), 1)
    slot = lax.broadcasted_iota(jnp.int32, (block, HEAD_DIM), 0) & (chunk - 1)
    for step in range(n // members):
        group = lax.rem(plane + step, n // members)
        count = members - 1 if step == 0 else members
        log_whole(count, group).wait_recv()
        back_whole(count, group).wait_recv()
        place = pl.ds(pl.multiple_of(group * block, block), block)
        held = log_held[pl.ds(group * members, members)]
        spread = jnp.broadcast_to(held, (members, chunk, HEAD_DIM)).reshape(block, HEAD_DIM)
        split = jnp.zeros((block, HEAD_DIM), jnp.float32)
        for head in range(local_heads):
            at = pl.ds(head * HEAD_DIM, HEAD_DIM)
            far_log = jnp.sum(
                jnp.where(lane == head * chunk + slot, spread, 0.0), axis=-1, keepdims=True
            )
            pair_log, pair_sum = stats[2 * head, place], stats[2 * head + 1, place]
            highest = jnp.maximum(pair_log, far_log)
            pair_share, far_share = jnp.exp(pair_log - highest), jnp.exp(far_log - highest)
            mass = pair_sum * pair_share + far_share
            inverse = 1.0 / mass
            merged = base[head, place] * (pair_share * inverse)
            merged = merged + back_held[place, at].astype(jnp.float32) * (far_share * inverse)
            merged_own[place, at] = merged.astype(jnp.bfloat16)
            rest = highest + jnp.log(mass)
            for term in range(3):
                piece = rest.astype(jnp.bfloat16).astype(jnp.float32)
                split = jnp.where(lane == 3 * head + term, piece, split)
                rest = rest - piece
        terms[place] = split.astype(jnp.bfloat16)
        merged_copy(group).start()

    lane = lax.broadcasted_iota(jnp.int32, (rows, HEAD_DIM), 1)
    totals = jnp.dot(to_tokens, terms[...], preferred_element_type=jnp.float32)
    summed = jnp.zeros((rows, HEAD_DIM), jnp.float32)
    for head in range(local_heads):
        total = jnp.sum(
            jnp.where((lane >= 3 * head) & (lane < 3 * head + 3), totals, 0.0), axis=-1, keepdims=True
        )
        summed = jnp.where(lane == head, total, summed)
    totals_ref[...] = summed
    wo_load.wait()
    partial_ref[...] = jnp.dot(
        moved(to_tokens, merged_own[...]), wo[pl.ds(pl.multiple_of(tp * width, width), width), :],
        preferred_element_type=jnp.float32,
    )

    far_whole(first_send, first_held, first_sem).wait_send()
    far_whole(second_send, second_held, second_sem).wait_send()
    log_whole(n - 1, 0).wait_send()
    back_whole(n - 1, 0).wait_send()

    @pl.when(crosses)
    def _():
        via_mid.wait_send()

    @pl.when(sends_two)
    def _():
        key_two.wait_send()

    @pl.when(sends_two & stays)
    def _():
        value_two.wait_send()

    @pl.when(sends_one)
    def _():
        key_one.wait_send()
        near_key.wait_send()
        near_value.wait_send()

    @pl.when(direct)
    def _():
        value_one.wait_send()

    @pl.when(forwards & even)
    def _():
        onward_even.wait_send()

    @pl.when(forwards & odd)
    def _():
        onward_odd.wait_send()

    @pl.when(relays)
    def _():
        relay_key.wait_send()
        relay_value.wait_send()

    for group in range(n // members):
        merged_copy(group).wait_recv()
    peer_ref[...] = moved(to_tokens, merged_held[...])
    for group in range(n // members):
        merged_copy(group).wait_send()


def mix(partial_ref, peer_ref, totals_ref, wo_ref, mixed_hbm, log_ref, out, sem):
    width = peer_ref.shape[1]
    steps = out.shape[0]
    piece = out.shape[2]
    at = pl.ds(pl.multiple_of((1 - lax.axis_index("tp")) * width, width), width)
    copies = []
    for step in range(steps):
        columns = pl.ds(step * piece, piece)
        product = jnp.dot(peer_ref[...], wo_ref[at, columns], preferred_element_type=jnp.float32)
        out[step] = (partial_ref[:, columns] + product).astype(jnp.bfloat16)
        copies.append(pltpu.make_async_copy(out.at[step], mixed_hbm.at[:, columns], sem.at[step]))
        copies[-1].start()
    log_ref[...] = jnp.transpose(totals_ref[...])[: log_ref.shape[0]]
    for copy in copies:
        copy.wait()


def fused(n, tokens, query_weight, key_weight, value_weight, out_weight):
    rows, depth = tokens.shape
    columns = query_weight.shape[1]
    out_columns = out_weight.shape[1]
    local_heads = columns // (3 * HEAD_DIM)
    width = local_heads * HEAD_DIM
    planes = MIDDLE_DILATION
    dma = pltpu.SemaphoreType.DMA
    half = jnp.bfloat16
    full = jnp.float32
    whole = pl.BlockSpec(memory_space=pltpu.VMEM)
    anywhere = pl.BlockSpec(memory_space=pl.ANY)
    partial, peer, totals = pl.pallas_call(
        functools.partial(kernel, n, local_heads),
        out_shape=(
            jax.ShapeDtypeStruct((rows, out_columns), full),
            jax.ShapeDtypeStruct((rows, width), half),
            jax.ShapeDtypeStruct((rows, HEAD_DIM), full),
        ),
        in_specs=[anywhere] * 5,
        out_specs=(whole, whole, whole),
        scratch_shapes=[
            pltpu.VMEM((rows, depth), half),
            pltpu.VMEM((depth, 3 * columns), half),
            pltpu.VMEM(out_weight.shape, half),
            pltpu.VMEM((rows, 2 * width), half),
            pltpu.VMEM((rows, 2 * width), half),
            pltpu.VMEM((rows, width), half),
            pltpu.VMEM((rows, width), half),
            pltpu.VMEM((rows, width), half),
            pltpu.VMEM((rows, width), half),
            pltpu.VMEM((n, 1, HEAD_DIM), full),
            pltpu.VMEM((n, 1, HEAD_DIM), full),
            pltpu.VMEM((rows, width), half),
            pltpu.VMEM((2, rows, width), half),
            pltpu.VMEM((2, 2, rows, width), half),
            pltpu.VMEM((rows, width), half),
            pltpu.VMEM((rows, width), half),
            pltpu.VMEM((2, rows, width), half),
            pltpu.VMEM((2, NEAR_WINDOW, width), half),
            pltpu.VMEM((local_heads, rows, HEAD_DIM), full),
            pltpu.VMEM((2 * local_heads, rows, 1), full),
            pltpu.VMEM((rows, HEAD_DIM), half),
            pltpu.VMEM((rows, width), half),
            pltpu.VMEM((rows, width), half),
            pltpu.VMEM((local_heads, rows, HEAD_DIM), full),
            dma((2 + 9 * local_heads,)),
            dma((2,)), dma((2,)), dma(()), dma((planes,)), dma(()), dma((planes,)),
            dma((4, 2)), dma((2, 2)), dma((1,)), dma((1,)), dma((2,)), dma((2,)), dma((planes,)), dma((planes,)),
        ],
        compiler_params=pltpu.CompilerParams(
            collective_id=0, has_side_effects=True, vmem_limit_bytes=53000 * 1024
        ),
    )(tokens, query_weight, key_weight, value_weight, out_weight)
    pieces = out_columns // width
    return pl.pallas_call(
        mix,
        out_shape=(
            jax.ShapeDtypeStruct((rows, out_columns), half),
            jax.ShapeDtypeStruct((local_heads, rows), full),
        ),
        in_specs=[whole] * 4,
        out_specs=(anywhere, whole),
        scratch_shapes=[pltpu.VMEM((pieces, rows, width), half), dma((pieces,))],
        compiler_params=pltpu.CompilerParams(vmem_limit_bytes=16000 * 1024),
    )(partial, peer, totals, out_weight)


def solution(mesh):
    n, n_tp = mesh.shape["sp"], mesh.shape["tp"]
    if n == FAR_DILATION and n_tp == 2:
        body = functools.partial(fused, n)
    else:
        body = local
    return jax.shard_map(
        body,
        mesh=mesh,
        in_specs=(P("sp", None), P(None, "tp"), P(None, "tp"), P(None, "tp"), P(None, "tp")),
        out_specs=(P("sp", "tp"), P("tp", "sp")),
        check_vma=False,
    )
```

```python
import functools
import jax
import jax.numpy as jnp
from jax import lax
from jax.experimental import pallas as pl
from jax.experimental.pallas import tpu as pltpu
from jax.sharding import PartitionSpec as P

HEADS = 4
HEAD_DIM = 128
NEAR_WINDOW = 128
MIDDLE_WINDOW = 512
MIDDLE_DILATION = 4
FAR_WINDOW = 2048
FAR_DILATION = 16


def from_behind(block, axis, distance):
    devices = range(lax.axis_size(axis))
    route = [(i - distance, i) for i in devices if i - distance in devices]
    return lax.ppermute(block, axis, route)


def window_table():
    return ((NEAR_WINDOW, 1), (MIDDLE_WINDOW, MIDDLE_DILATION), (FAR_WINDOW, FAR_DILATION))


def tail_counts(row_count, distance, held_rows):
    counts = []
    for entry, available in zip(window_table(), held_rows):
        counts.append(max(0, min(available, entry[0] - (distance - 1) * row_count)))
    return counts


def pack_tails(sources, counts):
    selected = [
        source[:, source.shape[1] - amount :]
        for source, amount in zip(sources, counts)
        if amount > 0
    ]
    return jnp.concatenate(selected, axis=1)


def unpack_rows(packed, counts):
    result = []
    cursor = 0
    for amount in counts:
        result.append(packed[:, cursor : cursor + amount])
        cursor = cursor + amount
    return result


def attend_group(group_queries, buffer, window, dilation, first_key, slopes_here):
    row_count = group_queries.shape[0]
    head_count = group_queries.shape[1]
    head_size = group_queries.shape[2]
    query_split = group_queries.reshape(row_count // dilation, dilation, head_count, head_size)
    key_split = buffer[0].reshape(-1, dilation, head_count, head_size)
    value_split = buffer[1].reshape(-1, dilation, head_count, head_size)
    scores = jnp.einsum(
        "mrhe,nrhe->rhmn", query_split, key_split, preferred_element_type=jnp.float32
    ) * head_size ** (-0.5)
    grid_shape = (row_count // dilation, key_split.shape[0])
    query_slot = lax.broadcasted_iota(jnp.int32, grid_shape, 0)
    key_slot = lax.broadcasted_iota(jnp.int32, grid_shape, 1)
    spacing = query_slot + window // dilation - key_slot
    residue = lax.broadcasted_iota(jnp.int32, (dilation, 1, 1), 0)
    key_place = first_key + residue + dilation * key_slot[None]
    valid = (spacing[None] >= 0) & (spacing[None] <= window // dilation) & (key_place >= 0)
    scores = (
        scores
        - slopes_here[None, :, None, None] * (dilation * spacing).astype(jnp.float32)[None, None]
    )
    masked = jnp.where(valid[:, None], scores, -jnp.inf)
    highest = jnp.max(masked, axis=-1, keepdims=True)
    log_sum = highest + jnp.log(jnp.sum(jnp.exp(masked - highest), axis=-1, keepdims=True))
    probs = jnp.exp(masked - log_sum).astype(jnp.bfloat16)
    attended = jnp.einsum("rhmn,nrhe->mrhe", probs, value_split, preferred_element_type=jnp.float32)
    attended = attended.reshape(row_count, head_count, head_size)
    log_rows = jnp.transpose(log_sum[..., 0], (1, 2, 0)).reshape(head_count, row_count)
    return (attended, log_rows)


def local(tokens, query_weight, key_weight, value_weight, out_weight):
    rows_here = tokens.shape[0]
    local_heads = query_weight.shape[1] // (3 * HEAD_DIM)

    def project(weight_matrix):
        product = jnp.dot(tokens, weight_matrix, preferred_element_type=jnp.float32)
        return product.astype(jnp.bfloat16).reshape(rows_here, local_heads, 3, HEAD_DIM)

    queries = project(query_weight)
    keys_all = project(key_weight)
    values_all = project(value_weight)
    table = window_table()
    own = [jnp.stack((keys_all[:, :, index], values_all[:, :, index])) for index in range(3)]
    held = list(own)
    span_now = 1
    while span_now * rows_here < FAR_WINDOW + rows_here:
        counts = tail_counts(rows_here, span_now, [item.shape[1] for item in held])
        packed = pack_tails(held, counts)
        arrived = from_behind(packed, "sp", span_now)
        pieces_in = unpack_rows(arrived, counts)
        for index in range(3):
            if counts[index] > 0:
                joined = jnp.concatenate((pieces_in[index], held[index]), axis=1)
                held[index] = joined
        span_now = span_now * 2
    priors = [held[index][:, : table[index][0]] for index in range(3)]
    position_start = lax.axis_index("sp") * rows_here
    head_ids = (
        lax.axis_index("tp") * local_heads + jnp.arange(local_heads, dtype=jnp.int32)
    ).astype(jnp.float32)
    outputs = []
    logs = []
    for index, (window, dilation) in enumerate(table):
        buffer = jnp.concatenate((priors[index], own[index]), axis=1)
        slopes_here = 2.0 ** (3.0 - 8.0 * (head_ids + 1.0) / HEADS) / window
        attended, log_rows = attend_group(
            queries[:, :, index], buffer, window, dilation, position_start - window, slopes_here
        )
        outputs.append(attended)
        logs.append(log_rows)
    stacked_logs = jnp.stack(logs)
    highest = jnp.max(stacked_logs, axis=0)
    total_log = highest + jnp.log(jnp.sum(jnp.exp(stacked_logs - highest), axis=0))
    mixing = jnp.exp(stacked_logs - total_log)
    merged = outputs[0] * jnp.transpose(mixing[0])[:, :, None]
    merged = merged + outputs[1] * jnp.transpose(mixing[1])[:, :, None]
    merged = merged + outputs[2] * jnp.transpose(mixing[2])[:, :, None]
    merged = merged.astype(jnp.bfloat16).reshape(rows_here, local_heads * HEAD_DIM)
    mixed = jnp.dot(
        lax.all_gather(merged, "tp", axis=1, tiled=True),
        out_weight,
        preferred_element_type=jnp.float32,
    ).astype(jnp.bfloat16)
    return (mixed, total_log)


MESH = pl.DeviceIdType.MESH
MASKED = -1e30


def scores_of(query, key):
    return lax.dot_general(
        query, key, (((1,), (1,)), ((), ())), preferred_element_type=jnp.float32
    ) * HEAD_DIM ** (-0.5)


def weigh(scores, slope, distance, valid):
    scores = jnp.where(valid, scores - slope * distance, MASKED)
    highest = jnp.max(scores, axis=-1, keepdims=True)
    weights = jnp.exp(scores - highest)
    return highest, weights, jnp.sum(weights, axis=-1, keepdims=True)


def apply(weights, value):
    return jnp.dot(weights.astype(jnp.bfloat16), value, preferred_element_type=jnp.float32)


def one_hot(rows, token_of_row):
    row = lax.broadcasted_iota(jnp.int32, (rows, rows), 0)
    column = lax.broadcasted_iota(jnp.int32, (rows, rows), 1)
    return jnp.where(column == token_of_row(row), 1.0, 0.0).astype(jnp.bfloat16)


def kernel(
    n, local_heads,
    tok_hbm, wq_hbm, wk_hbm, wv_hbm, wo_hbm,
    partial_ref, peer_ref, totals_ref,
    tok, weight, wo, first_send, first_held, second_send, second_held, back_send, back_held, log_send, log_held,
    mid_query, mid_own, mid_held, via_held, near_query, near_own, near_held,
    stats, terms, merged_own, merged_held, near_sum,
    load_sem, first_sem, second_sem, back_ssem, back_rsem, log_ssem, log_rsem,
    mid_ssem, mid_rsem, via_ssem, via_rsem, near_ssem, near_rsem, merged_ssem, merged_rsem,
):
    me = lax.axis_index("sp")
    tp = lax.axis_index("tp")
    rows = tok.shape[0]
    width = local_heads * HEAD_DIM
    chunk = rows // n
    classes = MIDDLE_DILATION
    members = n // classes
    stretch = rows // classes
    peer = 1 - tp
    sources = (wq_hbm, wk_hbm, wv_hbm)

    tok_load = pltpu.make_async_copy(tok_hbm, tok, load_sem.at[0])
    tok_load.start()
    wo_load = pltpu.make_async_copy(wo_hbm, wo, load_sem.at[1])
    loads = []
    order = [(2, part, head) for head in range(local_heads) for part in range(3)]
    for group, part in ((0, 0), (0, 1), (0, 2), (1, 0)):
        order += [(group, part, head) for head in range(local_heads)]
    middle = [(1, part, head) for part in (1, 2) for head in range(local_heads)]
    order[2 * local_heads : 2 * local_heads] = middle
    for place, (group, part, head) in enumerate(order):
        loads.append(pltpu.make_async_copy(
            sources[part].at[:, pl.ds((head * 3 + group) * HEAD_DIM, HEAD_DIM)],
            weight.at[:, pl.ds(place * HEAD_DIM, HEAD_DIM)],
            load_sem.at[2 + place],
        ))
    first = 2 * local_heads
    early = 4 * local_heads
    for copy in loads[:first]:
        copy.start()

    barrier = pltpu.get_barrier_semaphore()

    def greet(k, carry):
        pl.semaphore_signal(barrier, inc=1, device_id=(lax.rem(me + k, n), tp), device_id_type=MESH)
        return carry

    lax.fori_loop(1, n, greet, 0)
    pl.semaphore_signal(barrier, inc=1, device_id=(me, peer), device_id_type=MESH)
    for copy in loads[first:early]:
        copy.start()

    @pl.when(me < 2)
    def _():
        mid_held[0] = jnp.zeros((2, rows, width), jnp.bfloat16)

    @pl.when(me < 1)
    def _():
        mid_held[1] = jnp.zeros((2, rows, width), jnp.bfloat16)

    def project(first, last):
        for copy in loads[first * local_heads : last * local_heads]:
            copy.wait()
        return jnp.dot(
            tok[...], weight[:, first * width : last * width], preferred_element_type=jnp.float32
        ).astype(jnp.bfloat16)

    def at_rows(index):
        return pl.ds(pl.multiple_of(index * chunk, chunk), chunk)

    def scatter_token(row):
        group, index = row // chunk, row % chunk
        return index * n + (group % members) * classes + group // members

    def gather_row(token):
        index, residue = token // n, token % n
        return ((residue % classes) * members + residue // classes) * chunk + index

    def class_token(row):
        return (row % stretch) * classes + row // stretch

    to_scattered = one_hot(rows, scatter_token)
    to_tokens = one_hot(rows, gather_row)
    to_classes = one_hot(rows, class_token)

    def moved(matrix, block):
        return jnp.dot(matrix, block, preferred_element_type=jnp.float32).astype(jnp.bfloat16)

    def each(action):
        def step(k, carry):
            action(k)
            return carry

        lax.fori_loop(1, n, step, 0)

    plane = me // members
    upper = me // (n // 2)

    def target_of(k):
        rising = k - 1 + jnp.where(k - 1 >= me, 1, 0)
        falling = n - k - jnp.where(n - k <= me, 1, 0)
        return jnp.where(upper == 1, rising, falling)


    def far_copy(source, target, sem, k):
        to = target_of(k)
        return pltpu.make_async_remote_copy(
            src_ref=source.at[at_rows(to)],
            dst_ref=target.at[at_rows(me)],
            send_sem=sem.at[0],
            recv_sem=sem.at[1],
            device_id=(to, tp),
            device_id_type=MESH,
        )

    def far_whole(source, target, sem):
        others = pl.ds(0, rows - chunk)
        return pltpu.make_async_remote_copy(
            src_ref=source.at[others],
            dst_ref=target.at[others],
            send_sem=sem.at[0],
            recv_sem=sem.at[1],
            device_id=(lax.rem(me + 1, n), tp),
            device_id_type=MESH,
        )

    def back_copy(k):
        to = target_of(k)
        return pltpu.make_async_remote_copy(
            src_ref=back_send.at[at_rows(to)],
            dst_ref=back_held.at[at_rows(me)],
            send_sem=back_ssem,
            recv_sem=back_rsem.at[plane],
            device_id=(to, tp),
            device_id_type=MESH,
        )

    def back_whole(count, group):
        some = pl.ds(0, count * chunk)
        return pltpu.make_async_remote_copy(
            src_ref=back_send.at[some],
            dst_ref=back_held.at[some],
            send_sem=back_ssem,
            recv_sem=back_rsem.at[group],
            device_id=(lax.rem(me + 1, n), tp),
            device_id_type=MESH,
        )

    def log_copy(k):
        to = target_of(k)
        return pltpu.make_async_remote_copy(
            src_ref=log_send.at[to],
            dst_ref=log_held.at[me],
            send_sem=log_ssem,
            recv_sem=log_rsem.at[plane],
            device_id=(to, tp),
            device_id_type=MESH,
        )

    def log_whole(count, group):
        some = pl.ds(0, count)
        return pltpu.make_async_remote_copy(
            src_ref=log_send.at[some],
            dst_ref=log_held.at[some],
            send_sem=log_ssem,
            recv_sem=log_rsem.at[group],
            device_id=(lax.rem(me + 1, n), tp),
            device_id_type=MESH,
        )

    tok_load.wait()
    first_send[...] = moved(to_scattered, project(0, 2))
    for copy in loads[early:]:
        copy.start()
    pl.semaphore_wait(barrier, n)
    each(lambda k: far_copy(first_send, first_held, first_sem, k).start())
    first_held[at_rows(me), :] = first_send[at_rows(me), :]

    def mid_copy(slot, hop, source, part, sem):
        return pltpu.make_async_remote_copy(
            src_ref=source,
            dst_ref=mid_held.at[slot, part],
            send_sem=mid_ssem.at[sem, part],
            recv_sem=mid_rsem.at[slot, part],
            device_id=(lax.rem(me + hop + n, n), tp),
            device_id_type=MESH,
        )

    def near_copy(hop, source, part, sem):
        return pltpu.make_async_remote_copy(
            src_ref=source,
            dst_ref=near_held.at[part],
            send_sem=near_ssem.at[sem],
            recv_sem=near_rsem.at[part],
            device_id=(lax.rem(me + hop, n), tp),
            device_id_type=MESH,
        )

    def via_copy(which, source, target):
        return pltpu.make_async_remote_copy(
            src_ref=source,
            dst_ref=target,
            send_sem=via_ssem.at[which],
            recv_sem=via_rsem.at[which],
            device_id=(lax.rem(me + -2 + n, n), tp),
            device_id_type=MESH,
        )

    near_tail = pl.ds(rows - NEAR_WINDOW, NEAR_WINDOW)
    key_two = mid_copy(0, 2, mid_own.at[0], 0, 0)
    key_one = mid_copy(1, 1, mid_own.at[0], 0, 1)
    value_two = mid_copy(0, 2, mid_own.at[1], 1, 0)
    value_one = mid_copy(1, 1, mid_own.at[1], 1, 1)
    near_key = near_copy(1, near_own.at[0, near_tail], 0, 0)
    near_value = near_copy(1, near_own.at[1, near_tail], 1, 1)
    via_mid = via_copy(0, mid_own.at[1], via_held)
    onward_even = mid_copy(0, 4, via_held, 1, 3)
    onward_odd = mid_copy(1, 3, via_held, 1, 3)
    relay_key = mid_copy(0, 1, mid_held.at[1, 0], 0, 2)
    relay_value = mid_copy(0, 1, mid_held.at[1, 1], 1, 2)

    even = lax.rem(me, 2) == 0
    odd = jnp.logical_not(even)
    sends_one = me + 1 < n
    sends_two = even & (me + 2 < n)
    relays = even & (me >= 1)
    above = me + 4 - lax.rem(me, 4) < n
    crosses = (lax.rem(me, 4) >= 2) & above
    stays = jnp.logical_not(crosses)
    forwards = (lax.rem(me, 4) < 2) & above
    direct = sends_one & jnp.logical_not(crosses & odd)

    pair = moved(to_classes, project(2, 4))
    mid_own[0] = pair[:, :width]
    mid_own[1] = pair[:, width:]

    @pl.when(crosses)
    def _():
        via_mid.start()

    pair = moved(to_scattered, project(4, 6))
    second_send[...] = pair[:, :width]
    near_query[...] = pair[:, width:]
    each(lambda k: far_copy(second_send, second_held, second_sem, k).start())
    second_held[at_rows(me), :] = second_send[at_rows(me), :]
    wo_load.start()

    @pl.when(sends_two & stays)
    def _():
        key_two.start()
        value_two.start()

    @pl.when(direct)
    def _():
        key_one.start()
        value_one.start()

    pair = project(6, 8)
    near_own[0] = pair[:, :width]
    near_own[1] = pair[:, width:]

    @pl.when(direct)
    def _():
        near_key.start()
        near_value.start()

    @pl.when(crosses & even)
    def _():
        key_two.start()

    @pl.when(crosses & odd)
    def _():
        key_one.start()
        near_key.start()
        near_value.start()

    mid_query[...] = moved(to_scattered, project(8, 9))

    def slope_of(head, window):
        number = tp * local_heads + head
        slope = jnp.float32(0.0)
        for index in range(HEADS):
            value = 2.0 ** (3.0 - 8.0 * (index + 1.0) / HEADS) / window
            slope = jnp.where(number == index, jnp.float32(value), slope)
        return slope

    def grid(row_count, key_count):
        row = lax.broadcasted_iota(jnp.int32, (row_count, key_count), 0)
        column = lax.broadcasted_iota(jnp.int32, (row_count, key_count), 1)
        return row, column

    row, column = grid(rows, rows)
    apart = scatter_token(row) - column
    valid = (apart >= 0) & (apart <= NEAR_WINDOW)
    distance = apart.astype(jnp.float32)
    for head in range(local_heads):
        at = pl.ds(head * HEAD_DIM, HEAD_DIM)
        highest, weights, total = weigh(
            scores_of(near_query[:, at], near_own[0, :, at]), slope_of(head, NEAR_WINDOW), distance, valid
        )
        near_sum[head] = apply(weights, near_own[1, :, at])
        stats[2 * head] = highest
        stats[2 * head + 1] = total

    @pl.when(forwards)
    def _():
        via_mid.wait_recv()

    @pl.when(forwards & even)
    def _():
        onward_even.start()

    @pl.when(forwards & odd)
    def _():
        onward_odd.start()

    far_whole(first_send, first_held, first_sem).wait_recv()
    far_whole(second_send, second_held, second_sem).wait_recv()

    row, column = grid(rows, rows)
    apart = row - column
    valid = (apart >= 0) & (apart <= FAR_WINDOW // FAR_DILATION)
    distance = (apart * FAR_DILATION).astype(jnp.float32)
    lane = lax.broadcasted_iota(jnp.int32, (rows, HEAD_DIM), 1)
    slot = lax.broadcasted_iota(jnp.int32, (rows, HEAD_DIM), 0) & (chunk - 1)
    packed = jnp.zeros((rows, HEAD_DIM), jnp.float32)

    def far_part(head, part):
        place = head * 3 + part
        if place < 2 * local_heads:
            return first_held[:, place * HEAD_DIM : (place + 1) * HEAD_DIM]
        place -= 2 * local_heads
        return second_held[:, place * HEAD_DIM : (place + 1) * HEAD_DIM]

    for head in range(local_heads):
        highest, weights, total = weigh(
            scores_of(far_part(head, 0), far_part(head, 1)), slope_of(head, FAR_WINDOW), distance, valid
        )
        packed = jnp.where(lane == head * chunk + slot, highest + jnp.log(total), packed)
        back_send[:, head * HEAD_DIM : (head + 1) * HEAD_DIM] = apply(
            weights * (1.0 / total), far_part(head, 2)
        ).astype(jnp.bfloat16)
    log_send[...] = jnp.sum(packed.reshape(n, chunk, HEAD_DIM), axis=1, keepdims=True)

    def send_back(k):
        log_copy(k).start()
        back_copy(k).start()

    each(send_back)
    log_held[me] = log_send[me]
    back_held[at_rows(me), :] = back_send[at_rows(me), :]

    def near_rest():
        near_key.wait_recv()
        near_value.wait_recv()
        row, column = grid(rows, NEAR_WINDOW)
        apart = scatter_token(row) + NEAR_WINDOW - column
        valid = (apart >= 0) & (apart <= NEAR_WINDOW)
        distance = apart.astype(jnp.float32)
        for head in range(local_heads):
            at = pl.ds(head * HEAD_DIM, HEAD_DIM)
            high, weights, total = weigh(
                scores_of(near_query[:, at], near_held[0, :, at]), slope_of(head, NEAR_WINDOW), distance, valid
            )
            own_high = stats[2 * head]
            highest = jnp.maximum(own_high, high)
            own_share, share = jnp.exp(own_high - highest), jnp.exp(high - highest)
            near_sum[head] = near_sum[head] * own_share + apply(weights, near_held[1, :, at]) * share
            stats[2 * head] = highest
            stats[2 * head + 1] = stats[2 * head + 1] * own_share + total * share

    @pl.when(odd)
    def _():
        near_rest()

    @pl.when(me >= 1)
    def _():
        value_one.wait_recv()
        key_one.wait_recv()

    @pl.when(relays)
    def _():
        relay_value.start()
        relay_key.start()

    @pl.when(me >= 2)
    def _():
        key_two.wait_recv()
        value_two.wait_recv()

    keys = MIDDLE_WINDOW // classes + stretch
    row, column = grid(rows, keys)
    apart = (row % chunk) * members + (row // chunk) % members + MIDDLE_WINDOW // classes - column
    valid = (apart >= 0) & (apart <= MIDDLE_WINDOW // classes)
    valid = valid & (column + me * stretch >= MIDDLE_WINDOW // classes)
    distance = (apart * classes).astype(jnp.float32)

    def class_rows(part, group, at):
        of_class = pl.ds(group * stretch, stretch)
        return jnp.concatenate(
            (mid_held[0, part, of_class, at], mid_held[1, part, of_class, at], mid_own[part, of_class, at]), axis=0
        )

    for head in range(local_heads):
        at = pl.ds(head * HEAD_DIM, HEAD_DIM)
        scores = jnp.concatenate([
            scores_of(mid_query[group * stretch : (group + 1) * stretch, at], class_rows(0, group, at))
            for group in range(classes)
        ], axis=0)
        high, weights, total = weigh(scores, slope_of(head, MIDDLE_WINDOW), distance, valid)
        middle = jnp.concatenate([
            apply(weights[group * stretch : (group + 1) * stretch], class_rows(1, group, at))
            for group in range(classes)
        ], axis=0)
        near_high = stats[2 * head]
        highest = jnp.maximum(near_high, high)
        near_share, share = jnp.exp(near_high - highest), jnp.exp(high - highest)
        near_sum[head] = near_sum[head] * near_share + middle * share
        stats[2 * head] = highest
        stats[2 * head + 1] = stats[2 * head + 1] * near_share + total * share

    @pl.when(even & (me >= 1))
    def _():
        near_rest()

    def merged_copy(group):
        place = pl.ds(pl.multiple_of(group * members * chunk, members * chunk), members * chunk)
        return pltpu.make_async_remote_copy(
            src_ref=merged_own.at[place],
            dst_ref=merged_held.at[place],
            send_sem=merged_ssem.at[group],
            recv_sem=merged_rsem.at[group],
            device_id=(me, peer),
            device_id_type=MESH,
        )

    block = members * chunk
    lane = lax.broadcasted_iota(jnp.int32, (block, HEAD_DIM), 1)
    slot = lax.broadcasted_iota(jnp.int32, (block, HEAD_DIM), 0) & (chunk - 1)
    for step in range(n // members):
        group = lax.rem(plane + step, n // members)
        count = members - 1 if step == 0 else members
        log_whole(count, group).wait_recv()
        back_whole(count, group).wait_recv()
        place = pl.ds(pl.multiple_of(group * block, block), block)
        held = log_held[pl.ds(group * members, members)]
        spread = jnp.broadcast_to(held, (members, chunk, HEAD_DIM)).reshape(block, HEAD_DIM)
        split = jnp.zeros((block, HEAD_DIM), jnp.float32)
        for head in range(local_heads):
            at = pl.ds(head * HEAD_DIM, HEAD_DIM)
            far_log = jnp.sum(
                jnp.where(lane == head * chunk + slot, spread, 0.0), axis=-1, keepdims=True
            )
            pair_log, pair_sum = stats[2 * head, place], stats[2 * head + 1, place]
            highest = jnp.maximum(pair_log, far_log)
            pair_share, far_share = jnp.exp(pair_log - highest), jnp.exp(far_log - highest)
            mass = pair_sum * pair_share + far_share
            inverse = 1.0 / mass
            merged = near_sum[head, place] * (pair_share * inverse)
            merged = merged + back_held[place, at].astype(jnp.float32) * (far_share * inverse)
            merged_own[place, at] = merged.astype(jnp.bfloat16)
            rest = highest + jnp.log(mass)
            for term in range(3):
                piece = rest.astype(jnp.bfloat16).astype(jnp.float32)
                split = jnp.where(lane == 3 * head + term, piece, split)
                rest = rest - piece
        terms[place] = split.astype(jnp.bfloat16)
        merged_copy(group).start()

    lane = lax.broadcasted_iota(jnp.int32, (rows, HEAD_DIM), 1)
    totals = jnp.dot(to_tokens, terms[...], preferred_element_type=jnp.float32)
    summed = jnp.zeros((rows, HEAD_DIM), jnp.float32)
    for head in range(local_heads):
        total = jnp.sum(
            jnp.where((lane >= 3 * head) & (lane < 3 * head + 3), totals, 0.0), axis=-1, keepdims=True
        )
        summed = jnp.where(lane == head, total, summed)
    totals_ref[...] = summed
    wo_load.wait()
    partial_ref[...] = jnp.dot(
        moved(to_tokens, merged_own[...]), wo[pl.ds(pl.multiple_of(tp * width, width), width), :],
        preferred_element_type=jnp.float32,
    )

    far_whole(first_send, first_held, first_sem).wait_send()
    far_whole(second_send, second_held, second_sem).wait_send()
    log_whole(n - 1, 0).wait_send()
    back_whole(n - 1, 0).wait_send()

    @pl.when(crosses)
    def _():
        via_mid.wait_send()

    @pl.when(sends_two)
    def _():
        key_two.wait_send()

    @pl.when(sends_two & stays)
    def _():
        value_two.wait_send()

    @pl.when(sends_one)
    def _():
        key_one.wait_send()
        near_key.wait_send()
        near_value.wait_send()

    @pl.when(direct)
    def _():
        value_one.wait_send()

    @pl.when(forwards & even)
    def _():
        onward_even.wait_send()

    @pl.when(forwards & odd)
    def _():
        onward_odd.wait_send()

    @pl.when(relays)
    def _():
        relay_key.wait_send()
        relay_value.wait_send()

    for group in range(n // members):
        merged_copy(group).wait_recv()
    peer_ref[...] = moved(to_tokens, merged_held[...])
    for group in range(n // members):
        merged_copy(group).wait_send()


def mix(partial_ref, peer_ref, totals_ref, wo_ref, mixed_ref, log_ref):
    width = peer_ref.shape[1]
    at = pl.ds(pl.multiple_of((1 - lax.axis_index("tp")) * width, width), width)
    product = jnp.dot(peer_ref[...], wo_ref[at], preferred_element_type=jnp.float32)
    mixed_ref[...] = (partial_ref[...] + product).astype(jnp.bfloat16)
    log_ref[...] = jnp.transpose(totals_ref[...])[: log_ref.shape[0]]


def fused(n, tokens, query_weight, key_weight, value_weight, out_weight):
    rows, depth = tokens.shape
    columns = query_weight.shape[1]
    out_columns = out_weight.shape[1]
    local_heads = columns // (3 * HEAD_DIM)
    width = local_heads * HEAD_DIM
    planes = MIDDLE_DILATION
    dma = pltpu.SemaphoreType.DMA
    half = jnp.bfloat16
    full = jnp.float32
    whole = pl.BlockSpec(memory_space=pltpu.VMEM)
    anywhere = pl.BlockSpec(memory_space=pl.ANY)
    partial, peer, totals = pl.pallas_call(
        functools.partial(kernel, n, local_heads),
        out_shape=(
            jax.ShapeDtypeStruct((rows, out_columns), full),
            jax.ShapeDtypeStruct((rows, width), half),
            jax.ShapeDtypeStruct((rows, HEAD_DIM), full),
        ),
        in_specs=[anywhere] * 5,
        out_specs=(whole, whole, whole),
        scratch_shapes=[
            pltpu.VMEM((rows, depth), half),
            pltpu.VMEM((depth, 3 * columns), half),
            pltpu.VMEM(out_weight.shape, half),
            pltpu.VMEM((rows, 2 * width), half),
            pltpu.VMEM((rows, 2 * width), half),
            pltpu.VMEM((rows, width), half),
            pltpu.VMEM((rows, width), half),
            pltpu.VMEM((rows, width), half),
            pltpu.VMEM((rows, width), half),
            pltpu.VMEM((n, 1, HEAD_DIM), full),
            pltpu.VMEM((n, 1, HEAD_DIM), full),
            pltpu.VMEM((rows, width), half),
            pltpu.VMEM((2, rows, width), half),
            pltpu.VMEM((2, 2, rows, width), half),
            pltpu.VMEM((rows, width), half),
            pltpu.VMEM((rows, width), half),
            pltpu.VMEM((2, rows, width), half),
            pltpu.VMEM((2, NEAR_WINDOW, width), half),
            pltpu.VMEM((2 * local_heads, rows, 1), full),
            pltpu.VMEM((rows, HEAD_DIM), half),
            pltpu.VMEM((rows, width), half),
            pltpu.VMEM((rows, width), half),
            pltpu.VMEM((local_heads, rows, HEAD_DIM), full),
            dma((2 + 9 * local_heads,)),
            dma((2,)), dma((2,)), dma(()), dma((planes,)), dma(()), dma((planes,)),
            dma((4, 2)), dma((2, 2)), dma((1,)), dma((1,)), dma((2,)), dma((2,)), dma((planes,)), dma((planes,)),
        ],
        compiler_params=pltpu.CompilerParams(
            collective_id=0, has_side_effects=True, vmem_limit_bytes=53000 * 1024
        ),
    )(tokens, query_weight, key_weight, value_weight, out_weight)
    return pl.pallas_call(
        mix,
        out_shape=(
            jax.ShapeDtypeStruct((rows, out_columns), half),
            jax.ShapeDtypeStruct((local_heads, rows), full),
        ),
        in_specs=[whole] * 4,
        out_specs=(whole, whole),
        compiler_params=pltpu.CompilerParams(vmem_limit_bytes=16000 * 1024),
    )(partial, peer, totals, out_weight)


def solution(mesh):
    n, n_tp = mesh.shape["sp"], mesh.shape["tp"]
    if n == FAR_DILATION and n_tp == 2:
        body = functools.partial(fused, n)
    else:
        body = local
    return jax.shard_map(
        body,
        mesh=mesh,
        in_specs=(P("sp", None), P(None, "tp"), P(None, "tp"), P(None, "tp"), P(None, "tp")),
        out_specs=(P("sp", "tp"), P("tp", "sp")),
        check_vma=False,
    )
```

```python
import functools
import jax
import jax.numpy as jnp
from jax import lax
from jax.experimental import pallas as pl
from jax.experimental.pallas import tpu as pltpu
from jax.sharding import PartitionSpec as P

HEADS = 4
HEAD_DIM = 128
NEAR_WINDOW = 128
MIDDLE_WINDOW = 512
MIDDLE_DILATION = 4
FAR_WINDOW = 2048
FAR_DILATION = 16


def from_behind(block, axis, distance):
    devices = range(lax.axis_size(axis))
    route = [(i - distance, i) for i in devices if i - distance in devices]
    return lax.ppermute(block, axis, route)


def window_table():
    return ((NEAR_WINDOW, 1), (MIDDLE_WINDOW, MIDDLE_DILATION), (FAR_WINDOW, FAR_DILATION))


def tail_counts(row_count, distance, held_rows):
    counts = []
    for entry, available in zip(window_table(), held_rows):
        counts.append(max(0, min(available, entry[0] - (distance - 1) * row_count)))
    return counts


def pack_tails(sources, counts):
    selected = [
        source[:, source.shape[1] - amount :]
        for source, amount in zip(sources, counts)
        if amount > 0
    ]
    return jnp.concatenate(selected, axis=1)


def unpack_rows(packed, counts):
    result = []
    cursor = 0
    for amount in counts:
        result.append(packed[:, cursor : cursor + amount])
        cursor = cursor + amount
    return result


def attend_group(group_queries, buffer, window, dilation, first_key, slopes_here):
    row_count = group_queries.shape[0]
    head_count = group_queries.shape[1]
    head_size = group_queries.shape[2]
    query_split = group_queries.reshape(row_count // dilation, dilation, head_count, head_size)
    key_split = buffer[0].reshape(-1, dilation, head_count, head_size)
    value_split = buffer[1].reshape(-1, dilation, head_count, head_size)
    scores = jnp.einsum(
        "mrhe,nrhe->rhmn", query_split, key_split, preferred_element_type=jnp.float32
    ) * head_size ** (-0.5)
    grid_shape = (row_count // dilation, key_split.shape[0])
    query_slot = lax.broadcasted_iota(jnp.int32, grid_shape, 0)
    key_slot = lax.broadcasted_iota(jnp.int32, grid_shape, 1)
    spacing = query_slot + window // dilation - key_slot
    residue = lax.broadcasted_iota(jnp.int32, (dilation, 1, 1), 0)
    key_place = first_key + residue + dilation * key_slot[None]
    valid = (spacing[None] >= 0) & (spacing[None] <= window // dilation) & (key_place >= 0)
    scores = (
        scores
        - slopes_here[None, :, None, None] * (dilation * spacing).astype(jnp.float32)[None, None]
    )
    masked = jnp.where(valid[:, None], scores, -jnp.inf)
    highest = jnp.max(masked, axis=-1, keepdims=True)
    log_sum = highest + jnp.log(jnp.sum(jnp.exp(masked - highest), axis=-1, keepdims=True))
    probs = jnp.exp(masked - log_sum).astype(jnp.bfloat16)
    attended = jnp.einsum("rhmn,nrhe->mrhe", probs, value_split, preferred_element_type=jnp.float32)
    attended = attended.reshape(row_count, head_count, head_size)
    log_rows = jnp.transpose(log_sum[..., 0], (1, 2, 0)).reshape(head_count, row_count)
    return (attended, log_rows)


def local(tokens, query_weight, key_weight, value_weight, out_weight):
    rows_here = tokens.shape[0]
    local_heads = query_weight.shape[1] // (3 * HEAD_DIM)

    def project(weight_matrix):
        product = jnp.dot(tokens, weight_matrix, preferred_element_type=jnp.float32)
        return product.astype(jnp.bfloat16).reshape(rows_here, local_heads, 3, HEAD_DIM)

    queries = project(query_weight)
    keys_all = project(key_weight)
    values_all = project(value_weight)
    table = window_table()
    own = [jnp.stack((keys_all[:, :, index], values_all[:, :, index])) for index in range(3)]
    held = list(own)
    span_now = 1
    while span_now * rows_here < FAR_WINDOW + rows_here:
        counts = tail_counts(rows_here, span_now, [item.shape[1] for item in held])
        packed = pack_tails(held, counts)
        arrived = from_behind(packed, "sp", span_now)
        pieces_in = unpack_rows(arrived, counts)
        for index in range(3):
            if counts[index] > 0:
                joined = jnp.concatenate((pieces_in[index], held[index]), axis=1)
                held[index] = joined
        span_now = span_now * 2
    priors = [held[index][:, : table[index][0]] for index in range(3)]
    position_start = lax.axis_index("sp") * rows_here
    head_ids = (
        lax.axis_index("tp") * local_heads + jnp.arange(local_heads, dtype=jnp.int32)
    ).astype(jnp.float32)
    outputs = []
    logs = []
    for index, (window, dilation) in enumerate(table):
        buffer = jnp.concatenate((priors[index], own[index]), axis=1)
        slopes_here = 2.0 ** (3.0 - 8.0 * (head_ids + 1.0) / HEADS) / window
        attended, log_rows = attend_group(
            queries[:, :, index], buffer, window, dilation, position_start - window, slopes_here
        )
        outputs.append(attended)
        logs.append(log_rows)
    stacked_logs = jnp.stack(logs)
    highest = jnp.max(stacked_logs, axis=0)
    total_log = highest + jnp.log(jnp.sum(jnp.exp(stacked_logs - highest), axis=0))
    mixing = jnp.exp(stacked_logs - total_log)
    merged = outputs[0] * jnp.transpose(mixing[0])[:, :, None]
    merged = merged + outputs[1] * jnp.transpose(mixing[1])[:, :, None]
    merged = merged + outputs[2] * jnp.transpose(mixing[2])[:, :, None]
    merged = merged.astype(jnp.bfloat16).reshape(rows_here, local_heads * HEAD_DIM)
    mixed = jnp.dot(
        lax.all_gather(merged, "tp", axis=1, tiled=True),
        out_weight,
        preferred_element_type=jnp.float32,
    ).astype(jnp.bfloat16)
    return (mixed, total_log)


MESH = pl.DeviceIdType.MESH
MASKED = -1e30


def scores_of(query, key):
    return lax.dot_general(
        query, key, (((1,), (1,)), ((), ())), preferred_element_type=jnp.float32
    ) * HEAD_DIM ** (-0.5)


def weigh(scores, slope, distance, valid):
    scores = jnp.where(valid, scores - slope * distance, MASKED)
    highest = jnp.max(scores, axis=-1, keepdims=True)
    weights = jnp.exp(scores - highest)
    return highest, weights, jnp.sum(weights, axis=-1, keepdims=True)


def apply(weights, value):
    return jnp.dot(weights.astype(jnp.bfloat16), value, preferred_element_type=jnp.float32)


def split_by(value, size):
    shift = size.bit_length() - 1
    return value >> shift, value & (size - 1)


def grid(row_count, key_count):
    row = lax.broadcasted_iota(jnp.int32, (row_count, 1), 0)
    column = lax.broadcasted_iota(jnp.int32, (row_count, key_count), 1)
    return row, column


def one_hot(rows, token_of_row):
    row, column = grid(rows, rows)
    return jnp.where(column == token_of_row(row), 1.0, 0.0).astype(jnp.bfloat16)


def kernel(
    n, local_heads,
    tok_hbm, wq_hbm, wk_hbm, wv_hbm, wo_hbm,
    partial_ref, peer_ref, totals_ref,
    tok, weight, wo, first_send, first_held, second_send, second_held, back_send, back_held, log_send, log_held,
    mid_query, mid_own, mid_held, via_held, near_query, near_own, near_held,
    stats, merged_own, merged_held, near_sum,
    load_sem, half_sem, first_sem, second_sem, back_ssem, back_rsem, log_ssem, log_rsem,
    mid_ssem, mid_rsem, via_ssem, via_rsem, near_ssem, near_rsem, merged_ssem, merged_rsem,
):
    me = lax.axis_index("sp")
    tp = lax.axis_index("tp")
    rows = tok.shape[0]
    width = local_heads * HEAD_DIM
    chunk = rows // n
    classes = MIDDLE_DILATION
    members = n // classes
    stretch = rows // classes
    peer = 1 - tp
    sources = (wq_hbm, wk_hbm, wv_hbm)

    depth = tok.shape[1]
    halves = (pl.ds(0, depth // 2), pl.ds(depth // 2, depth // 2))
    tok_loads = [
        pltpu.make_async_copy(tok_hbm.at[:, part], tok.at[:, part], half_sem.at[side, 0])
        for side, part in enumerate(halves)
    ]
    wo_load = pltpu.make_async_copy(wo_hbm, wo, load_sem.at[0])
    loads = []
    order = [(2, part, head) for head in range(local_heads) for part in range(3)]
    for group, part in ((0, 0), (0, 1), (0, 2), (1, 0)):
        order += [(group, part, head) for head in range(local_heads)]
    middle = [(1, part, head) for part in (1, 2) for head in range(local_heads)]
    order[2 * local_heads : 2 * local_heads] = middle
    first = 2 * local_heads
    early = 4 * local_heads
    for place, (group, part, head) in enumerate(order):
        source = sources[part].at[:, pl.ds((head * 3 + group) * HEAD_DIM, HEAD_DIM)]
        target = weight.at[:, pl.ds(place * HEAD_DIM, HEAD_DIM)]
        if place < first:
            loads.append([
                pltpu.make_async_copy(source.at[side], target.at[side], half_sem.at[index, 1 + place])
                for index, side in enumerate(halves)
            ])
        else:
            loads.append(pltpu.make_async_copy(source, target, load_sem.at[1 + place]))
    for side in range(2):
        tok_loads[side].start()
        for copy in loads[:first]:
            copy[side].start()

    barrier = pltpu.get_barrier_semaphore()

    def greet(k, carry):
        pl.semaphore_signal(barrier, inc=1, device_id=(lax.rem(me + k, n), tp), device_id_type=MESH)
        return carry

    lax.fori_loop(1, n, greet, 0)
    pl.semaphore_signal(barrier, inc=1, device_id=(me, peer), device_id_type=MESH)
    for copy in loads[first:early]:
        copy.start()

    @pl.when(me < 2)
    def _():
        mid_held[0] = jnp.zeros((2, rows, width), jnp.bfloat16)

    @pl.when(me < 1)
    def _():
        mid_held[1] = jnp.zeros((2, rows, width), jnp.bfloat16)

    def project(first, last):
        for copy in loads[first * local_heads : last * local_heads]:
            copy.wait()
        return jnp.dot(
            tok[...], weight[:, first * width : last * width], preferred_element_type=jnp.float32
        ).astype(jnp.bfloat16)

    def at_rows(index):
        return pl.ds(pl.multiple_of(index * chunk, chunk), chunk)

    def scatter_token(row):
        group, index = split_by(row, chunk)
        high, low = split_by(group, members)
        return index * n + low * classes + high

    def gather_row(token):
        index, residue = split_by(token, n)
        high, low = split_by(residue, classes)
        return (low * members + high) * chunk + index

    def class_token(row):
        group, index = split_by(row, stretch)
        return index * classes + group

    to_scattered = one_hot(rows, scatter_token)
    to_tokens = one_hot(rows, gather_row)
    to_classes = one_hot(rows, class_token)

    def moved(matrix, block):
        return jnp.dot(matrix, block, preferred_element_type=jnp.float32).astype(jnp.bfloat16)

    def each(action):
        for k in range(1, n):
            action(k)

    upper = me // (n // 2)

    def target_of(k):
        rising = k - 1 + jnp.where(k - 1 >= me, 1, 0)
        falling = n - k - jnp.where(n - k <= me, 1, 0)
        return jnp.where(upper == 1, rising, falling)


    def far_copy(source, target, sem, k):
        to = target_of(k)
        return pltpu.make_async_remote_copy(
            src_ref=source.at[at_rows(to)],
            dst_ref=target.at[at_rows(me)],
            send_sem=sem.at[0],
            recv_sem=sem.at[1],
            device_id=(to, tp),
            device_id_type=MESH,
        )

    def far_whole(source, target, sem):
        others = pl.ds(0, rows - chunk)
        return pltpu.make_async_remote_copy(
            src_ref=source.at[others],
            dst_ref=target.at[others],
            send_sem=sem.at[0],
            recv_sem=sem.at[1],
            device_id=(lax.rem(me + 1, n), tp),
            device_id_type=MESH,
        )

    def back_copy(head, k):
        to = target_of(k)
        return pltpu.make_async_remote_copy(
            src_ref=back_send.at[head, at_rows(to)],
            dst_ref=back_held.at[head, at_rows(me)],
            send_sem=back_ssem.at[head],
            recv_sem=back_rsem.at[head],
            device_id=(to, tp),
            device_id_type=MESH,
        )

    def back_whole(head):
        others = pl.ds(0, rows - chunk)
        return pltpu.make_async_remote_copy(
            src_ref=back_send.at[head, others],
            dst_ref=back_held.at[head, others],
            send_sem=back_ssem.at[head],
            recv_sem=back_rsem.at[head],
            device_id=(lax.rem(me + 1, n), tp),
            device_id_type=MESH,
        )

    def log_copy(head, k):
        to = target_of(k)
        return pltpu.make_async_remote_copy(
            src_ref=log_send.at[head, to],
            dst_ref=log_held.at[head, me],
            send_sem=log_ssem.at[head],
            recv_sem=log_rsem.at[head],
            device_id=(to, tp),
            device_id_type=MESH,
        )

    def log_whole(head):
        others = pl.ds(0, n - 1)
        return pltpu.make_async_remote_copy(
            src_ref=log_send.at[head, others],
            dst_ref=log_held.at[head, others],
            send_sem=log_ssem.at[head],
            recv_sem=log_rsem.at[head],
            device_id=(lax.rem(me + 1, n), tp),
            device_id_type=MESH,
        )

    product = None
    for side, part in enumerate(halves):
        tok_loads[side].wait()
        for copy in loads[:first]:
            copy[side].wait()
        term = jnp.dot(tok[:, part], weight[part, : 2 * width], preferred_element_type=jnp.float32)
        product = term if product is None else product + term
    first_send[...] = moved(to_scattered, product.astype(jnp.bfloat16))
    for copy in loads[early:]:
        copy.start()
    pl.semaphore_wait(barrier, n)
    each(lambda k: far_copy(first_send, first_held, first_sem, k).start())
    first_held[at_rows(me), :] = first_send[at_rows(me), :]

    def mid_copy(slot, hop, source, part, sem):
        return pltpu.make_async_remote_copy(
            src_ref=source,
            dst_ref=mid_held.at[slot, part],
            send_sem=mid_ssem.at[sem, part],
            recv_sem=mid_rsem.at[slot, part],
            device_id=(lax.rem(me + hop + n, n), tp),
            device_id_type=MESH,
        )

    def near_copy(hop, source, part, sem):
        return pltpu.make_async_remote_copy(
            src_ref=source,
            dst_ref=near_held.at[part],
            send_sem=near_ssem.at[sem],
            recv_sem=near_rsem.at[part],
            device_id=(lax.rem(me + hop, n), tp),
            device_id_type=MESH,
        )

    def via_copy(which, source, target):
        return pltpu.make_async_remote_copy(
            src_ref=source,
            dst_ref=target,
            send_sem=via_ssem.at[which],
            recv_sem=via_rsem.at[which],
            device_id=(lax.rem(me + -2 + n, n), tp),
            device_id_type=MESH,
        )

    near_tail = pl.ds(rows - NEAR_WINDOW, NEAR_WINDOW)
    key_two = mid_copy(0, 2, mid_own.at[0], 0, 0)
    key_one = mid_copy(1, 1, mid_own.at[0], 0, 1)
    value_two = mid_copy(0, 2, mid_own.at[1], 1, 0)
    value_one = mid_copy(1, 1, mid_own.at[1], 1, 1)
    near_key = near_copy(1, near_own.at[0, near_tail], 0, 0)
    near_value = near_copy(1, near_own.at[1, near_tail], 1, 1)
    via_mid = via_copy(0, mid_own.at[1], via_held)
    onward_even = mid_copy(0, 4, via_held, 1, 3)
    onward_odd = mid_copy(1, 3, via_held, 1, 3)
    relay_key = mid_copy(0, 1, mid_held.at[1, 0], 0, 2)
    relay_value = mid_copy(0, 1, mid_held.at[1, 1], 1, 2)

    even = lax.rem(me, 2) == 0
    odd = jnp.logical_not(even)
    sends_one = me + 1 < n
    sends_two = even & (me + 2 < n)
    relays = even & (me >= 1)
    above = me + 4 - lax.rem(me, 4) < n
    crosses = (lax.rem(me, 4) >= 2) & above
    stays = jnp.logical_not(crosses)
    forwards = (lax.rem(me, 4) < 2) & above
    direct = sends_one & jnp.logical_not(crosses & odd)

    pair = moved(to_classes, project(2, 4))
    mid_own[0] = pair[:, :width]
    mid_own[1] = pair[:, width:]

    @pl.when(crosses)
    def _():
        via_mid.start()

    pair = moved(to_scattered, project(4, 6))
    second_send[...] = pair[:, :width]
    near_query[...] = pair[:, width:]
    each(lambda k: far_copy(second_send, second_held, second_sem, k).start())
    second_held[at_rows(me), :] = second_send[at_rows(me), :]
    wo_load.start()

    @pl.when(sends_two & stays)
    def _():
        value_two.start()
        key_two.start()

    @pl.when(direct)
    def _():
        value_one.start()
        key_one.start()

    @pl.when(crosses & even)
    def _():
        key_two.start()

    @pl.when(crosses & odd)
    def _():
        key_one.start()

    pair = project(6, 8)
    near_own[0] = pair[:, :width]
    near_own[1] = pair[:, width:]

    @pl.when(sends_one)
    def _():
        near_key.start()
        near_value.start()

    mid_query[...] = moved(to_scattered, project(8, 9))

    def slope_of(head, window):
        number = tp * local_heads + head
        slope = jnp.float32(0.0)
        for index in range(HEADS):
            value = 2.0 ** (3.0 - 8.0 * (index + 1.0) / HEADS) / window
            slope = jnp.where(number == index, jnp.float32(value), slope)
        return slope

    row, column = grid(rows, rows)
    apart = scatter_token(row) - column
    valid = (apart >= 0) & (apart <= NEAR_WINDOW)
    distance = apart.astype(jnp.float32)
    heads = [pl.ds(head * HEAD_DIM, HEAD_DIM) for head in range(local_heads)]

    def join(parts):
        held = [(stats[2 * head], stats[2 * head + 1], near_sum[head]) for head in range(local_heads)]
        joined = []
        for (high, total, part), (held_high, held_total, held_part) in zip(parts, held):
            highest = jnp.maximum(held_high, high)
            held_share, share = jnp.exp(held_high - highest), jnp.exp(high - highest)
            joined.append((
                highest, held_total * held_share + total * share, held_part * held_share + part * share
            ))
        keep(joined)

    def keep(parts):
        for head, (high, total, part) in enumerate(parts):
            stats[2 * head] = high
            stats[2 * head + 1] = total
            near_sum[head] = part

    def partial_of(query, key_value, slopes, distance, valid):
        weighed = [
            weigh(scores_of(query[:, at], key_value[0, :, at]), slope, distance, valid)
            for at, slope in zip(heads, slopes)
        ]
        return [
            (high, total, apply(weights, key_value[1, :, at]))
            for at, (high, weights, total) in zip(heads, weighed)
        ]

    near_slopes = [slope_of(head, NEAR_WINDOW) for head in range(local_heads)]
    keep(partial_of(near_query, near_own, near_slopes, distance, valid))

    def near_rest():
        near_key.wait_recv()
        near_value.wait_recv()
        row, column = grid(rows, NEAR_WINDOW)
        apart = scatter_token(row) + NEAR_WINDOW - column
        valid = (apart >= 0) & (apart <= NEAR_WINDOW)
        distance = apart.astype(jnp.float32)
        join(partial_of(near_query, near_held, near_slopes, distance, valid))

    @pl.when(odd)
    def _():
        near_rest()

    @pl.when(forwards)
    def _():
        via_mid.wait_recv()

    @pl.when(forwards & even)
    def _():
        onward_even.start()

    @pl.when(forwards & odd)
    def _():
        onward_odd.start()

    far_whole(first_send, first_held, first_sem).wait_recv()

    reach = FAR_WINDOW // FAR_DILATION
    lane = lax.broadcasted_iota(jnp.int32, (rows, HEAD_DIM), 1)
    slot = lax.broadcasted_iota(jnp.int32, (rows, HEAD_DIM), 0) & (chunk - 1)
    of_slot = lane == slot

    def far_part(head, part, first_row, last_row):
        place = head * 3 + part
        source = first_held
        if place >= 2 * local_heads:
            place -= 2 * local_heads
            source = second_held
        return source[first_row:last_row, place * HEAD_DIM : (place + 1) * HEAD_DIM]

    for head in range(local_heads):
        if head == local_heads - 1:
            far_whole(second_send, second_held, second_sem).wait_recv()
        logs = []
        shares = []
        for first_row, last_row in ((0, reach), (reach, rows)):
            row, column = grid(last_row - first_row, last_row)
            apart = row + first_row - column
            highest, weights, total = weigh(
                scores_of(far_part(head, 0, first_row, last_row), far_part(head, 1, 0, last_row)),
                slope_of(head, FAR_WINDOW), (apart * FAR_DILATION).astype(jnp.float32),
                (apart >= 0) & (apart <= reach),
            )
            logs.append(highest + jnp.log(total))
            shares.append(weights * (1.0 / total))
        packed = jnp.where(of_slot, jnp.concatenate(logs, axis=0), 0.0)
        log_send[head] = jnp.sum(packed.reshape(n, chunk, HEAD_DIM), axis=1, keepdims=True)
        for (first_row, last_row), share in zip(((0, reach), (reach, rows)), shares):
            back_send[head, first_row:last_row] = apply(
                share, far_part(head, 2, 0, last_row)
            ).astype(jnp.bfloat16)

        def send_back(k):
            log_copy(head, k).start()
            back_copy(head, k).start()

        each(send_back)
        log_held[head, me] = log_send[head, me]
        back_held[head, at_rows(me), :] = back_send[head, at_rows(me), :]

    @pl.when(me >= 1)
    def _():
        value_one.wait_recv()
        key_one.wait_recv()

    @pl.when(relays)
    def _():
        relay_value.start()
        relay_key.start()

    @pl.when(me >= 2)
    def _():
        key_two.wait_recv()
        value_two.wait_recv()

    keys = MIDDLE_WINDOW // classes + stretch
    row, column = grid(rows, keys)
    group, index = split_by(row, chunk)
    apart = index * members + split_by(group, members)[1] + MIDDLE_WINDOW // classes - column
    valid = (apart >= 0) & (apart <= MIDDLE_WINDOW // classes)
    valid = valid & (column + me * stretch >= MIDDLE_WINDOW // classes)
    distance = (apart * classes).astype(jnp.float32)

    def class_rows(part, group, at):
        of_class = pl.ds(group * stretch, stretch)
        return jnp.concatenate(
            (mid_held[0, part, of_class, at], mid_held[1, part, of_class, at], mid_own[part, of_class, at]), axis=0
        )

    weighed = []
    for head, at in enumerate(heads):
        scores = jnp.concatenate([
            scores_of(mid_query[group * stretch : (group + 1) * stretch, at], class_rows(0, group, at))
            for group in range(classes)
        ], axis=0)
        weighed.append(weigh(scores, slope_of(head, MIDDLE_WINDOW), distance, valid))
    join([
        (high, total, jnp.concatenate([
            apply(weights[group * stretch : (group + 1) * stretch], class_rows(1, group, at))
            for group in range(classes)
        ], axis=0))
        for at, (high, weights, total) in zip(heads, weighed)
    ])

    @pl.when(even & (me >= 1))
    def _():
        near_rest()

    def merged_copy(head):
        return pltpu.make_async_remote_copy(
            src_ref=merged_own.at[head],
            dst_ref=merged_held.at[head],
            send_sem=merged_ssem.at[head],
            recv_sem=merged_rsem.at[head],
            device_id=(me, peer),
            device_id_type=MESH,
        )

    split = jnp.zeros((rows, HEAD_DIM), jnp.float32)
    for head in range(local_heads):
        log_whole(head).wait_recv()
        spread = jnp.broadcast_to(log_held[head], (n, chunk, HEAD_DIM)).reshape(rows, HEAD_DIM)
        far_log = jnp.sum(jnp.where(of_slot, spread, 0.0), axis=-1, keepdims=True)
        pair_log, pair_sum = stats[2 * head], stats[2 * head + 1]
        highest = jnp.maximum(pair_log, far_log)
        pair_share, far_share = jnp.exp(pair_log - highest), jnp.exp(far_log - highest)
        mass = pair_sum * pair_share + far_share
        inverse = 1.0 / mass
        back_whole(head).wait_recv()
        merged = near_sum[head] * (pair_share * inverse)
        merged = merged + back_held[head].astype(jnp.float32) * (far_share * inverse)
        merged_own[head] = merged.astype(jnp.bfloat16)
        merged_copy(head).start()
        rest = highest + jnp.log(mass)
        for term in range(3):
            piece = rest.astype(jnp.bfloat16).astype(jnp.float32)
            split = jnp.where(lane == 3 * head + term, piece, split)
            rest = rest - piece

    totals = jnp.dot(to_tokens, split.astype(jnp.bfloat16), preferred_element_type=jnp.float32)
    summed = jnp.zeros((rows, HEAD_DIM), jnp.float32)
    for head in range(local_heads):
        total = jnp.sum(
            jnp.where((lane >= 3 * head) & (lane < 3 * head + 3), totals, 0.0), axis=-1, keepdims=True
        )
        summed = jnp.where(lane == head, total, summed)
    totals_ref[...] = summed
    wo_load.wait()
    partial_ref[...] = jnp.dot(
        moved(to_tokens, jnp.concatenate([merged_own[head] for head in range(local_heads)], axis=1)), wo[pl.ds(pl.multiple_of(tp * width, width), width), :],
        preferred_element_type=jnp.float32,
    )

    far_whole(first_send, first_held, first_sem).wait_send()
    far_whole(second_send, second_held, second_sem).wait_send()
    for head in range(local_heads):
        log_whole(head).wait_send()
        back_whole(head).wait_send()

    @pl.when(crosses)
    def _():
        via_mid.wait_send()

    @pl.when(sends_two)
    def _():
        key_two.wait_send()

    @pl.when(sends_two & stays)
    def _():
        value_two.wait_send()

    @pl.when(sends_one)
    def _():
        key_one.wait_send()
        near_key.wait_send()
        near_value.wait_send()

    @pl.when(direct)
    def _():
        value_one.wait_send()

    @pl.when(forwards & even)
    def _():
        onward_even.wait_send()

    @pl.when(forwards & odd)
    def _():
        onward_odd.wait_send()

    @pl.when(relays)
    def _():
        relay_key.wait_send()
        relay_value.wait_send()

    for head in range(local_heads):
        merged_copy(head).wait_recv()
    peer_ref[...] = moved(to_tokens, jnp.concatenate([merged_held[head] for head in range(local_heads)], axis=1))
    for head in range(local_heads):
        merged_copy(head).wait_send()


def mix(partial_ref, peer_ref, totals_ref, wo_ref, mixed_ref, log_ref):
    width = peer_ref.shape[1]
    at = pl.ds(pl.multiple_of((1 - lax.axis_index("tp")) * width, width), width)
    product = jnp.dot(peer_ref[...], wo_ref[at], preferred_element_type=jnp.float32)
    mixed_ref[...] = (partial_ref[...] + product).astype(jnp.bfloat16)
    log_ref[...] = jnp.transpose(totals_ref[...])[: log_ref.shape[0]]


def fused(n, tokens, query_weight, key_weight, value_weight, out_weight):
    rows, depth = tokens.shape
    columns = query_weight.shape[1]
    out_columns = out_weight.shape[1]
    local_heads = columns // (3 * HEAD_DIM)
    width = local_heads * HEAD_DIM
    dma = pltpu.SemaphoreType.DMA
    half = jnp.bfloat16
    full = jnp.float32
    whole = pl.BlockSpec(memory_space=pltpu.VMEM)
    anywhere = pl.BlockSpec(memory_space=pl.ANY)
    partial, peer, totals = pl.pallas_call(
        functools.partial(kernel, n, local_heads),
        out_shape=(
            jax.ShapeDtypeStruct((rows, out_columns), full),
            jax.ShapeDtypeStruct((rows, width), half),
            jax.ShapeDtypeStruct((rows, HEAD_DIM), full),
        ),
        in_specs=[anywhere] * 5,
        out_specs=(whole, whole, whole),
        scratch_shapes=[
            pltpu.VMEM((rows, depth), half),
            pltpu.VMEM((depth, 3 * columns), half),
            pltpu.VMEM(out_weight.shape, half),
            pltpu.VMEM((rows, 2 * width), half),
            pltpu.VMEM((rows, 2 * width), half),
            pltpu.VMEM((rows, width), half),
            pltpu.VMEM((rows, width), half),
            pltpu.VMEM((local_heads, rows, HEAD_DIM), half),
            pltpu.VMEM((local_heads, rows, HEAD_DIM), half),
            pltpu.VMEM((local_heads, n, 1, HEAD_DIM), full),
            pltpu.VMEM((local_heads, n, 1, HEAD_DIM), full),
            pltpu.VMEM((rows, width), half),
            pltpu.VMEM((2, rows, width), half),
            pltpu.VMEM((2, 2, rows, width), half),
            pltpu.VMEM((rows, width), half),
            pltpu.VMEM((rows, width), half),
            pltpu.VMEM((2, rows, width), half),
            pltpu.VMEM((2, NEAR_WINDOW, width), half),
            pltpu.VMEM((2 * local_heads, rows, 1), full),
            pltpu.VMEM((local_heads, rows, HEAD_DIM), half),
            pltpu.VMEM((local_heads, rows, HEAD_DIM), half),
            pltpu.VMEM((local_heads, rows, HEAD_DIM), full),
            dma((1 + 9 * local_heads,)), dma((2, 1 + 2 * local_heads)), dma((2,)), dma((2,)),
            dma((local_heads,)), dma((local_heads,)), dma((local_heads,)), dma((local_heads,)),
            dma((4, 2)), dma((2, 2)), dma((1,)), dma((1,)), dma((2,)), dma((2,)), dma((local_heads,)), dma((local_heads,)),
        ],
        compiler_params=pltpu.CompilerParams(
            collective_id=0, has_side_effects=True, vmem_limit_bytes=53000 * 1024
        ),
    )(tokens, query_weight, key_weight, value_weight, out_weight)
    return pl.pallas_call(
        mix,
        out_shape=(
            jax.ShapeDtypeStruct((rows, out_columns), half),
            jax.ShapeDtypeStruct((local_heads, rows), full),
        ),
        in_specs=[whole] * 4,
        out_specs=(whole, whole),
        compiler_params=pltpu.CompilerParams(vmem_limit_bytes=16000 * 1024),
    )(partial, peer, totals, out_weight)


def solution(mesh):
    n, n_tp = mesh.shape["sp"], mesh.shape["tp"]
    if n == FAR_DILATION and n_tp == 2:
        body = functools.partial(fused, n)
    else:
        body = local
    return jax.shard_map(
        body,
        mesh=mesh,
        in_specs=(P("sp", None), P(None, "tp"), P(None, "tp"), P(None, "tp"), P(None, "tp")),
        out_specs=(P("sp", "tp"), P("tp", "sp")),
        check_vma=False,
    )
```

```python
import functools
import jax
import jax.numpy as jnp
from jax import lax
from jax.experimental import pallas as pl
from jax.experimental.pallas import tpu as pltpu
from jax.sharding import PartitionSpec as P

HEADS = 4
HEAD_DIM = 128
NEAR_WINDOW = 128
MIDDLE_WINDOW = 512
MIDDLE_DILATION = 4
FAR_WINDOW = 2048
FAR_DILATION = 16


def from_behind(block, axis, distance):
    devices = range(lax.axis_size(axis))
    route = [(i - distance, i) for i in devices if i - distance in devices]
    return lax.ppermute(block, axis, route)


def window_table():
    return ((NEAR_WINDOW, 1), (MIDDLE_WINDOW, MIDDLE_DILATION), (FAR_WINDOW, FAR_DILATION))


def tail_counts(row_count, distance, held_rows):
    counts = []
    for entry, available in zip(window_table(), held_rows):
        counts.append(max(0, min(available, entry[0] - (distance - 1) * row_count)))
    return counts


def pack_tails(sources, counts):
    selected = [
        source[:, source.shape[1] - amount :]
        for source, amount in zip(sources, counts)
        if amount > 0
    ]
    return jnp.concatenate(selected, axis=1)


def unpack_rows(packed, counts):
    result = []
    cursor = 0
    for amount in counts:
        result.append(packed[:, cursor : cursor + amount])
        cursor = cursor + amount
    return result


def attend_group(group_queries, buffer, window, dilation, first_key, slopes_here):
    row_count = group_queries.shape[0]
    head_count = group_queries.shape[1]
    head_size = group_queries.shape[2]
    query_split = group_queries.reshape(row_count // dilation, dilation, head_count, head_size)
    key_split = buffer[0].reshape(-1, dilation, head_count, head_size)
    value_split = buffer[1].reshape(-1, dilation, head_count, head_size)
    scores = jnp.einsum(
        "mrhe,nrhe->rhmn", query_split, key_split, preferred_element_type=jnp.float32
    ) * head_size ** (-0.5)
    grid_shape = (row_count // dilation, key_split.shape[0])
    query_slot = lax.broadcasted_iota(jnp.int32, grid_shape, 0)
    key_slot = lax.broadcasted_iota(jnp.int32, grid_shape, 1)
    spacing = query_slot + window // dilation - key_slot
    residue = lax.broadcasted_iota(jnp.int32, (dilation, 1, 1), 0)
    key_place = first_key + residue + dilation * key_slot[None]
    valid = (spacing[None] >= 0) & (spacing[None] <= window // dilation) & (key_place >= 0)
    scores = (
        scores
        - slopes_here[None, :, None, None] * (dilation * spacing).astype(jnp.float32)[None, None]
    )
    masked = jnp.where(valid[:, None], scores, -jnp.inf)
    highest = jnp.max(masked, axis=-1, keepdims=True)
    log_sum = highest + jnp.log(jnp.sum(jnp.exp(masked - highest), axis=-1, keepdims=True))
    probs = jnp.exp(masked - log_sum).astype(jnp.bfloat16)
    attended = jnp.einsum("rhmn,nrhe->mrhe", probs, value_split, preferred_element_type=jnp.float32)
    attended = attended.reshape(row_count, head_count, head_size)
    log_rows = jnp.transpose(log_sum[..., 0], (1, 2, 0)).reshape(head_count, row_count)
    return (attended, log_rows)


def local(tokens, query_weight, key_weight, value_weight, out_weight):
    rows_here = tokens.shape[0]
    local_heads = query_weight.shape[1] // (3 * HEAD_DIM)

    def project(weight_matrix):
        product = jnp.dot(tokens, weight_matrix, preferred_element_type=jnp.float32)
        return product.astype(jnp.bfloat16).reshape(rows_here, local_heads, 3, HEAD_DIM)

    queries = project(query_weight)
    keys_all = project(key_weight)
    values_all = project(value_weight)
    table = window_table()
    own = [jnp.stack((keys_all[:, :, index], values_all[:, :, index])) for index in range(3)]
    held = list(own)
    span_now = 1
    while span_now * rows_here < FAR_WINDOW + rows_here:
        counts = tail_counts(rows_here, span_now, [item.shape[1] for item in held])
        packed = pack_tails(held, counts)
        arrived = from_behind(packed, "sp", span_now)
        pieces_in = unpack_rows(arrived, counts)
        for index in range(3):
            if counts[index] > 0:
                joined = jnp.concatenate((pieces_in[index], held[index]), axis=1)
                held[index] = joined
        span_now = span_now * 2
    priors = [held[index][:, : table[index][0]] for index in range(3)]
    position_start = lax.axis_index("sp") * rows_here
    head_ids = (
        lax.axis_index("tp") * local_heads + jnp.arange(local_heads, dtype=jnp.int32)
    ).astype(jnp.float32)
    outputs = []
    logs = []
    for index, (window, dilation) in enumerate(table):
        buffer = jnp.concatenate((priors[index], own[index]), axis=1)
        slopes_here = 2.0 ** (3.0 - 8.0 * (head_ids + 1.0) / HEADS) / window
        attended, log_rows = attend_group(
            queries[:, :, index], buffer, window, dilation, position_start - window, slopes_here
        )
        outputs.append(attended)
        logs.append(log_rows)
    stacked_logs = jnp.stack(logs)
    highest = jnp.max(stacked_logs, axis=0)
    total_log = highest + jnp.log(jnp.sum(jnp.exp(stacked_logs - highest), axis=0))
    mixing = jnp.exp(stacked_logs - total_log)
    merged = outputs[0] * jnp.transpose(mixing[0])[:, :, None]
    merged = merged + outputs[1] * jnp.transpose(mixing[1])[:, :, None]
    merged = merged + outputs[2] * jnp.transpose(mixing[2])[:, :, None]
    merged = merged.astype(jnp.bfloat16).reshape(rows_here, local_heads * HEAD_DIM)
    mixed = jnp.dot(
        lax.all_gather(merged, "tp", axis=1, tiled=True),
        out_weight,
        preferred_element_type=jnp.float32,
    ).astype(jnp.bfloat16)
    return (mixed, total_log)


MESH = pl.DeviceIdType.MESH
MASKED = -1e30


def scores_of(query, key):
    return lax.dot_general(
        query, key, (((1,), (1,)), ((), ())), preferred_element_type=jnp.float32
    ) * HEAD_DIM ** (-0.5)


def weigh(scores, slope, distance, valid):
    scores = jnp.where(valid, scores - slope * distance, MASKED)
    highest = jnp.max(scores, axis=-1, keepdims=True)
    weights = jnp.exp(scores - highest)
    return highest, weights, jnp.sum(weights, axis=-1, keepdims=True)


def apply(weights, value):
    return jnp.dot(weights.astype(jnp.bfloat16), value, preferred_element_type=jnp.float32)


def split_by(value, size):
    shift = size.bit_length() - 1
    return value >> shift, value & (size - 1)


def grid(row_count, key_count):
    row = lax.broadcasted_iota(jnp.int32, (row_count, 1), 0)
    column = lax.broadcasted_iota(jnp.int32, (row_count, key_count), 1)
    return row, column


def one_hot(rows, token_of_row):
    row, column = grid(rows, rows)
    return jnp.where(column == token_of_row(row), 1.0, 0.0).astype(jnp.bfloat16)


def kernel(
    n, local_heads,
    tok_hbm, wq_hbm, wk_hbm, wv_hbm, wo_hbm,
    partial_ref, peer_ref, totals_ref,
    tok, scattered, product, weight, wo, first_send, first_held, second_send, second_held, back_send, back_held, log_send, log_held, probs,
    mid_query, mid_own, mid_held, via_held, near_query, near_low, near_own, near_held,
    stats, terms, merged_own, merged_held, near_sum,
    load_sem, half_sem, first_sem, second_sem, back_ssem, back_rsem, log_ssem, log_rsem,
    mid_ssem, mid_rsem, via_ssem, via_rsem, near_ssem, near_rsem, merged_ssem, merged_rsem,
):
    me = lax.axis_index("sp")
    tp = lax.axis_index("tp")
    rows = tok.shape[0]
    width = local_heads * HEAD_DIM
    chunk = rows // n
    classes = MIDDLE_DILATION
    members = n // classes
    stretch = rows // classes
    part_rows = chunk // 2
    low_rows = rows // 2
    peer = 1 - tp
    sources = (wq_hbm, wk_hbm, wv_hbm)

    depth = tok.shape[1]
    halves = (pl.ds(0, depth // 2), pl.ds(depth // 2, depth // 2))
    tok_loads = [
        pltpu.make_async_copy(tok_hbm.at[:, part], tok.at[:, part], half_sem.at[side, 0])
        for side, part in enumerate(halves)
    ]
    wo_load = pltpu.make_async_copy(wo_hbm, wo, load_sem.at[0])
    loads = []
    order = [(2, part, head) for head in range(local_heads) for part in (0, 1)]
    for group, part in ((1, 1), (1, 2), (2, 2), (0, 0), (0, 1), (0, 2), (1, 0)):
        order += [(group, part, head) for head in range(local_heads)]
    first = 2 * local_heads
    early = 4 * local_heads
    for place, (group, part, head) in enumerate(order):
        source = sources[part].at[:, pl.ds((head * 3 + group) * HEAD_DIM, HEAD_DIM)]
        target = weight.at[:, pl.ds(place * HEAD_DIM, HEAD_DIM)]
        if place < first:
            loads.append([
                pltpu.make_async_copy(source.at[side], target.at[side], half_sem.at[index, 1 + place])
                for index, side in enumerate(halves)
            ])
        else:
            loads.append(pltpu.make_async_copy(source, target, load_sem.at[1 + place]))
    for copy in tok_loads:
        copy.start()
    for side in range(2):
        for copy in loads[:first]:
            copy[side].start()

    barrier = pltpu.get_barrier_semaphore()

    def greet(k, carry):
        pl.semaphore_signal(barrier, inc=1, device_id=(lax.rem(me + k, n), tp), device_id_type=MESH)
        return carry

    lax.fori_loop(1, n, greet, 0)
    pl.semaphore_signal(barrier, inc=1, device_id=(me, peer), device_id_type=MESH)
    for copy in loads[first:early]:
        copy.start()

    @pl.when(me < 2)
    def _():
        mid_held[0] = jnp.zeros((2, rows, width), jnp.bfloat16)

    @pl.when(me < 1)
    def _():
        mid_held[1] = jnp.zeros((2, rows, width), jnp.bfloat16)

    def project(source, first, last):
        for copy in loads[first * local_heads : last * local_heads]:
            copy.wait()
        return jnp.dot(
            source[...], weight[:, first * width : last * width], preferred_element_type=jnp.float32
        ).astype(jnp.bfloat16)

    def at_rows(index):
        return pl.ds(pl.multiple_of(index * chunk, chunk), chunk)

    def scatter_token(row):
        group, index = split_by(row, chunk)
        high, low = split_by(group, members)
        return index * n + low * classes + high

    def gather_row(token):
        index, residue = split_by(token, n)
        high, low = split_by(residue, classes)
        side, inner = split_by(index, part_rows)
        return side * low_rows + (low * members + high) * part_rows + inner

    def low_row(row):
        group, inner = split_by(row, part_rows)
        return group * chunk + inner

    def class_token(row):
        group, index = split_by(row, stretch)
        return index * classes + group

    to_scattered = one_hot(rows, scatter_token)
    to_tokens = one_hot(rows, gather_row)
    to_classes = one_hot(rows, class_token)

    def moved(matrix, block):
        return jnp.dot(matrix, block, preferred_element_type=jnp.float32).astype(jnp.bfloat16)

    def each(action):
        for k in range(1, n):
            action(k)

    upper = me // (n // 2)

    def target_of(k):
        rising = k - 1 + jnp.where(k - 1 >= me, 1, 0)
        falling = n - k - jnp.where(n - k <= me, 1, 0)
        return jnp.where(upper == 1, rising, falling)


    def far_copy(source, target, sem, k):
        to = target_of(k)
        return pltpu.make_async_remote_copy(
            src_ref=source.at[at_rows(to)],
            dst_ref=target.at[at_rows(me)],
            send_sem=sem.at[0],
            recv_sem=sem.at[1],
            device_id=(to, tp),
            device_id_type=MESH,
        )

    def far_whole(source, target, sem):
        others = pl.ds(0, rows - chunk)
        return pltpu.make_async_remote_copy(
            src_ref=source.at[others],
            dst_ref=target.at[others],
            send_sem=sem.at[0],
            recv_sem=sem.at[1],
            device_id=(lax.rem(me + 1, n), tp),
            device_id_type=MESH,
        )

    plane = me // members
    planes = n // members

    def back_copy(k):
        to = target_of(k)
        return pltpu.make_async_remote_copy(
            src_ref=back_send.at[at_rows(to)],
            dst_ref=back_held.at[at_rows(me)],
            send_sem=back_ssem,
            recv_sem=back_rsem.at[plane],
            device_id=(to, tp),
            device_id_type=MESH,
        )

    def back_some(count, group):
        some = pl.ds(0, count * chunk)
        return pltpu.make_async_remote_copy(
            src_ref=back_send.at[some],
            dst_ref=back_held.at[some],
            send_sem=back_ssem,
            recv_sem=back_rsem.at[group],
            device_id=(lax.rem(me + 1, n), tp),
            device_id_type=MESH,
        )

    def log_copy(k):
        to = target_of(k)
        return pltpu.make_async_remote_copy(
            src_ref=log_send.at[to],
            dst_ref=log_held.at[me],
            send_sem=log_ssem,
            recv_sem=log_rsem.at[plane],
            device_id=(to, tp),
            device_id_type=MESH,
        )

    def log_some(count, group):
        some = pl.ds(0, count)
        return pltpu.make_async_remote_copy(
            src_ref=log_send.at[some],
            dst_ref=log_held.at[some],
            send_sem=log_ssem,
            recv_sem=log_rsem.at[group],
            device_id=(lax.rem(me + 1, n), tp),
            device_id_type=MESH,
        )

    for copy, part in zip(tok_loads, halves):
        copy.wait()
        scattered[:, part] = moved(to_scattered, tok[:, part])
    for side, part in enumerate(halves):
        for copy in loads[:first]:
            copy[side].wait()
        term = jnp.dot(scattered[:, part], weight[part, : 2 * width], preferred_element_type=jnp.float32)
        if side == 0:
            product[...] = term
        else:
            first_send[...] = (product[...] + term).astype(jnp.bfloat16)
    for copy in loads[early:]:
        copy.start()
    pl.semaphore_wait(barrier, n)
    each(lambda k: far_copy(first_send, first_held, first_sem, k).start())
    first_held[at_rows(me), :] = first_send[at_rows(me), :]

    def mid_copy(slot, hop, source, part, sem):
        return pltpu.make_async_remote_copy(
            src_ref=source,
            dst_ref=mid_held.at[slot, part],
            send_sem=mid_ssem.at[sem, part],
            recv_sem=mid_rsem.at[slot, part],
            device_id=(lax.rem(me + hop + n, n), tp),
            device_id_type=MESH,
        )

    def near_copy(hop, source, part, sem):
        return pltpu.make_async_remote_copy(
            src_ref=source,
            dst_ref=near_held.at[part],
            send_sem=near_ssem.at[sem],
            recv_sem=near_rsem.at[part],
            device_id=(lax.rem(me + hop, n), tp),
            device_id_type=MESH,
        )

    def via_copy(which, source, target):
        return pltpu.make_async_remote_copy(
            src_ref=source,
            dst_ref=target,
            send_sem=via_ssem.at[which],
            recv_sem=via_rsem.at[which],
            device_id=(lax.rem(me + -2 + n, n), tp),
            device_id_type=MESH,
        )

    near_tail = pl.ds(rows - NEAR_WINDOW, NEAR_WINDOW)
    key_two = mid_copy(0, 2, mid_own.at[0], 0, 0)
    key_one = mid_copy(1, 1, mid_own.at[0], 0, 1)
    value_two = mid_copy(0, 2, mid_own.at[1], 1, 0)
    value_one = mid_copy(1, 1, mid_own.at[1], 1, 1)
    near_key = near_copy(1, near_own.at[0, near_tail], 0, 0)
    near_value = near_copy(1, near_own.at[1, near_tail], 1, 1)
    via_mid = via_copy(0, mid_own.at[1], via_held)
    onward_even = mid_copy(0, 4, via_held, 1, 3)
    onward_odd = mid_copy(1, 3, via_held, 1, 3)
    relay_key = mid_copy(0, 1, mid_held.at[1, 0], 0, 2)
    relay_value = mid_copy(0, 1, mid_held.at[1, 1], 1, 2)

    even = lax.rem(me, 2) == 0
    odd = jnp.logical_not(even)
    sends_one = me + 1 < n
    sends_two = even & (me + 2 < n)
    relays = even & (me >= 1)
    above = me + 4 - lax.rem(me, 4) < n
    crosses = (lax.rem(me, 4) >= 2) & above
    stays = jnp.logical_not(crosses)
    forwards = (lax.rem(me, 4) < 2) & above
    direct = sends_one & jnp.logical_not(crosses & odd)

    pair = moved(to_classes, project(tok, 2, 4))
    mid_own[0] = pair[:, :width]
    mid_own[1] = pair[:, width:]

    @pl.when(crosses)
    def _():
        via_mid.start()

    pair = project(scattered, 4, 6)
    second_send[...] = pair[:, :width]
    near_query[...] = pair[:, width:]
    near_low[...] = moved(one_hot(rows, low_row)[:low_rows], pair[:, width:])
    each(lambda k: far_copy(second_send, second_held, second_sem, k).start())
    second_held[at_rows(me), :] = second_send[at_rows(me), :]
    wo_load.start()

    @pl.when(sends_two & stays)
    def _():
        value_two.start()
        key_two.start()

    @pl.when(direct)
    def _():
        value_one.start()
        key_one.start()

    @pl.when(crosses & even)
    def _():
        key_two.start()

    @pl.when(crosses & odd)
    def _():
        key_one.start()

    pair = project(tok, 6, 8)
    near_own[0] = pair[:, :width]
    near_own[1] = pair[:, width:]

    @pl.when(sends_one)
    def _():
        near_key.start()
        near_value.start()

    mid_query[...] = project(scattered, 8, 9)

    def slope_of(head, window):
        number = tp * local_heads + head
        slope = jnp.float32(0.0)
        for index in range(HEADS):
            value = 2.0 ** (3.0 - 8.0 * (index + 1.0) / HEADS) / window
            slope = jnp.where(number == index, jnp.float32(value), slope)
        return slope

    row, column = grid(rows, rows)
    apart = scatter_token(row) - column
    valid = (apart >= 0) & (apart <= NEAR_WINDOW)
    distance = apart.astype(jnp.float32)
    heads = [pl.ds(head * HEAD_DIM, HEAD_DIM) for head in range(local_heads)]

    def join(parts, side):
        held = [
            (
                stats[2 * head, :, side].reshape(-1, 1), stats[2 * head + 1, :, side].reshape(-1, 1),
                near_sum[head, :, side].reshape(-1, HEAD_DIM),
            )
            for head in range(local_heads)
        ]
        joined = []
        for (high, total, part), (held_high, held_total, held_part) in zip(parts, held):
            highest = jnp.maximum(held_high, high)
            held_share, share = jnp.exp(held_high - highest), jnp.exp(high - highest)
            joined.append((
                highest, held_total * held_share + total * share, held_part * held_share + part * share
            ))
        keep(joined, side)

    def keep(parts, side):
        shape = (n, -1, part_rows) if isinstance(side, slice) else (n, part_rows)
        for head, (high, total, part) in enumerate(parts):
            stats[2 * head, :, side] = high.reshape(*shape, 1)
            stats[2 * head + 1, :, side] = total.reshape(*shape, 1)
            near_sum[head, :, side] = part.reshape(*shape, HEAD_DIM)

    both = slice(0, 2)

    def partial_of(query, key_value, slopes, distance, valid):
        weighed = [
            weigh(scores_of(query[:, at], key_value[0, :, at]), slope, distance, valid)
            for at, slope in zip(heads, slopes)
        ]
        return [
            (high, total, apply(weights, key_value[1, :, at]))
            for at, (high, weights, total) in zip(heads, weighed)
        ]

    near_slopes = [slope_of(head, NEAR_WINDOW) for head in range(local_heads)]
    keep(partial_of(near_query, near_own, near_slopes, distance, valid), both)

    def near_rest():
        near_key.wait_recv()
        near_value.wait_recv()
        row, column = grid(low_rows, NEAR_WINDOW)
        apart = scatter_token(low_row(row)) + NEAR_WINDOW - column
        valid = (apart >= 0) & (apart <= NEAR_WINDOW)
        distance = apart.astype(jnp.float32)
        join(partial_of(near_low, near_held, near_slopes, distance, valid), 0)

    @pl.when(odd)
    def _():
        near_rest()

    @pl.when(forwards)
    def _():
        via_mid.wait_recv()

    @pl.when(forwards & even)
    def _():
        onward_even.start()

    @pl.when(forwards & odd)
    def _():
        onward_odd.start()

    far_whole(first_send, first_held, first_sem).wait_recv()

    reach = FAR_WINDOW // FAR_DILATION
    lane = lax.broadcasted_iota(jnp.int32, (rows, HEAD_DIM), 1)
    slot = lax.broadcasted_iota(jnp.int32, (rows, HEAD_DIM), 0) & (chunk - 1)
    of_slot = lane == slot

    blocks = ((0, reach), (reach, rows))
    weighed = []
    for head in range(local_heads):
        at = pl.ds(2 * head * HEAD_DIM, HEAD_DIM)
        key_at = pl.ds((2 * head + 1) * HEAD_DIM, HEAD_DIM)
        for first_row, last_row in blocks:
            row, column = grid(last_row - first_row, last_row)
            apart = row + first_row - column
            weighed.append(weigh(
                scores_of(first_held[first_row:last_row, at], first_held[:last_row, key_at]),
                slope_of(head, FAR_WINDOW), (apart * FAR_DILATION).astype(jnp.float32),
                (apart >= 0) & (apart <= reach),
            ))
    packed = []
    for head in range(local_heads):
        parts = weighed[head * len(blocks) : (head + 1) * len(blocks)]
        logs = jnp.concatenate([high + jnp.log(total) for high, _, total in parts], axis=0)
        packed.append(jnp.sum(
            jnp.where(of_slot, logs, 0.0).reshape(n, chunk, HEAD_DIM), axis=1, keepdims=True
        ))
    log_send[...] = jnp.concatenate(packed, axis=2)
    for head in range(local_heads):
        parts = weighed[head * len(blocks) : (head + 1) * len(blocks)]
        for (first_row, last_row), (_, weights, total) in zip(blocks, parts):
            probs[head, first_row:last_row, :last_row] = (weights * (1.0 / total)).astype(jnp.bfloat16)
    each(lambda k: log_copy(k).start())
    log_held[me] = log_send[me]

    far_whole(second_send, second_held, second_sem).wait_recv()
    for head, at in enumerate(heads):
        for first_row, last_row in blocks:
            back_send[first_row:last_row, at] = jnp.dot(
                probs[head, first_row:last_row, :last_row], second_held[:last_row, at],
                preferred_element_type=jnp.float32,
            ).astype(jnp.bfloat16)
    each(lambda k: back_copy(k).start())
    back_held[at_rows(me), :] = back_send[at_rows(me), :]

    @pl.when(me >= 1)
    def _():
        value_one.wait_recv()
        key_one.wait_recv()

    @pl.when(relays)
    def _():
        relay_value.start()
        relay_key.start()

    @pl.when(me >= 2)
    def _():
        key_two.wait_recv()
        value_two.wait_recv()

    keys = MIDDLE_WINDOW // classes + stretch
    row, column = grid(rows, keys)
    group, index = split_by(row, chunk)
    apart = index * members + split_by(group, members)[1] + MIDDLE_WINDOW // classes - column
    valid = (apart >= 0) & (apart <= MIDDLE_WINDOW // classes)
    valid = valid & (column + me * stretch >= MIDDLE_WINDOW // classes)
    distance = (apart * classes).astype(jnp.float32)

    def class_rows(part, group, at):
        of_class = pl.ds(group * stretch, stretch)
        return jnp.concatenate(
            (mid_held[0, part, of_class, at], mid_held[1, part, of_class, at], mid_own[part, of_class, at]), axis=0
        )

    weighed = []
    for head, at in enumerate(heads):
        scores = jnp.concatenate([
            scores_of(mid_query[group * stretch : (group + 1) * stretch, at], class_rows(0, group, at))
            for group in range(classes)
        ], axis=0)
        weighed.append(weigh(scores, slope_of(head, MIDDLE_WINDOW), distance, valid))
    join([
        (high, total, jnp.concatenate([
            apply(weights[group * stretch : (group + 1) * stretch], class_rows(1, group, at))
            for group in range(classes)
        ], axis=0))
        for at, (high, weights, total) in zip(heads, weighed)
    ], both)

    block = members * part_rows

    def merged_copy(group, side):
        place = pl.ds(pl.multiple_of(side * low_rows + group * block, block), block)
        return pltpu.make_async_remote_copy(
            src_ref=merged_own.at[place],
            dst_ref=merged_held.at[place],
            send_sem=merged_ssem.at[group, side],
            recv_sem=merged_rsem.at[group, side],
            device_id=(me, peer),
            device_id_type=MESH,
        )

    lane = lax.broadcasted_iota(jnp.int32, (block, HEAD_DIM), 1)
    slot = lax.broadcasted_iota(jnp.int32, (block, HEAD_DIM), 0) & (part_rows - 1)

    def factors(group, side):
        some = pl.ds(group * members, members)
        split = jnp.zeros((block, HEAD_DIM), jnp.float32)
        shares = []
        held = log_held[some]
        for head in range(local_heads):
            spread = jnp.broadcast_to(
                held[:, :, head * HEAD_DIM : (head + 1) * HEAD_DIM], (members, part_rows, HEAD_DIM)
            ).reshape(block, HEAD_DIM)
            far_log = jnp.sum(jnp.where(lane == slot + side * part_rows, spread, 0.0), axis=-1, keepdims=True)
            pair_log = stats[2 * head, some, side].reshape(block, 1)
            pair_sum = stats[2 * head + 1, some, side].reshape(block, 1)
            highest = jnp.maximum(pair_log, far_log)
            pair_part, far_part = jnp.exp(pair_log - highest), jnp.exp(far_log - highest)
            mass = pair_sum * pair_part + far_part
            inverse = 1.0 / mass
            pair_term = near_sum[head, some, side].reshape(block, HEAD_DIM) * (pair_part * inverse)
            shares.append((pair_term, far_part * inverse))
            rest = highest + jnp.log(mass)
            for term in range(3):
                piece = rest.astype(jnp.bfloat16).astype(jnp.float32)
                split = jnp.where(lane == 3 * head + term, piece, split)
                rest = rest - piece
        return shares, split

    def merge(group, side, shares, split):
        source = pl.ds(pl.multiple_of(group * members * chunk, members * chunk), members * chunk)
        place = pl.ds(pl.multiple_of(side * low_rows + group * block, block), block)
        merged = []
        for at, (pair_term, share) in zip(heads, shares):
            far = back_held[source, at].astype(jnp.float32).reshape(members, 2, part_rows, HEAD_DIM)
            merged.append((pair_term + far[:, side].reshape(block, HEAD_DIM) * share).astype(jnp.bfloat16))
        for at, value in zip(heads, merged):
            merged_own[place, at] = value
        merged_copy(group, side).start()
        terms[place] = split.astype(jnp.bfloat16)

    twin = plane + 1 - 2 * lax.rem(plane, 2)
    below = (1 - upper) * (planes // 2)
    soon = ((plane, members - 1), (twin, members), (below, members))
    late = below + 1
    waits_near = (lax.rem(me, members) == 0) & (plane == planes // 2)

    @pl.when(jnp.logical_not(waits_near))
    def _():
        @pl.when(even & (me >= 1))
        def _():
            near_rest()

        for lot in (soon, ((late, members),)):
            for group, count in lot:
                log_some(count, group).wait_recv()
            ready = [[factors(group, side) for side in range(2)] for group, _ in lot]
            for (group, count), sides in zip(lot, ready):
                back_some(count, group).wait_recv()
                for side, held in enumerate(sides):
                    merge(group, side, *held)

    @pl.when(waits_near)
    def _():
        for group, count in soon:
            log_some(count, group).wait_recv()
        ready = [factors(group, 1) for group, _ in soon]
        for (group, count), held in zip(soon, ready):
            back_some(count, group).wait_recv()
            merge(group, 1, *held)
        near_rest()
        ready = [factors(group, 0) for group, _ in soon]
        for (group, _), held in zip(soon, ready):
            merge(group, 0, *held)
        log_some(members, late).wait_recv()
        ready = [factors(late, side) for side in range(2)]
        back_some(members, late).wait_recv()
        for side, held in enumerate(ready):
            merge(late, side, *held)

    lane = lax.broadcasted_iota(jnp.int32, (rows, HEAD_DIM), 1)
    totals = jnp.dot(to_tokens, terms[...], preferred_element_type=jnp.float32)
    summed = jnp.zeros((rows, HEAD_DIM), jnp.float32)
    for head in range(local_heads):
        total = jnp.sum(
            jnp.where((lane >= 3 * head) & (lane < 3 * head + 3), totals, 0.0), axis=-1, keepdims=True
        )
        summed = jnp.where(lane == head, total, summed)
    totals_ref[...] = summed
    wo_load.wait()
    partial_ref[...] = jnp.dot(
        moved(to_tokens, merged_own[...]), wo[pl.ds(pl.multiple_of(tp * width, width), width), :],
        preferred_element_type=jnp.float32,
    )

    far_whole(first_send, first_held, first_sem).wait_send()
    far_whole(second_send, second_held, second_sem).wait_send()
    log_some(n - 1, 0).wait_send()
    back_some(n - 1, 0).wait_send()

    @pl.when(crosses)
    def _():
        via_mid.wait_send()

    @pl.when(sends_two)
    def _():
        key_two.wait_send()

    @pl.when(sends_two & stays)
    def _():
        value_two.wait_send()

    @pl.when(sends_one)
    def _():
        key_one.wait_send()
        near_key.wait_send()
        near_value.wait_send()

    @pl.when(direct)
    def _():
        value_one.wait_send()

    @pl.when(forwards & even)
    def _():
        onward_even.wait_send()

    @pl.when(forwards & odd)
    def _():
        onward_odd.wait_send()

    @pl.when(relays)
    def _():
        relay_key.wait_send()
        relay_value.wait_send()

    for group in range(planes):
        for side in range(2):
            merged_copy(group, side).wait_recv()
    peer_ref[...] = moved(to_tokens, merged_held[...])
    for group in range(planes):
        for side in range(2):
            merged_copy(group, side).wait_send()


def mix(partial_ref, peer_ref, totals_ref, wo_ref, mixed_ref, log_ref):
    width = peer_ref.shape[1]
    at = pl.ds(pl.multiple_of((1 - lax.axis_index("tp")) * width, width), width)
    product = jnp.dot(peer_ref[...], wo_ref[at], preferred_element_type=jnp.float32)
    mixed_ref[...] = (partial_ref[...] + product).astype(jnp.bfloat16)
    log_ref[...] = jnp.transpose(totals_ref[...])[: log_ref.shape[0]]


def fused(n, tokens, query_weight, key_weight, value_weight, out_weight):
    rows, depth = tokens.shape
    columns = query_weight.shape[1]
    out_columns = out_weight.shape[1]
    local_heads = columns // (3 * HEAD_DIM)
    width = local_heads * HEAD_DIM
    planes = MIDDLE_DILATION
    dma = pltpu.SemaphoreType.DMA
    half = jnp.bfloat16
    full = jnp.float32
    whole = pl.BlockSpec(memory_space=pltpu.VMEM)
    anywhere = pl.BlockSpec(memory_space=pl.ANY)
    partial, peer, totals = pl.pallas_call(
        functools.partial(kernel, n, local_heads),
        out_shape=(
            jax.ShapeDtypeStruct((rows, out_columns), full),
            jax.ShapeDtypeStruct((rows, width), half),
            jax.ShapeDtypeStruct((rows, HEAD_DIM), full),
        ),
        in_specs=[anywhere] * 5,
        out_specs=(whole, whole, whole),
        scratch_shapes=[
            pltpu.VMEM((rows, depth), half),
            pltpu.VMEM((rows, depth), half),
            pltpu.VMEM((rows, 2 * width), full),
            pltpu.VMEM((depth, 3 * columns), half),
            pltpu.VMEM(out_weight.shape, half),
            pltpu.VMEM((rows, 2 * width), half),
            pltpu.VMEM((rows, 2 * width), half),
            pltpu.VMEM((rows, width), half),
            pltpu.VMEM((rows, width), half),
            pltpu.VMEM((rows, width), half),
            pltpu.VMEM((rows, width), half),
            pltpu.VMEM((n, 1, width), full),
            pltpu.VMEM((n, 1, width), full),
            pltpu.VMEM((local_heads, rows, rows), half),
            pltpu.VMEM((rows, width), half),
            pltpu.VMEM((2, rows, width), half),
            pltpu.VMEM((2, 2, rows, width), half),
            pltpu.VMEM((rows, width), half),
            pltpu.VMEM((rows, width), half),
            pltpu.VMEM((rows // 2, width), half),
            pltpu.VMEM((2, rows, width), half),
            pltpu.VMEM((2, NEAR_WINDOW, width), half),
            pltpu.VMEM((2 * local_heads, n, 2, rows // (2 * n), 1), full),
            pltpu.VMEM((rows, HEAD_DIM), half),
            pltpu.VMEM((rows, width), half),
            pltpu.VMEM((rows, width), half),
            pltpu.VMEM((local_heads, n, 2, rows // (2 * n), HEAD_DIM), full),
            dma((1 + 9 * local_heads,)), dma((2, 1 + 2 * local_heads)), dma((2,)), dma((2,)),
            dma(()), dma((planes,)), dma(()), dma((planes,)),
            dma((4, 2)), dma((2, 2)), dma((1,)), dma((1,)), dma((2,)), dma((2,)), dma((planes, 2)), dma((planes, 2)),
        ],
        compiler_params=pltpu.CompilerParams(
            collective_id=0, has_side_effects=True, vmem_limit_bytes=53000 * 1024
        ),
    )(tokens, query_weight, key_weight, value_weight, out_weight)
    return pl.pallas_call(
        mix,
        out_shape=(
            jax.ShapeDtypeStruct((rows, out_columns), half),
            jax.ShapeDtypeStruct((local_heads, rows), full),
        ),
        in_specs=[whole] * 4,
        out_specs=(whole, whole),
        compiler_params=pltpu.CompilerParams(vmem_limit_bytes=16000 * 1024),
    )(partial, peer, totals, out_weight)


def solution(mesh):
    n, n_tp = mesh.shape["sp"], mesh.shape["tp"]
    if n == FAR_DILATION and n_tp == 2:
        body = functools.partial(fused, n)
    else:
        body = local
    return jax.shard_map(
        body,
        mesh=mesh,
        in_specs=(P("sp", None), P(None, "tp"), P(None, "tp"), P(None, "tp"), P(None, "tp")),
        out_specs=(P("sp", "tp"), P("tp", "sp")),
        check_vma=False,
    )
```

```python
import functools
import jax
import jax.numpy as jnp
from jax import lax
from jax.experimental import pallas as pl
from jax.experimental.pallas import tpu as pltpu
from jax.sharding import PartitionSpec as P

HEADS = 4
HEAD_DIM = 128
NEAR_WINDOW = 128
MIDDLE_WINDOW = 512
MIDDLE_DILATION = 4
FAR_WINDOW = 2048
FAR_DILATION = 16


def from_behind(block, axis, distance):
    devices = range(lax.axis_size(axis))
    route = [(i - distance, i) for i in devices if i - distance in devices]
    return lax.ppermute(block, axis, route)


def window_table():
    return ((NEAR_WINDOW, 1), (MIDDLE_WINDOW, MIDDLE_DILATION), (FAR_WINDOW, FAR_DILATION))


def tail_counts(row_count, distance, held_rows):
    counts = []
    for entry, available in zip(window_table(), held_rows):
        counts.append(max(0, min(available, entry[0] - (distance - 1) * row_count)))
    return counts


def pack_tails(sources, counts):
    selected = [
        source[:, source.shape[1] - amount :]
        for source, amount in zip(sources, counts)
        if amount > 0
    ]
    return jnp.concatenate(selected, axis=1)


def unpack_rows(packed, counts):
    result = []
    cursor = 0
    for amount in counts:
        result.append(packed[:, cursor : cursor + amount])
        cursor = cursor + amount
    return result


def attend_group(group_queries, buffer, window, dilation, first_key, slopes_here):
    row_count = group_queries.shape[0]
    head_count = group_queries.shape[1]
    head_size = group_queries.shape[2]
    query_split = group_queries.reshape(row_count // dilation, dilation, head_count, head_size)
    key_split = buffer[0].reshape(-1, dilation, head_count, head_size)
    value_split = buffer[1].reshape(-1, dilation, head_count, head_size)
    scores = jnp.einsum(
        "mrhe,nrhe->rhmn", query_split, key_split, preferred_element_type=jnp.float32
    ) * head_size ** (-0.5)
    grid_shape = (row_count // dilation, key_split.shape[0])
    query_slot = lax.broadcasted_iota(jnp.int32, grid_shape, 0)
    key_slot = lax.broadcasted_iota(jnp.int32, grid_shape, 1)
    spacing = query_slot + window // dilation - key_slot
    residue = lax.broadcasted_iota(jnp.int32, (dilation, 1, 1), 0)
    key_place = first_key + residue + dilation * key_slot[None]
    valid = (spacing[None] >= 0) & (spacing[None] <= window // dilation) & (key_place >= 0)
    scores = (
        scores
        - slopes_here[None, :, None, None] * (dilation * spacing).astype(jnp.float32)[None, None]
    )
    masked = jnp.where(valid[:, None], scores, -jnp.inf)
    highest = jnp.max(masked, axis=-1, keepdims=True)
    log_sum = highest + jnp.log(jnp.sum(jnp.exp(masked - highest), axis=-1, keepdims=True))
    probs = jnp.exp(masked - log_sum).astype(jnp.bfloat16)
    attended = jnp.einsum("rhmn,nrhe->mrhe", probs, value_split, preferred_element_type=jnp.float32)
    attended = attended.reshape(row_count, head_count, head_size)
    log_rows = jnp.transpose(log_sum[..., 0], (1, 2, 0)).reshape(head_count, row_count)
    return (attended, log_rows)


def local(tokens, query_weight, key_weight, value_weight, out_weight):
    rows_here = tokens.shape[0]
    local_heads = query_weight.shape[1] // (3 * HEAD_DIM)

    def project(weight_matrix):
        product = jnp.dot(tokens, weight_matrix, preferred_element_type=jnp.float32)
        return product.astype(jnp.bfloat16).reshape(rows_here, local_heads, 3, HEAD_DIM)

    queries = project(query_weight)
    keys_all = project(key_weight)
    values_all = project(value_weight)
    table = window_table()
    own = [jnp.stack((keys_all[:, :, index], values_all[:, :, index])) for index in range(3)]
    held = list(own)
    span_now = 1
    while span_now * rows_here < FAR_WINDOW + rows_here:
        counts = tail_counts(rows_here, span_now, [item.shape[1] for item in held])
        packed = pack_tails(held, counts)
        arrived = from_behind(packed, "sp", span_now)
        pieces_in = unpack_rows(arrived, counts)
        for index in range(3):
            if counts[index] > 0:
                joined = jnp.concatenate((pieces_in[index], held[index]), axis=1)
                held[index] = joined
        span_now = span_now * 2
    priors = [held[index][:, : table[index][0]] for index in range(3)]
    position_start = lax.axis_index("sp") * rows_here
    head_ids = (
        lax.axis_index("tp") * local_heads + jnp.arange(local_heads, dtype=jnp.int32)
    ).astype(jnp.float32)
    outputs = []
    logs = []
    for index, (window, dilation) in enumerate(table):
        buffer = jnp.concatenate((priors[index], own[index]), axis=1)
        slopes_here = 2.0 ** (3.0 - 8.0 * (head_ids + 1.0) / HEADS) / window
        attended, log_rows = attend_group(
            queries[:, :, index], buffer, window, dilation, position_start - window, slopes_here
        )
        outputs.append(attended)
        logs.append(log_rows)
    stacked_logs = jnp.stack(logs)
    highest = jnp.max(stacked_logs, axis=0)
    total_log = highest + jnp.log(jnp.sum(jnp.exp(stacked_logs - highest), axis=0))
    mixing = jnp.exp(stacked_logs - total_log)
    merged = outputs[0] * jnp.transpose(mixing[0])[:, :, None]
    merged = merged + outputs[1] * jnp.transpose(mixing[1])[:, :, None]
    merged = merged + outputs[2] * jnp.transpose(mixing[2])[:, :, None]
    merged = merged.astype(jnp.bfloat16).reshape(rows_here, local_heads * HEAD_DIM)
    mixed = jnp.dot(
        lax.all_gather(merged, "tp", axis=1, tiled=True),
        out_weight,
        preferred_element_type=jnp.float32,
    ).astype(jnp.bfloat16)
    return (mixed, total_log)


MESH = pl.DeviceIdType.MESH
MASKED = -1e30


def scores_of(query, key):
    return lax.dot_general(
        query, key, (((1,), (1,)), ((), ())), preferred_element_type=jnp.float32
    ) * HEAD_DIM ** (-0.5)


def weigh(scores, slope, distance, valid):
    scores = jnp.where(valid, scores - slope * distance, MASKED)
    highest = jnp.max(scores, axis=-1, keepdims=True)
    weights = jnp.exp(scores - highest)
    return highest, weights, jnp.sum(weights, axis=-1, keepdims=True)


def apply(weights, value):
    return jnp.dot(weights.astype(jnp.bfloat16), value, preferred_element_type=jnp.float32)


def split_by(value, size):
    shift = size.bit_length() - 1
    return value >> shift, value & (size - 1)


def grid(row_count, key_count):
    row = lax.broadcasted_iota(jnp.int32, (row_count, 1), 0)
    column = lax.broadcasted_iota(jnp.int32, (row_count, key_count), 1)
    return row, column


def one_hot(rows, token_of_row):
    row, column = grid(rows, rows)
    return jnp.where(column == token_of_row(row), 1.0, 0.0).astype(jnp.bfloat16)


def kernel(
    n, local_heads,
    tok_hbm, wq_hbm, wk_hbm, wv_hbm, wo_hbm,
    partial_ref, peer_ref, totals_ref,
    tok, scattered, product, weight, wo, first_send, first_held, second_send, second_held, back_send, back_held, log_send, log_held, probs,
    mid_query, mid_own, mid_held, via_held, near_query, near_low, near_own, near_held, guest_query, guest_out, guest_log, guest_back, guest_back_log,
    stats, terms, merged_own, merged_held, near_sum,
    load_sem, first_sem, second_sem, back_ssem, back_rsem, log_ssem, log_rsem,
    mid_ssem, mid_rsem, via_rsem, near_ssem, near_rsem, guest_sem, merged_sem,
):
    me = lax.axis_index("sp")
    tp = lax.axis_index("tp")
    rows = tok.shape[0]
    width = local_heads * HEAD_DIM
    chunk = rows // n
    classes = MIDDLE_DILATION
    members = n // classes
    stretch = rows // classes
    part_rows = chunk // 2
    low_rows = rows // 2
    peer = 1 - tp
    sources = (wq_hbm, wk_hbm, wv_hbm)

    depth = tok.shape[1]
    halves = (pl.ds(0, depth // 2), pl.ds(depth // 2, depth // 2))
    tok_loads = [
        pltpu.make_async_copy(tok_hbm.at[:, part], tok.at[:, part], load_sem.at[side])
        for side, part in enumerate(halves)
    ]
    wo_load = pltpu.make_async_copy(wo_hbm, wo, load_sem.at[4])
    loads = []
    far_order = [(2, part, head) for head in range(local_heads) for part in range(3)]
    order = far_order[: 2 * local_heads]
    order += [(1, part, head) for part in (1, 2) for head in range(local_heads)]
    order += far_order[2 * local_heads :]
    for group, part in ((0, 0), (0, 1), (0, 2), (1, 0)):
        order += [(group, part, head) for head in range(local_heads)]
    first = 2 * local_heads
    early = 4 * local_heads
    for place, (group, part, head) in enumerate(order):
        source = sources[part].at[:, pl.ds((head * 3 + group) * HEAD_DIM, HEAD_DIM)]
        target = weight.at[:, pl.ds(place * HEAD_DIM, HEAD_DIM)]
        if place < first:
            loads.append([
                pltpu.make_async_copy(source.at[side], target.at[side], load_sem.at[2 + index])
                for index, side in enumerate(halves)
            ])
        else:
            loads.append(pltpu.make_async_copy(source, target, load_sem.at[4 + place // first]))
    for copy in tok_loads:
        copy.start()
    for side in range(2):
        for copy in loads[:first]:
            copy[side].start()

    barrier = pltpu.get_barrier_semaphore()

    def greet(k, carry):
        pl.semaphore_signal(barrier, inc=1, device_id=(lax.rem(me + k, n), tp), device_id_type=MESH)
        return carry

    lax.fori_loop(1, n, greet, 0)
    pl.semaphore_signal(barrier, inc=1, device_id=(me, peer), device_id_type=MESH)
    for copy in loads[first:early]:
        copy.start()

    @pl.when(me < 2)
    def _():
        mid_held[0] = jnp.zeros((2, rows, width), jnp.bfloat16)

    @pl.when(me < 1)
    def _():
        mid_held[1] = jnp.zeros((2, rows, width), jnp.bfloat16)

    def project(source, first, last):
        part = weight.at[:, pl.ds(first * width, (last - first) * width)]
        pltpu.make_async_copy(part, part, load_sem.at[4 + first // 2]).wait()
        return jnp.dot(
            source[...], weight[:, first * width : last * width], preferred_element_type=jnp.float32
        ).astype(jnp.bfloat16)

    def at_rows(index):
        return pl.ds(pl.multiple_of(index * chunk, chunk), chunk)

    def scatter_token(row):
        group, index = split_by(row, chunk)
        high, low = split_by(group, members)
        return index * n + low * classes + high

    def gather_row(token):
        index, residue = split_by(token, n)
        high, low = split_by(residue, classes)
        side, inner = split_by(index, part_rows)
        return side * low_rows + (low * members + high) * part_rows + inner

    def low_row(row):
        group, inner = split_by(row, part_rows)
        return group * chunk + inner

    def class_token(row):
        group, index = split_by(row, stretch)
        return index * classes + group

    to_scattered = one_hot(rows, scatter_token)
    to_tokens = one_hot(rows, gather_row)
    to_classes = one_hot(rows, class_token)

    def moved(matrix, block):
        return jnp.dot(matrix, block, preferred_element_type=jnp.float32).astype(jnp.bfloat16)

    def each(action):
        for k in range(1, n):
            action(k)

    upper = me // (n // 2)

    def target_of(k):
        rising = k - 1 + jnp.where(k - 1 >= me, 1, 0)
        falling = n - k - jnp.where(n - k <= me, 1, 0)
        return jnp.where(upper == 1, rising, falling)


    def far_copy(source, target, sem, k):
        to = target_of(k)
        return pltpu.make_async_remote_copy(
            src_ref=source.at[at_rows(to)],
            dst_ref=target.at[at_rows(me)],
            send_sem=sem.at[0],
            recv_sem=sem.at[1],
            device_id=(to, tp),
            device_id_type=MESH,
        )

    def far_whole(source, target, sem):
        others = pl.ds(0, rows - chunk)
        return pltpu.make_async_remote_copy(
            src_ref=source.at[others],
            dst_ref=target.at[others],
            send_sem=sem.at[0],
            recv_sem=sem.at[1],
            device_id=(lax.rem(me + 1, n), tp),
            device_id_type=MESH,
        )

    plane = me // members
    planes = n // members

    def back_copy(head, k):
        to = target_of(k)
        return pltpu.make_async_remote_copy(
            src_ref=back_send.at[head, at_rows(to)],
            dst_ref=back_held.at[head, at_rows(me)],
            send_sem=back_ssem,
            recv_sem=back_rsem.at[head, plane],
            device_id=(to, tp),
            device_id_type=MESH,
        )

    def back_some(head, count, group):
        some = pl.ds(0, count * chunk)
        return pltpu.make_async_remote_copy(
            src_ref=back_send.at[head, some],
            dst_ref=back_held.at[head, some],
            send_sem=back_ssem,
            recv_sem=back_rsem.at[head, group],
            device_id=(lax.rem(me + 1, n), tp),
            device_id_type=MESH,
        )

    def log_copy(head, k):
        to = target_of(k)
        return pltpu.make_async_remote_copy(
            src_ref=log_send.at[head, to],
            dst_ref=log_held.at[head, me],
            send_sem=log_ssem,
            recv_sem=log_rsem.at[head, plane],
            device_id=(to, tp),
            device_id_type=MESH,
        )

    def log_some(head, count, group):
        some = pl.ds(0, count)
        return pltpu.make_async_remote_copy(
            src_ref=log_send.at[head, some],
            dst_ref=log_held.at[head, some],
            send_sem=log_ssem,
            recv_sem=log_rsem.at[head, group],
            device_id=(lax.rem(me + 1, n), tp),
            device_id_type=MESH,
        )

    for copy, part in zip(tok_loads, halves):
        copy.wait()
        scattered[:, part] = moved(to_scattered, tok[:, part])
    for side, part in enumerate(halves):
        piece = weight.at[part, pl.ds(0, 2 * width)]
        pltpu.make_async_copy(piece, piece, load_sem.at[2 + side]).wait()
        term = jnp.dot(scattered[:, part], weight[part, : 2 * width], preferred_element_type=jnp.float32)
        if side == 0:
            product[...] = term
        else:
            first_send[...] = (product[...] + term).astype(jnp.bfloat16)
    for copy in loads[early:]:
        copy.start()
    pl.semaphore_wait(barrier, n)
    each(lambda k: far_copy(first_send, first_held, first_sem, k).start())
    first_held[at_rows(me), :] = first_send[at_rows(me), :]

    def mid_copy(slot, hop, source, part, sem):
        return pltpu.make_async_remote_copy(
            src_ref=source,
            dst_ref=mid_held.at[slot, part],
            send_sem=mid_ssem.at[min(2 * sem + part, 6)],
            recv_sem=mid_rsem.at[slot, part],
            device_id=(lax.rem(me + hop + n, n), tp),
            device_id_type=MESH,
        )

    def near_copy(hop, source, part, sem):
        return pltpu.make_async_remote_copy(
            src_ref=source,
            dst_ref=near_held.at[part],
            send_sem=near_ssem.at[sem],
            recv_sem=near_rsem.at[part],
            device_id=(lax.rem(me + hop, n), tp),
            device_id_type=MESH,
        )

    def via_copy(source, target):
        return pltpu.make_async_remote_copy(
            src_ref=source,
            dst_ref=target,
            send_sem=mid_ssem.at[1],
            recv_sem=via_rsem,
            device_id=(lax.rem(me + -2 + n, n), tp),
            device_id_type=MESH,
        )

    near_tail = pl.ds(rows - NEAR_WINDOW, NEAR_WINDOW)
    key_two = mid_copy(0, 2, mid_own.at[0], 0, 0)
    key_one = mid_copy(1, 1, mid_own.at[0], 0, 1)
    value_two = mid_copy(0, 2, mid_own.at[1], 1, 0)
    value_one = mid_copy(1, 1, mid_own.at[1], 1, 1)
    near_key = near_copy(1, near_own.at[0, near_tail], 0, 0)
    near_value = near_copy(1, near_own.at[1, near_tail], 1, 1)
    via_mid = via_copy(mid_own.at[1], via_held)
    onward_even = mid_copy(0, 4, via_held, 1, 3)
    onward_odd = mid_copy(1, 3, via_held, 1, 3)
    relay_key = mid_copy(0, 1, mid_held.at[1, 0], 0, 2)
    relay_value = mid_copy(0, 1, mid_held.at[1, 1], 1, 2)

    def guest_copy(hop, source, target, ssem, rsem):
        return pltpu.make_async_remote_copy(
            src_ref=source,
            dst_ref=target,
            send_sem=ssem,
            recv_sem=rsem,
            device_id=(lax.rem(me + hop + n, n), tp),
            device_id_type=MESH,
        )

    guest_ask = guest_copy(-1, near_low, guest_query, guest_sem.at[0], guest_sem.at[1])
    guest_tell = guest_copy(1, guest_out, guest_back, near_ssem.at[0], near_rsem.at[0])
    guest_tell_log = guest_copy(1, guest_log, guest_back_log, near_ssem.at[1], near_rsem.at[1])

    even = lax.rem(me, 2) == 0
    odd = jnp.logical_not(even)
    sends_one = me + 1 < n
    sends_two = even & (me + 2 < n)
    relays = even & (me >= 1)
    above = me + 4 - lax.rem(me, 4) < n
    crosses = (lax.rem(me, 4) >= 2) & above
    stays = jnp.logical_not(crosses)
    forwards = (lax.rem(me, 4) < 2) & above
    hosts = odd & sends_one
    guests = even & (me >= 1)
    direct = sends_one & jnp.logical_not(crosses & odd)

    pair = moved(to_classes, project(tok, 2, 4))
    mid_own[0] = pair[:, :width]
    mid_own[1] = pair[:, width:]

    @pl.when(crosses)
    def _():
        via_mid.start()

    pair = project(scattered, 4, 6)
    for head in range(local_heads):
        second_send[head] = pair[:, head * HEAD_DIM : (head + 1) * HEAD_DIM]
    near_query[...] = pair[:, width:]
    near_low[...] = moved(one_hot(rows, low_row)[:low_rows], pair[:, width:])
    for piece in range(2):
        each(lambda k: far_copy(
            second_send.at[piece], second_held.at[piece], second_sem.at[piece], k
        ).start())
    second_held[:, at_rows(me), :] = second_send[:, at_rows(me), :]
    wo_load.start()

    @pl.when(guests)
    def _():
        guest_ask.start()

    @pl.when(sends_two & stays)
    def _():
        value_two.start()
        key_two.start()

    @pl.when(direct)
    def _():
        value_one.start()
        key_one.start()

    @pl.when(crosses & even)
    def _():
        key_two.start()

    @pl.when(crosses & odd)
    def _():
        key_one.start()

    pair = project(tok, 6, 8)
    near_own[0] = pair[:, :width]
    near_own[1] = pair[:, width:]

    @pl.when(even)
    def _():
        near_key.start()
        near_value.start()

    mid_query[...] = project(scattered, 8, 9)

    def slope_of(head, window):
        number = tp * local_heads + head
        slope = jnp.float32(0.0)
        for index in range(HEADS):
            value = 2.0 ** (3.0 - 8.0 * (index + 1.0) / HEADS) / window
            slope = jnp.where(number == index, jnp.float32(value), slope)
        return slope

    row, column = grid(rows, rows)
    apart = scatter_token(row) - column
    valid = (apart >= 0) & (apart <= NEAR_WINDOW)
    distance = apart.astype(jnp.float32)
    heads = [pl.ds(head * HEAD_DIM, HEAD_DIM) for head in range(local_heads)]

    def join(parts, side):
        held = [
            (
                stats[2 * head, :, side].reshape(-1, 1), stats[2 * head + 1, :, side].reshape(-1, 1),
                near_sum[head, :, side].reshape(-1, HEAD_DIM),
            )
            for head in range(local_heads)
        ]
        joined = []
        for (high, total, part), (held_high, held_total, held_part) in zip(parts, held):
            highest = jnp.maximum(held_high, high)
            held_share, share = jnp.exp(held_high - highest), jnp.exp(high - highest)
            joined.append((
                highest, held_total * held_share + total * share, held_part * held_share + part * share
            ))
        keep(joined, side)

    def keep(parts, side):
        shape = (n, -1, part_rows) if isinstance(side, slice) else (n, part_rows)
        for head, (high, total, part) in enumerate(parts):
            stats[2 * head, :, side] = high.reshape(*shape, 1)
            stats[2 * head + 1, :, side] = total.reshape(*shape, 1)
            near_sum[head, :, side] = part.reshape(*shape, HEAD_DIM)

    both = slice(0, 2)

    def partial_of(query, key_value, slopes, distance, valid):
        weighed = [
            weigh(scores_of(query[:, at], key_value[0, :, at]), slope, distance, valid)
            for at, slope in zip(heads, slopes)
        ]
        return [
            (high, total, apply(weights, key_value[1, :, at]))
            for at, (high, weights, total) in zip(heads, weighed)
        ]

    near_slopes = [slope_of(head, NEAR_WINDOW) for head in range(local_heads)]
    keep(partial_of(near_query, near_own, near_slopes, distance, valid), both)

    def class_slot(row):
        group, index = split_by(row, chunk)
        return index * members + split_by(group, members)[1]

    def own_rows(part, group, at):
        return mid_own[part, pl.ds(group * stretch, stretch), at]

    def held_rows(part, group, at):
        of_class = pl.ds(group * stretch, stretch)
        return jnp.concatenate((mid_held[0, part, of_class, at], mid_held[1, part, of_class, at]), axis=0)

    def middle_of(rows_of, apart, valid):
        distance = (apart * classes).astype(jnp.float32)
        weighed = []
        for head, at in enumerate(heads):
            scores = jnp.concatenate([
                scores_of(mid_query[group * stretch : (group + 1) * stretch, at], rows_of(0, group, at))
                for group in range(classes)
            ], axis=0)
            weighed.append(weigh(scores, slope_of(head, MIDDLE_WINDOW), distance, valid))
        return [
            (high, total, jnp.concatenate([
                apply(weights[group * stretch : (group + 1) * stretch], rows_of(1, group, at))
                for group in range(classes)
            ], axis=0))
            for at, (high, weights, total) in zip(heads, weighed)
        ]

    row, column = grid(rows, stretch)
    apart = class_slot(row) - column
    join(middle_of(own_rows, apart, apart >= 0), both)


    def near_rest():
        near_key.wait_recv()
        near_value.wait_recv()
        row, column = grid(low_rows, NEAR_WINDOW)
        apart = scatter_token(low_row(row)) + NEAR_WINDOW - column
        valid = (apart >= 0) & (apart <= NEAR_WINDOW)
        distance = apart.astype(jnp.float32)
        join(partial_of(near_low, near_held, near_slopes, distance, valid), 0)

    def near_join():
        guest_tell.wait_recv()
        guest_tell_log.wait_recv()
        row, column = grid(low_rows, HEAD_DIM)
        parts = []
        for at in heads:
            log = jnp.sum(
                jnp.where(row == column, jnp.broadcast_to(guest_back_log[:, at], (low_rows, HEAD_DIM)), 0.0),
                axis=-1, keepdims=True,
            )
            parts.append((log, jnp.ones_like(log), guest_back[:, at].astype(jnp.float32)))
        join(parts, 0)

    def near_host():
        guest_ask.wait_recv()
        row, column = grid(low_rows, NEAR_WINDOW)
        apart = scatter_token(low_row(row)) + NEAR_WINDOW - column
        valid = (apart >= 0) & (apart <= NEAR_WINDOW)
        distance = apart.astype(jnp.float32)
        weighed = [
            weigh(scores_of(guest_query[:, at], near_own[0, near_tail, at]), slope, distance, valid)
            for at, slope in zip(heads, near_slopes)
        ]
        row, column = grid(low_rows, HEAD_DIM)
        for at, (high, weights, total) in zip(heads, weighed):
            guest_out[:, at] = apply(weights * (1.0 / total), near_own[1, near_tail, at]).astype(jnp.bfloat16)
            guest_log[:, at] = jnp.sum(
                jnp.where(row == column, high + jnp.log(total), 0.0), axis=0, keepdims=True
            )
        guest_tell_log.start()
        guest_tell.start()

    @pl.when(odd)
    def _():
        near_rest()

    @pl.when(forwards)
    def _():
        via_mid.wait_recv()

    @pl.when(forwards & even)
    def _():
        onward_even.start()

    @pl.when(forwards & odd)
    def _():
        onward_odd.start()

    far_whole(first_send, first_held, first_sem).wait_recv()

    reach = FAR_WINDOW // FAR_DILATION
    lane = lax.broadcasted_iota(jnp.int32, (rows, HEAD_DIM), 1)
    slot = lax.broadcasted_iota(jnp.int32, (rows, HEAD_DIM), 0) & (chunk - 1)
    of_slot = lane == slot

    blocks = ((0, reach), (reach, rows))

    def far_part(head, part, first_row, last_row):
        place = head * 3 + part
        if place < 2 * local_heads:
            return first_held[first_row:last_row, place * HEAD_DIM : (place + 1) * HEAD_DIM]
        return second_held[place - 2 * local_heads, first_row:last_row]

    def second_arrives(piece):
        far_whole(second_send.at[piece], second_held.at[piece], second_sem.at[piece]).wait_recv()

    for head in range(local_heads):
        if head == local_heads - 1:
            second_arrives(0)
        parts = []
        for first_row, last_row in blocks:
            row, column = grid(last_row - first_row, last_row)
            apart = row + first_row - column
            high, weights, total = weigh(
                scores_of(far_part(head, 0, first_row, last_row), far_part(head, 1, 0, last_row)),
                slope_of(head, FAR_WINDOW), (apart * FAR_DILATION).astype(jnp.float32),
                (apart >= 0) & (apart <= reach),
            )
            parts.append((high + jnp.log(total), weights * (1.0 / total)))
        logs = jnp.concatenate([log for log, _ in parts], axis=0)
        log_send[head] = jnp.sum(
            jnp.where(of_slot, logs, 0.0).reshape(n, chunk, HEAD_DIM), axis=1, keepdims=True
        )
        for (first_row, last_row), (_, shares) in zip(blocks, parts):
            probs[first_row:last_row, :last_row] = shares.astype(jnp.bfloat16)
        each(lambda k: log_copy(head, k).start())
        log_held[head, me] = log_send[head, me]
        if head == local_heads - 1:
            second_arrives(1)
        for first_row, last_row in blocks:
            back_send[head, first_row:last_row] = jnp.dot(
                probs[first_row:last_row, :last_row], far_part(head, 2, 0, last_row),
                preferred_element_type=jnp.float32,
            ).astype(jnp.bfloat16)
        each(lambda k: back_copy(head, k).start())
        back_held[head, at_rows(me), :] = back_send[head, at_rows(me), :]

    @pl.when(hosts)
    def _():
        near_host()

    @pl.when(me >= 1)
    def _():
        value_one.wait_recv()

    @pl.when(relays)
    def _():
        relay_value.start()

    @pl.when(me >= 1)
    def _():
        key_one.wait_recv()

    @pl.when(relays)
    def _():
        relay_key.start()

    @pl.when(me >= 2)
    def _():
        key_two.wait_recv()
        value_two.wait_recv()

    reach_slots = MIDDLE_WINDOW // classes
    row, column = grid(rows, reach_slots)
    apart = class_slot(row) + reach_slots - column
    valid = (apart >= 0) & (apart <= reach_slots) & (column + me * stretch >= reach_slots)
    join(middle_of(held_rows, apart, valid), both)

    block = members * part_rows

    def merged_copy(head, group, side):
        place = pl.ds(pl.multiple_of(side * low_rows + group * block, block), block)
        return pltpu.make_async_remote_copy(
            src_ref=merged_own.at[head, place],
            dst_ref=merged_held.at[head, place],
            send_sem=merged_sem.at[0],
            recv_sem=merged_sem.at[1],
            device_id=(me, peer),
            device_id_type=MESH,
        )

    lane = lax.broadcasted_iota(jnp.int32, (block, HEAD_DIM), 1)
    slot = lax.broadcasted_iota(jnp.int32, (block, HEAD_DIM), 0) & (part_rows - 1)

    def factors(head, group, side):
        some = pl.ds(group * members, members)
        spread = jnp.broadcast_to(
            log_held[head, some], (members, part_rows, HEAD_DIM)
        ).reshape(block, HEAD_DIM)
        far_log = jnp.sum(jnp.where(lane == slot + side * part_rows, spread, 0.0), axis=-1, keepdims=True)
        pair_log = stats[2 * head, some, side].reshape(block, 1)
        pair_sum = stats[2 * head + 1, some, side].reshape(block, 1)
        highest = jnp.maximum(pair_log, far_log)
        pair_part, far_share = jnp.exp(pair_log - highest), jnp.exp(far_log - highest)
        mass = pair_sum * pair_part + far_share
        inverse = 1.0 / mass
        pair_term = near_sum[head, some, side].reshape(block, HEAD_DIM) * (pair_part * inverse)
        rest = highest + jnp.log(mass)
        split = jnp.zeros((block, HEAD_DIM), jnp.float32)
        for term in range(3):
            piece = rest.astype(jnp.bfloat16).astype(jnp.float32)
            split = jnp.where(lane == 3 * head + term, piece, split)
            rest = rest - piece
        return pair_term, far_share * inverse, split

    def merge(head, group, side, pair_term, share, split):
        source = pl.ds(pl.multiple_of(group * members * chunk, members * chunk), members * chunk)
        place = pl.ds(pl.multiple_of(side * low_rows + group * block, block), block)
        far = back_held[head, source].astype(jnp.float32).reshape(members, 2, part_rows, HEAD_DIM)
        merged = pair_term + far[:, side].reshape(block, HEAD_DIM) * share
        merged_own[head, place] = merged.astype(jnp.bfloat16)
        merged_copy(head, group, side).start()
        terms[head, place] = split.astype(jnp.bfloat16)

    twin = plane + 1 - 2 * lax.rem(plane, 2)
    below = (1 - upper) * (planes // 2)
    soon = ((plane, members - 1), (twin, members), (below, members))
    late = below + 1
    def finish(heads_here, lot, sides, arrives):
        if arrives:
            for head in heads_here:
                for group, count in lot:
                    log_some(head, count, group).wait_recv()
        ready = [
            [(head, group, side, factors(head, group, side)) for head in heads_here for side in sides]
            for group, _ in lot
        ]
        for (group, count), held in zip(lot, ready):
            if arrives:
                for head in heads_here:
                    back_some(head, count, group).wait_recv()
            for head, group, side, values in held:
                merge(head, group, side, *values)

    late_lot = ((late, members),)
    every = range(local_heads)

    @pl.when(me < 2)
    def _():
        finish((0,), soon + late_lot, (0, 1), True)
        for head in range(1, local_heads):
            for one in soon + late_lot:
                finish((head,), (one,), (0, 1), True)

    @pl.when((upper == 0) & odd & (me >= 2))
    def _():
        for head in every:
            finish((head,), soon + late_lot, (0, 1), True)

    @pl.when((upper == 1) & odd)
    def _():
        for head in every:
            finish((head,), soon, (0, 1), True)
            finish((head,), late_lot, (0, 1), True)

    @pl.when(guests)
    def _():
        for head in every:
            finish((head,), soon, (1,), True)
        near_join()
        finish(every, soon, (0,), False)
        finish(every, late_lot, (0, 1), True)

    lane = lax.broadcasted_iota(jnp.int32, (rows, HEAD_DIM), 1)
    split = terms[0]
    for head in range(1, local_heads):
        split = split + terms[head]
    totals = jnp.dot(to_tokens, split, preferred_element_type=jnp.float32)
    summed = jnp.zeros((rows, HEAD_DIM), jnp.float32)
    for head in range(local_heads):
        total = jnp.sum(
            jnp.where((lane >= 3 * head) & (lane < 3 * head + 3), totals, 0.0), axis=-1, keepdims=True
        )
        summed = jnp.where(lane == head, total, summed)
    totals_ref[...] = summed
    wo_load.wait()
    partial_ref[...] = jnp.dot(
        moved(to_tokens, jnp.concatenate([merged_own[head] for head in range(local_heads)], axis=1)), wo[pl.ds(pl.multiple_of(tp * width, width), width), :],
        preferred_element_type=jnp.float32,
    )

    far_whole(first_send, first_held, first_sem).wait_send()
    for piece in range(2):
        far_whole(second_send.at[piece], second_held.at[piece], second_sem.at[piece]).wait_send()
    sent_logs = log_send.at[:, pl.ds(0, n - 1)]
    pltpu.make_async_copy(sent_logs, sent_logs, log_ssem).wait()
    sent_back = back_send.at[:, pl.ds(0, rows - chunk)]
    pltpu.make_async_copy(sent_back, sent_back, back_ssem).wait()

    @pl.when(crosses)
    def _():
        via_mid.wait_send()

    @pl.when(sends_two)
    def _():
        key_two.wait_send()

    @pl.when(sends_two & stays)
    def _():
        value_two.wait_send()

    @pl.when(sends_one)
    def _():
        key_one.wait_send()

    @pl.when(hosts)
    def _():
        guest_tell.wait_send()
        guest_tell_log.wait_send()

    @pl.when(guests)
    def _():
        guest_ask.wait_send()

    @pl.when(even)
    def _():
        near_key.wait_send()
        near_value.wait_send()

    @pl.when(direct)
    def _():
        value_one.wait_send()

    @pl.when(forwards & even)
    def _():
        onward_even.wait_send()

    @pl.when(forwards & odd)
    def _():
        onward_odd.wait_send()

    @pl.when(relays)
    def _():
        relay_key.wait_send()
        relay_value.wait_send()

    pltpu.make_async_copy(merged_held, merged_held, merged_sem.at[1]).wait()
    peer_ref[...] = moved(to_tokens, jnp.concatenate([merged_held[head] for head in range(local_heads)], axis=1))
    pltpu.make_async_copy(merged_own, merged_own, merged_sem.at[0]).wait()


def mix(partial_ref, peer_ref, totals_ref, wo_ref, mixed_ref, log_ref):
    width = peer_ref.shape[1]
    at = pl.ds(pl.multiple_of((1 - lax.axis_index("tp")) * width, width), width)
    product = jnp.dot(peer_ref[...], wo_ref[at], preferred_element_type=jnp.float32)
    mixed_ref[...] = (partial_ref[...] + product).astype(jnp.bfloat16)
    log_ref[...] = jnp.transpose(totals_ref[...])[: log_ref.shape[0]]


def fused(n, tokens, query_weight, key_weight, value_weight, out_weight):
    rows, depth = tokens.shape
    columns = query_weight.shape[1]
    out_columns = out_weight.shape[1]
    local_heads = columns // (3 * HEAD_DIM)
    width = local_heads * HEAD_DIM
    planes = MIDDLE_DILATION
    dma = pltpu.SemaphoreType.DMA
    half = jnp.bfloat16
    full = jnp.float32
    whole = pl.BlockSpec(memory_space=pltpu.VMEM)
    anywhere = pl.BlockSpec(memory_space=pl.ANY)
    partial, peer, totals = pl.pallas_call(
        functools.partial(kernel, n, local_heads),
        out_shape=(
            jax.ShapeDtypeStruct((rows, out_columns), full),
            jax.ShapeDtypeStruct((rows, width), half),
            jax.ShapeDtypeStruct((rows, HEAD_DIM), full),
        ),
        in_specs=[anywhere] * 5,
        out_specs=(whole, whole, whole),
        scratch_shapes=[
            pltpu.VMEM((rows, depth), half),
            pltpu.VMEM((rows, depth), half),
            pltpu.VMEM((rows, 2 * width), full),
            pltpu.VMEM((depth, 3 * columns), half),
            pltpu.VMEM(out_weight.shape, half),
            pltpu.VMEM((rows, 2 * width), half),
            pltpu.VMEM((rows, 2 * width), half),
            pltpu.VMEM((local_heads, rows, HEAD_DIM), half),
            pltpu.VMEM((local_heads, rows, HEAD_DIM), half),
            pltpu.VMEM((local_heads, rows, HEAD_DIM), half),
            pltpu.VMEM((local_heads, rows, HEAD_DIM), half),
            pltpu.VMEM((local_heads, n, 1, HEAD_DIM), full),
            pltpu.VMEM((local_heads, n, 1, HEAD_DIM), full),
            pltpu.VMEM((rows, rows), half),
            pltpu.VMEM((rows, width), half),
            pltpu.VMEM((2, rows, width), half),
            pltpu.VMEM((2, 2, rows, width), half),
            pltpu.VMEM((rows, width), half),
            pltpu.VMEM((rows, width), half),
            pltpu.VMEM((rows // 2, width), half),
            pltpu.VMEM((2, rows, width), half),
            pltpu.VMEM((2, NEAR_WINDOW, width), half),
            pltpu.VMEM((rows // 2, width), half),
            pltpu.VMEM((rows // 2, width), half),
            pltpu.VMEM((1, width), full),
            pltpu.VMEM((rows // 2, width), half),
            pltpu.VMEM((1, width), full),
            pltpu.VMEM((2 * local_heads, n, 2, rows // (2 * n), 1), full),
            pltpu.VMEM((local_heads, rows, HEAD_DIM), half),
            pltpu.VMEM((local_heads, rows, HEAD_DIM), half),
            pltpu.VMEM((local_heads, rows, HEAD_DIM), half),
            pltpu.VMEM((local_heads, n, 2, rows // (2 * n), HEAD_DIM), full),
            dma((9,)), dma((2,)), dma((2, 2)),
            dma(()), dma((local_heads, planes)), dma(()), dma((local_heads, planes)),
            dma((7,)), dma((2, 2)), dma(()), dma((2,)), dma((2,)), dma((2,)),
            dma((2,)),
        ],
        compiler_params=pltpu.CompilerParams(
            collective_id=0, has_side_effects=True, vmem_limit_bytes=53000 * 1024
        ),
    )(tokens, query_weight, key_weight, value_weight, out_weight)
    return pl.pallas_call(
        mix,
        out_shape=(
            jax.ShapeDtypeStruct((rows, out_columns), half),
            jax.ShapeDtypeStruct((local_heads, rows), full),
        ),
        in_specs=[whole] * 4,
        out_specs=(whole, whole),
        compiler_params=pltpu.CompilerParams(vmem_limit_bytes=16000 * 1024),
    )(partial, peer, totals, out_weight)


def solution(mesh):
    n, n_tp = mesh.shape["sp"], mesh.shape["tp"]
    if n == FAR_DILATION and n_tp == 2:
        body = functools.partial(fused, n)
    else:
        body = local
    return jax.shard_map(
        body,
        mesh=mesh,
        in_specs=(P("sp", None), P(None, "tp"), P(None, "tp"), P(None, "tp"), P(None, "tp")),
        out_specs=(P("sp", "tp"), P("tp", "sp")),
        check_vma=False,
    )
```

```python
import functools
import jax
import jax.numpy as jnp
from jax import lax
from jax.experimental import pallas as pl
from jax.experimental.pallas import tpu as pltpu
from jax.sharding import PartitionSpec as P

HEADS = 4
HEAD_DIM = 128
NEAR_WINDOW = 128
MIDDLE_WINDOW = 512
MIDDLE_DILATION = 4
FAR_WINDOW = 2048
FAR_DILATION = 16


def from_behind(block, axis, distance):
    devices = range(lax.axis_size(axis))
    route = [(i - distance, i) for i in devices if i - distance in devices]
    return lax.ppermute(block, axis, route)


def window_table():
    return ((NEAR_WINDOW, 1), (MIDDLE_WINDOW, MIDDLE_DILATION), (FAR_WINDOW, FAR_DILATION))


def tail_counts(row_count, distance, held_rows):
    counts = []
    for entry, available in zip(window_table(), held_rows):
        counts.append(max(0, min(available, entry[0] - (distance - 1) * row_count)))
    return counts


def pack_tails(sources, counts):
    selected = [
        source[:, source.shape[1] - amount :]
        for source, amount in zip(sources, counts)
        if amount > 0
    ]
    return jnp.concatenate(selected, axis=1)


def unpack_rows(packed, counts):
    result = []
    cursor = 0
    for amount in counts:
        result.append(packed[:, cursor : cursor + amount])
        cursor = cursor + amount
    return result


def attend_group(group_queries, buffer, window, dilation, first_key, slopes_here):
    row_count = group_queries.shape[0]
    head_count = group_queries.shape[1]
    head_size = group_queries.shape[2]
    query_split = group_queries.reshape(row_count // dilation, dilation, head_count, head_size)
    key_split = buffer[0].reshape(-1, dilation, head_count, head_size)
    value_split = buffer[1].reshape(-1, dilation, head_count, head_size)
    scores = jnp.einsum(
        "mrhe,nrhe->rhmn", query_split, key_split, preferred_element_type=jnp.float32
    ) * head_size ** (-0.5)
    grid_shape = (row_count // dilation, key_split.shape[0])
    query_slot = lax.broadcasted_iota(jnp.int32, grid_shape, 0)
    key_slot = lax.broadcasted_iota(jnp.int32, grid_shape, 1)
    spacing = query_slot + window // dilation - key_slot
    residue = lax.broadcasted_iota(jnp.int32, (dilation, 1, 1), 0)
    key_place = first_key + residue + dilation * key_slot[None]
    valid = (spacing[None] >= 0) & (spacing[None] <= window // dilation) & (key_place >= 0)
    scores = (
        scores
        - slopes_here[None, :, None, None] * (dilation * spacing).astype(jnp.float32)[None, None]
    )
    masked = jnp.where(valid[:, None], scores, -jnp.inf)
    highest = jnp.max(masked, axis=-1, keepdims=True)
    log_sum = highest + jnp.log(jnp.sum(jnp.exp(masked - highest), axis=-1, keepdims=True))
    probs = jnp.exp(masked - log_sum).astype(jnp.bfloat16)
    attended = jnp.einsum("rhmn,nrhe->mrhe", probs, value_split, preferred_element_type=jnp.float32)
    attended = attended.reshape(row_count, head_count, head_size)
    log_rows = jnp.transpose(log_sum[..., 0], (1, 2, 0)).reshape(head_count, row_count)
    return (attended, log_rows)


def local(tokens, query_weight, key_weight, value_weight, out_weight):
    rows_here = tokens.shape[0]
    local_heads = query_weight.shape[1] // (3 * HEAD_DIM)

    def project(weight_matrix):
        product = jnp.dot(tokens, weight_matrix, preferred_element_type=jnp.float32)
        return product.astype(jnp.bfloat16).reshape(rows_here, local_heads, 3, HEAD_DIM)

    queries = project(query_weight)
    keys_all = project(key_weight)
    values_all = project(value_weight)
    table = window_table()
    own = [jnp.stack((keys_all[:, :, index], values_all[:, :, index])) for index in range(3)]
    held = list(own)
    span_now = 1
    while span_now * rows_here < FAR_WINDOW + rows_here:
        counts = tail_counts(rows_here, span_now, [item.shape[1] for item in held])
        packed = pack_tails(held, counts)
        arrived = from_behind(packed, "sp", span_now)
        pieces_in = unpack_rows(arrived, counts)
        for index in range(3):
            if counts[index] > 0:
                joined = jnp.concatenate((pieces_in[index], held[index]), axis=1)
                held[index] = joined
        span_now = span_now * 2
    priors = [held[index][:, : table[index][0]] for index in range(3)]
    position_start = lax.axis_index("sp") * rows_here
    head_ids = (
        lax.axis_index("tp") * local_heads + jnp.arange(local_heads, dtype=jnp.int32)
    ).astype(jnp.float32)
    outputs = []
    logs = []
    for index, (window, dilation) in enumerate(table):
        buffer = jnp.concatenate((priors[index], own[index]), axis=1)
        slopes_here = 2.0 ** (3.0 - 8.0 * (head_ids + 1.0) / HEADS) / window
        attended, log_rows = attend_group(
            queries[:, :, index], buffer, window, dilation, position_start - window, slopes_here
        )
        outputs.append(attended)
        logs.append(log_rows)
    stacked_logs = jnp.stack(logs)
    highest = jnp.max(stacked_logs, axis=0)
    total_log = highest + jnp.log(jnp.sum(jnp.exp(stacked_logs - highest), axis=0))
    mixing = jnp.exp(stacked_logs - total_log)
    merged = outputs[0] * jnp.transpose(mixing[0])[:, :, None]
    merged = merged + outputs[1] * jnp.transpose(mixing[1])[:, :, None]
    merged = merged + outputs[2] * jnp.transpose(mixing[2])[:, :, None]
    merged = merged.astype(jnp.bfloat16).reshape(rows_here, local_heads * HEAD_DIM)
    mixed = jnp.dot(
        lax.all_gather(merged, "tp", axis=1, tiled=True),
        out_weight,
        preferred_element_type=jnp.float32,
    ).astype(jnp.bfloat16)
    return (mixed, total_log)


MESH = pl.DeviceIdType.MESH
MASKED = -1e30


def scores_of(query, key):
    return lax.dot_general(
        query, key, (((1,), (1,)), ((), ())), preferred_element_type=jnp.float32
    ) * HEAD_DIM ** (-0.5)


def weigh(scores, slope, distance, valid):
    scores = jnp.where(valid, scores - slope * distance, MASKED)
    highest = jnp.max(scores, axis=-1, keepdims=True)
    weights = jnp.exp(scores - highest)
    return highest, weights, jnp.sum(weights, axis=-1, keepdims=True)


def apply(weights, value):
    return jnp.dot(weights.astype(jnp.bfloat16), value, preferred_element_type=jnp.float32)


def split_by(value, size):
    shift = size.bit_length() - 1
    return value >> shift, value & (size - 1)


def grid(row_count, key_count):
    row = lax.broadcasted_iota(jnp.int32, (row_count, 1), 0)
    column = lax.broadcasted_iota(jnp.int32, (row_count, key_count), 1)
    return row, column


def one_hot(rows, token_of_row):
    row, column = grid(rows, rows)
    return jnp.where(column == token_of_row(row), 1.0, 0.0).astype(jnp.bfloat16)


def kernel(
    n, local_heads,
    tok_hbm, wq_hbm, wk_hbm, wv_hbm, wo_hbm,
    partial_ref, peer_ref, totals_ref,
    tok, scattered, product, weight, wo, first_send, first_held, second_send, second_held, back_send, back_held, log_send, log_held, probs,
    mid_query, mid_own, mid_held, via_held, near_query, near_low, near_own, near_held, guest_query, guest_out, guest_log, guest_back, guest_back_log,
    stats, terms, merged_own, merged_held, near_sum,
    load_sem, first_sem, second_sem, back_ssem, back_rsem, log_ssem, log_rsem,
    mid_ssem, mid_rsem, via_rsem, near_ssem, near_rsem, guest_sem, merged_sem,
):
    me = lax.axis_index("sp")
    tp = lax.axis_index("tp")
    rows = tok.shape[0]
    width = local_heads * HEAD_DIM
    chunk = rows // n
    classes = MIDDLE_DILATION
    members = n // classes
    stretch = rows // classes
    part_rows = chunk // 2
    low_rows = rows // 2
    peer = 1 - tp
    sources = (wq_hbm, wk_hbm, wv_hbm)

    depth = tok.shape[1]
    halves = (pl.ds(0, depth // 2), pl.ds(depth // 2, depth // 2))
    tok_loads = [
        pltpu.make_async_copy(tok_hbm.at[:, part], tok.at[:, part], load_sem.at[side])
        for side, part in enumerate(halves)
    ]
    wo_load = pltpu.make_async_copy(wo_hbm, wo, load_sem.at[4])
    loads = []
    far_order = [(2, part, head) for head in range(local_heads) for part in range(3)]
    order = far_order[: 2 * local_heads]
    order += [(1, part, head) for part in (1, 2) for head in range(local_heads)]
    order += far_order[2 * local_heads :]
    for group, part in ((0, 0), (0, 1), (0, 2), (1, 0)):
        order += [(group, part, head) for head in range(local_heads)]
    first = 2 * local_heads
    early = 4 * local_heads
    for place, (group, part, head) in enumerate(order):
        source = sources[part].at[:, pl.ds((head * 3 + group) * HEAD_DIM, HEAD_DIM)]
        target = weight.at[:, pl.ds(place * HEAD_DIM, HEAD_DIM)]
        if place < first:
            loads.append([
                pltpu.make_async_copy(source.at[side], target.at[side], load_sem.at[2 + index])
                for index, side in enumerate(halves)
            ])
        else:
            loads.append(pltpu.make_async_copy(source, target, load_sem.at[4 + place // first]))
    for copy in tok_loads:
        copy.start()
    for side in range(2):
        for copy in loads[:first]:
            copy[side].start()

    barrier = pltpu.get_barrier_semaphore()

    def greet(k, carry):
        pl.semaphore_signal(barrier, inc=1, device_id=(lax.rem(me + k, n), tp), device_id_type=MESH)
        return carry

    lax.fori_loop(1, n, greet, 0)
    pl.semaphore_signal(barrier, inc=1, device_id=(me, peer), device_id_type=MESH)
    for copy in loads[first:early]:
        copy.start()

    @pl.when(me < 2)
    def _():
        mid_held[0] = jnp.zeros((2, rows, width), jnp.bfloat16)

    @pl.when(me < 1)
    def _():
        mid_held[1] = jnp.zeros((2, rows, width), jnp.bfloat16)

    def project(source, first, last):
        part = weight.at[:, pl.ds(first * width, (last - first) * width)]
        pltpu.make_async_copy(part, part, load_sem.at[4 + first // 2]).wait()
        return jnp.dot(
            source[...], weight[:, first * width : last * width], preferred_element_type=jnp.float32
        ).astype(jnp.bfloat16)

    def at_rows(index):
        return pl.ds(pl.multiple_of(index * chunk, chunk), chunk)

    def scatter_token(row):
        group, index = split_by(row, chunk)
        high, low = split_by(group, members)
        return index * n + low * classes + high

    def gather_row(token):
        index, residue = split_by(token, n)
        high, low = split_by(residue, classes)
        side, inner = split_by(index, part_rows)
        return side * low_rows + (low * members + high) * part_rows + inner

    def low_row(row):
        group, inner = split_by(row, part_rows)
        return group * chunk + inner

    def class_token(row):
        group, index = split_by(row, stretch)
        return index * classes + group

    to_scattered = one_hot(rows, scatter_token)
    to_tokens = one_hot(rows, gather_row)
    to_classes = one_hot(rows, class_token)

    def moved(matrix, block):
        return jnp.dot(matrix, block, preferred_element_type=jnp.float32).astype(jnp.bfloat16)

    def each(action):
        for k in range(1, n):
            action(k)

    upper = me // (n // 2)

    def target_of(k):
        rising = k - 1 + jnp.where(k - 1 >= me, 1, 0)
        falling = n - k - jnp.where(n - k <= me, 1, 0)
        return jnp.where(upper == 1, rising, falling)


    def far_copy(source, target, sem, k):
        to = target_of(k)
        return pltpu.make_async_remote_copy(
            src_ref=source.at[at_rows(to)],
            dst_ref=target.at[at_rows(me)],
            send_sem=sem.at[0],
            recv_sem=sem.at[1],
            device_id=(to, tp),
            device_id_type=MESH,
        )

    def far_whole(source, target, sem):
        others = pl.ds(0, rows - chunk)
        return pltpu.make_async_remote_copy(
            src_ref=source.at[others],
            dst_ref=target.at[others],
            send_sem=sem.at[0],
            recv_sem=sem.at[1],
            device_id=(lax.rem(me + 1, n), tp),
            device_id_type=MESH,
        )

    plane = me // members
    planes = n // members

    def back_copy(head, k):
        to = target_of(k)
        return pltpu.make_async_remote_copy(
            src_ref=back_send.at[head, at_rows(to)],
            dst_ref=back_held.at[head, at_rows(me)],
            send_sem=back_ssem,
            recv_sem=back_rsem.at[head, plane],
            device_id=(to, tp),
            device_id_type=MESH,
        )

    def back_some(head, count, group):
        some = pl.ds(0, count * chunk)
        return pltpu.make_async_remote_copy(
            src_ref=back_send.at[head, some],
            dst_ref=back_held.at[head, some],
            send_sem=back_ssem,
            recv_sem=back_rsem.at[head, group],
            device_id=(lax.rem(me + 1, n), tp),
            device_id_type=MESH,
        )

    def log_copy(head, k):
        to = target_of(k)
        return pltpu.make_async_remote_copy(
            src_ref=log_send.at[head, to],
            dst_ref=log_held.at[head, me],
            send_sem=log_ssem,
            recv_sem=log_rsem.at[head, plane],
            device_id=(to, tp),
            device_id_type=MESH,
        )

    def log_some(head, count, group):
        some = pl.ds(0, count)
        return pltpu.make_async_remote_copy(
            src_ref=log_send.at[head, some],
            dst_ref=log_held.at[head, some],
            send_sem=log_ssem,
            recv_sem=log_rsem.at[head, group],
            device_id=(lax.rem(me + 1, n), tp),
            device_id_type=MESH,
        )

    for copy, part in zip(tok_loads, halves):
        copy.wait()
        scattered[:, part] = moved(to_scattered, tok[:, part])
    for side, part in enumerate(halves):
        piece = weight.at[part, pl.ds(0, 2 * width)]
        pltpu.make_async_copy(piece, piece, load_sem.at[2 + side]).wait()
        term = jnp.dot(scattered[:, part], weight[part, : 2 * width], preferred_element_type=jnp.float32)
        if side == 0:
            product[...] = term
        else:
            first_send[...] = (product[...] + term).astype(jnp.bfloat16)
    for copy in loads[early:]:
        copy.start()
    pl.semaphore_wait(barrier, n)
    each(lambda k: far_copy(first_send, first_held, first_sem, k).start())
    first_held[at_rows(me), :] = first_send[at_rows(me), :]

    def mid_copy(slot, hop, source, part, sem):
        return pltpu.make_async_remote_copy(
            src_ref=source,
            dst_ref=mid_held.at[slot, part],
            send_sem=mid_ssem.at[min(2 * sem + part, 6)],
            recv_sem=mid_rsem.at[slot, part],
            device_id=(lax.rem(me + hop + n, n), tp),
            device_id_type=MESH,
        )

    def near_copy(hop, source, part, sem):
        return pltpu.make_async_remote_copy(
            src_ref=source,
            dst_ref=near_held.at[part],
            send_sem=near_ssem.at[sem],
            recv_sem=near_rsem.at[part],
            device_id=(lax.rem(me + hop, n), tp),
            device_id_type=MESH,
        )

    def via_copy(source, target):
        return pltpu.make_async_remote_copy(
            src_ref=source,
            dst_ref=target,
            send_sem=mid_ssem.at[1],
            recv_sem=via_rsem,
            device_id=(lax.rem(me + -2 + n, n), tp),
            device_id_type=MESH,
        )

    near_tail = pl.ds(rows - NEAR_WINDOW, NEAR_WINDOW)
    key_two = mid_copy(0, 2, mid_own.at[0], 0, 0)
    key_one = mid_copy(1, 1, mid_own.at[0], 0, 1)
    value_two = mid_copy(0, 2, mid_own.at[1], 1, 0)
    value_one = mid_copy(1, 1, mid_own.at[1], 1, 1)
    near_key = near_copy(1, near_own.at[0, near_tail], 0, 0)
    near_value = near_copy(1, near_own.at[1, near_tail], 1, 1)
    via_mid = via_copy(mid_own.at[1], via_held)
    onward_even = mid_copy(0, 4, via_held, 1, 3)
    onward_odd = mid_copy(1, 3, via_held, 1, 3)
    key_pass = mid_copy(0, 1, mid_held.at[1, 0], 0, 0)
    relay_key = mid_copy(0, 1, mid_held.at[1, 0], 0, 2)
    relay_value = mid_copy(0, 1, mid_held.at[1, 1], 1, 2)

    def guest_copy(hop, source, target, ssem, rsem):
        return pltpu.make_async_remote_copy(
            src_ref=source,
            dst_ref=target,
            send_sem=ssem,
            recv_sem=rsem,
            device_id=(lax.rem(me + hop + n, n), tp),
            device_id_type=MESH,
        )

    guest_ask = guest_copy(-1, near_low, guest_query, guest_sem.at[0], guest_sem.at[1])
    guest_tell = guest_copy(1, guest_out, guest_back, near_ssem.at[0], near_rsem.at[0])
    guest_tell_log = guest_copy(1, guest_log, guest_back_log, near_ssem.at[1], near_rsem.at[1])

    even = lax.rem(me, 2) == 0
    odd = jnp.logical_not(even)
    sends_one = me + 1 < n
    sends_two = even & (me + 2 < n)
    relays = even & (me >= 1)
    above = me + 4 - lax.rem(me, 4) < n
    crosses = (lax.rem(me, 4) >= 2) & above
    stays = jnp.logical_not(crosses)
    forwards = (lax.rem(me, 4) < 2) & above
    hosts = odd & sends_one
    guests = even & (me >= 1)
    direct = sends_one & jnp.logical_not(crosses & odd)

    pair = moved(to_classes, project(tok, 2, 4))
    mid_own[0] = pair[:, :width]
    mid_own[1] = pair[:, width:]

    @pl.when(crosses)
    def _():
        via_mid.start()

    pair = project(scattered, 4, 6)
    for head in range(local_heads):
        second_send[head] = pair[:, head * HEAD_DIM : (head + 1) * HEAD_DIM]
    near_query[...] = pair[:, width:]
    near_low[...] = moved(one_hot(rows, low_row)[:low_rows], pair[:, width:])
    for piece in range(2):
        each(lambda k: far_copy(
            second_send.at[piece], second_held.at[piece], second_sem.at[piece], k
        ).start())
    second_held[:, at_rows(me), :] = second_send[:, at_rows(me), :]
    wo_load.start()

    @pl.when(guests)
    def _():
        guest_ask.start()

    @pl.when(direct)
    def _():
        value_one.start()
        key_one.start()

    @pl.when(crosses & odd)
    def _():
        key_one.start()

    pair = project(tok, 6, 8)
    near_own[0] = pair[:, :width]
    near_own[1] = pair[:, width:]

    @pl.when(even)
    def _():
        near_key.start()
        near_value.start()

    mid_query[...] = project(scattered, 8, 9)

    def slope_of(head, window):
        number = tp * local_heads + head
        slope = jnp.float32(0.0)
        for index in range(HEADS):
            value = 2.0 ** (3.0 - 8.0 * (index + 1.0) / HEADS) / window
            slope = jnp.where(number == index, jnp.float32(value), slope)
        return slope

    row, column = grid(rows, rows)
    apart = scatter_token(row) - column
    valid = (apart >= 0) & (apart <= NEAR_WINDOW)
    distance = apart.astype(jnp.float32)
    heads = [pl.ds(head * HEAD_DIM, HEAD_DIM) for head in range(local_heads)]

    def join(parts, side):
        held = [
            (
                stats[2 * head, :, side].reshape(-1, 1), stats[2 * head + 1, :, side].reshape(-1, 1),
                near_sum[head, :, side].reshape(-1, HEAD_DIM),
            )
            for head in range(local_heads)
        ]
        joined = []
        for (high, total, part), (held_high, held_total, held_part) in zip(parts, held):
            highest = jnp.maximum(held_high, high)
            held_share, share = jnp.exp(held_high - highest), jnp.exp(high - highest)
            joined.append((
                highest, held_total * held_share + total * share, held_part * held_share + part * share
            ))
        keep(joined, side)

    def keep(parts, side):
        shape = (n, -1, part_rows) if isinstance(side, slice) else (n, part_rows)
        for head, (high, total, part) in enumerate(parts):
            stats[2 * head, :, side] = high.reshape(*shape, 1)
            stats[2 * head + 1, :, side] = total.reshape(*shape, 1)
            near_sum[head, :, side] = part.reshape(*shape, HEAD_DIM)

    both = slice(0, 2)

    def partial_of(query, key_value, slopes, distance, valid):
        weighed = [
            weigh(scores_of(query[:, at], key_value[0, :, at]), slope, distance, valid)
            for at, slope in zip(heads, slopes)
        ]
        return [
            (high, total, apply(weights, key_value[1, :, at]))
            for at, (high, weights, total) in zip(heads, weighed)
        ]

    near_slopes = [slope_of(head, NEAR_WINDOW) for head in range(local_heads)]
    keep(partial_of(near_query, near_own, near_slopes, distance, valid), both)

    def class_slot(row):
        group, index = split_by(row, chunk)
        return index * members + split_by(group, members)[1]

    def own_rows(part, group, at):
        return mid_own[part, pl.ds(group * stretch, stretch), at]

    def held_rows(part, group, at):
        of_class = pl.ds(group * stretch, stretch)
        return jnp.concatenate((mid_held[0, part, of_class, at], mid_held[1, part, of_class, at]), axis=0)

    def middle_of(rows_of, apart, valid):
        distance = (apart * classes).astype(jnp.float32)
        weighed = []
        for head, at in enumerate(heads):
            scores = jnp.concatenate([
                scores_of(mid_query[group * stretch : (group + 1) * stretch, at], rows_of(0, group, at))
                for group in range(classes)
            ], axis=0)
            weighed.append(weigh(scores, slope_of(head, MIDDLE_WINDOW), distance, valid))
        return [
            (high, total, jnp.concatenate([
                apply(weights[group * stretch : (group + 1) * stretch], rows_of(1, group, at))
                for group in range(classes)
            ], axis=0))
            for at, (high, weights, total) in zip(heads, weighed)
        ]

    row, column = grid(rows, stretch)
    apart = class_slot(row) - column
    join(middle_of(own_rows, apart, apart >= 0), both)


    def near_rest():
        near_key.wait_recv()
        near_value.wait_recv()
        row, column = grid(low_rows, NEAR_WINDOW)
        apart = scatter_token(low_row(row)) + NEAR_WINDOW - column
        valid = (apart >= 0) & (apart <= NEAR_WINDOW)
        distance = apart.astype(jnp.float32)
        join(partial_of(near_low, near_held, near_slopes, distance, valid), 0)

    def near_join():
        guest_tell.wait_recv()
        guest_tell_log.wait_recv()
        row, column = grid(low_rows, HEAD_DIM)
        parts = []
        for at in heads:
            log = jnp.sum(
                jnp.where(row == column, jnp.broadcast_to(guest_back_log[:, at], (low_rows, HEAD_DIM)), 0.0),
                axis=-1, keepdims=True,
            )
            parts.append((log, jnp.ones_like(log), guest_back[:, at].astype(jnp.float32)))
        join(parts, 0)

    def near_host():
        guest_ask.wait_recv()
        row, column = grid(low_rows, NEAR_WINDOW)
        apart = scatter_token(low_row(row)) + NEAR_WINDOW - column
        valid = (apart >= 0) & (apart <= NEAR_WINDOW)
        distance = apart.astype(jnp.float32)
        weighed = [
            weigh(scores_of(guest_query[:, at], near_own[0, near_tail, at]), slope, distance, valid)
            for at, slope in zip(heads, near_slopes)
        ]
        row, column = grid(low_rows, HEAD_DIM)
        for at, (high, weights, total) in zip(heads, weighed):
            guest_out[:, at] = apply(weights * (1.0 / total), near_own[1, near_tail, at]).astype(jnp.bfloat16)
            guest_log[:, at] = jnp.sum(
                jnp.where(row == column, high + jnp.log(total), 0.0), axis=0, keepdims=True
            )
        guest_tell_log.start()
        guest_tell.start()

    @pl.when(odd)
    def _():
        near_rest()

    @pl.when(sends_two & stays)
    def _():
        value_two.start()
        key_two.start()

    @pl.when(crosses & odd)
    def _():
        key_one.wait_recv()
        key_pass.start()

    @pl.when(forwards)
    def _():
        via_mid.wait_recv()

    @pl.when(forwards & even)
    def _():
        onward_even.start()

    @pl.when(forwards & odd)
    def _():
        onward_odd.start()

    far_whole(first_send, first_held, first_sem).wait_recv()

    reach = FAR_WINDOW // FAR_DILATION
    lane = lax.broadcasted_iota(jnp.int32, (rows, HEAD_DIM), 1)
    slot = lax.broadcasted_iota(jnp.int32, (rows, HEAD_DIM), 0) & (chunk - 1)
    of_slot = lane == slot

    blocks = ((0, reach), (reach, rows))

    def far_part(head, part, first_row, last_row):
        place = head * 3 + part
        if place < 2 * local_heads:
            return first_held[first_row:last_row, place * HEAD_DIM : (place + 1) * HEAD_DIM]
        return second_held[place - 2 * local_heads, first_row:last_row]

    def second_arrives(piece):
        far_whole(second_send.at[piece], second_held.at[piece], second_sem.at[piece]).wait_recv()

    for head in range(local_heads):
        if head == local_heads - 1:
            second_arrives(0)
        parts = []
        for first_row, last_row in blocks:
            row, column = grid(last_row - first_row, last_row)
            apart = row + first_row - column
            high, weights, total = weigh(
                scores_of(far_part(head, 0, first_row, last_row), far_part(head, 1, 0, last_row)),
                slope_of(head, FAR_WINDOW), (apart * FAR_DILATION).astype(jnp.float32),
                (apart >= 0) & (apart <= reach),
            )
            parts.append((high + jnp.log(total), weights * (1.0 / total)))
        logs = jnp.concatenate([log for log, _ in parts], axis=0)
        log_send[head] = jnp.sum(
            jnp.where(of_slot, logs, 0.0).reshape(n, chunk, HEAD_DIM), axis=1, keepdims=True
        )
        for (first_row, last_row), (_, shares) in zip(blocks, parts):
            probs[first_row:last_row, :last_row] = shares.astype(jnp.bfloat16)
        each(lambda k: log_copy(head, k).start())
        log_held[head, me] = log_send[head, me]
        if head == local_heads - 1:
            second_arrives(1)
        for first_row, last_row in blocks:
            back_send[head, first_row:last_row] = jnp.dot(
                probs[first_row:last_row, :last_row], far_part(head, 2, 0, last_row),
                preferred_element_type=jnp.float32,
            ).astype(jnp.bfloat16)
        each(lambda k: back_copy(head, k).start())
        back_held[head, at_rows(me), :] = back_send[head, at_rows(me), :]

    @pl.when(hosts)
    def _():
        near_host()

    @pl.when(me >= 1)
    def _():
        value_one.wait_recv()

    @pl.when(relays)
    def _():
        relay_value.start()

    @pl.when((me >= 1) & jnp.logical_not(crosses & odd))
    def _():
        key_one.wait_recv()

    @pl.when(relays)
    def _():
        relay_key.start()

    @pl.when(me >= 2)
    def _():
        key_two.wait_recv()
        value_two.wait_recv()

    reach_slots = MIDDLE_WINDOW // classes
    row, column = grid(rows, reach_slots)
    apart = class_slot(row) + reach_slots - column
    valid = (apart >= 0) & (apart <= reach_slots) & (column + me * stretch >= reach_slots)
    join(middle_of(held_rows, apart, valid), both)

    block = members * part_rows

    def merged_copy(head, group, side):
        place = pl.ds(pl.multiple_of(side * low_rows + group * block, block), block)
        return pltpu.make_async_remote_copy(
            src_ref=merged_own.at[head, place],
            dst_ref=merged_held.at[head, place],
            send_sem=merged_sem.at[0],
            recv_sem=merged_sem.at[1],
            device_id=(me, peer),
            device_id_type=MESH,
        )

    lane = lax.broadcasted_iota(jnp.int32, (block, HEAD_DIM), 1)
    slot = lax.broadcasted_iota(jnp.int32, (block, HEAD_DIM), 0) & (part_rows - 1)

    def factors(head, group, side):
        some = pl.ds(group * members, members)
        spread = jnp.broadcast_to(
            log_held[head, some], (members, part_rows, HEAD_DIM)
        ).reshape(block, HEAD_DIM)
        far_log = jnp.sum(jnp.where(lane == slot + side * part_rows, spread, 0.0), axis=-1, keepdims=True)
        pair_log = stats[2 * head, some, side].reshape(block, 1)
        pair_sum = stats[2 * head + 1, some, side].reshape(block, 1)
        highest = jnp.maximum(pair_log, far_log)
        pair_part, far_share = jnp.exp(pair_log - highest), jnp.exp(far_log - highest)
        mass = pair_sum * pair_part + far_share
        inverse = 1.0 / mass
        pair_term = near_sum[head, some, side].reshape(block, HEAD_DIM) * (pair_part * inverse)
        rest = highest + jnp.log(mass)
        split = jnp.zeros((block, HEAD_DIM), jnp.float32)
        for term in range(3):
            piece = rest.astype(jnp.bfloat16).astype(jnp.float32)
            split = jnp.where(lane == 3 * head + term, piece, split)
            rest = rest - piece
        return pair_term, far_share * inverse, split

    def merge(head, group, side, pair_term, share, split):
        source = pl.ds(pl.multiple_of(group * members * chunk, members * chunk), members * chunk)
        place = pl.ds(pl.multiple_of(side * low_rows + group * block, block), block)
        far = back_held[head, source].astype(jnp.float32).reshape(members, 2, part_rows, HEAD_DIM)
        merged = pair_term + far[:, side].reshape(block, HEAD_DIM) * share
        merged_own[head, place] = merged.astype(jnp.bfloat16)
        merged_copy(head, group, side).start()
        terms[head, place] = split.astype(jnp.bfloat16)

    twin = plane + 1 - 2 * lax.rem(plane, 2)
    below = (1 - upper) * (planes // 2)
    soon = ((plane, members - 1), (twin, members), (below, members))
    late = below + 1
    def finish(heads_here, lot, sides, arrives):
        if arrives:
            for head in heads_here:
                for group, count in lot:
                    log_some(head, count, group).wait_recv()
        ready = [
            [(head, group, side, factors(head, group, side)) for head in heads_here for side in sides]
            for group, _ in lot
        ]
        for (group, count), held in zip(lot, ready):
            if arrives:
                for head in heads_here:
                    back_some(head, count, group).wait_recv()
            for head, group, side, values in held:
                merge(head, group, side, *values)

    late_lot = ((late, members),)
    every = range(local_heads)

    @pl.when(me < 2)
    def _():
        for head in every:
            for one in soon + late_lot:
                finish((head,), (one,), (0, 1), True)

    @pl.when((upper == 0) & odd & (me >= 2))
    def _():
        for head in every:
            finish((head,), soon + late_lot, (0, 1), True)

    @pl.when((upper == 1) & odd)
    def _():
        for head in every:
            finish((head,), soon, (0, 1), True)
            finish((head,), late_lot, (0, 1), True)

    @pl.when(guests)
    def _():
        finish(every, soon, (1,), True)
        near_join()
        finish(every, soon, (0,), False)
        finish(every, late_lot, (0, 1), True)

    lane = lax.broadcasted_iota(jnp.int32, (rows, HEAD_DIM), 1)
    split = terms[0]
    for head in range(1, local_heads):
        split = split + terms[head]
    totals = jnp.dot(to_tokens, split, preferred_element_type=jnp.float32)
    summed = jnp.zeros((rows, HEAD_DIM), jnp.float32)
    for head in range(local_heads):
        total = jnp.sum(
            jnp.where((lane >= 3 * head) & (lane < 3 * head + 3), totals, 0.0), axis=-1, keepdims=True
        )
        summed = jnp.where(lane == head, total, summed)
    totals_ref[...] = summed
    wo_load.wait()
    partial_ref[...] = jnp.dot(
        moved(to_tokens, jnp.concatenate([merged_own[head] for head in range(local_heads)], axis=1)), wo[pl.ds(pl.multiple_of(tp * width, width), width), :],
        preferred_element_type=jnp.float32,
    )

    far_whole(first_send, first_held, first_sem).wait_send()
    for piece in range(2):
        far_whole(second_send.at[piece], second_held.at[piece], second_sem.at[piece]).wait_send()
    sent_logs = log_send.at[:, pl.ds(0, n - 1)]
    pltpu.make_async_copy(sent_logs, sent_logs, log_ssem).wait()
    sent_back = back_send.at[:, pl.ds(0, rows - chunk)]
    pltpu.make_async_copy(sent_back, sent_back, back_ssem).wait()

    @pl.when(crosses)
    def _():
        via_mid.wait_send()

    @pl.when(crosses & odd)
    def _():
        key_pass.wait_send()

    @pl.when(sends_two & stays)
    def _():
        key_two.wait_send()

    @pl.when(sends_two & stays)
    def _():
        value_two.wait_send()

    @pl.when(sends_one)
    def _():
        key_one.wait_send()

    @pl.when(hosts)
    def _():
        guest_tell.wait_send()
        guest_tell_log.wait_send()

    @pl.when(guests)
    def _():
        guest_ask.wait_send()

    @pl.when(even)
    def _():
        near_key.wait_send()
        near_value.wait_send()

    @pl.when(direct)
    def _():
        value_one.wait_send()

    @pl.when(forwards & even)
    def _():
        onward_even.wait_send()

    @pl.when(forwards & odd)
    def _():
        onward_odd.wait_send()

    @pl.when(relays)
    def _():
        relay_key.wait_send()
        relay_value.wait_send()

    pltpu.make_async_copy(merged_held, merged_held, merged_sem.at[1]).wait()
    peer_ref[...] = moved(to_tokens, jnp.concatenate([merged_held[head] for head in range(local_heads)], axis=1))
    pltpu.make_async_copy(merged_own, merged_own, merged_sem.at[0]).wait()


def mix(partial_ref, peer_ref, totals_ref, wo_ref, mixed_ref, log_ref):
    width = peer_ref.shape[1]
    at = pl.ds(pl.multiple_of((1 - lax.axis_index("tp")) * width, width), width)
    product = jnp.dot(peer_ref[...], wo_ref[at], preferred_element_type=jnp.float32)
    mixed_ref[...] = (partial_ref[...] + product).astype(jnp.bfloat16)
    log_ref[...] = jnp.transpose(totals_ref[...])[: log_ref.shape[0]]


def fused(n, tokens, query_weight, key_weight, value_weight, out_weight):
    rows, depth = tokens.shape
    columns = query_weight.shape[1]
    out_columns = out_weight.shape[1]
    local_heads = columns // (3 * HEAD_DIM)
    width = local_heads * HEAD_DIM
    planes = MIDDLE_DILATION
    dma = pltpu.SemaphoreType.DMA
    half = jnp.bfloat16
    full = jnp.float32
    whole = pl.BlockSpec(memory_space=pltpu.VMEM)
    anywhere = pl.BlockSpec(memory_space=pl.ANY)
    partial, peer, totals = pl.pallas_call(
        functools.partial(kernel, n, local_heads),
        out_shape=(
            jax.ShapeDtypeStruct((rows, out_columns), full),
            jax.ShapeDtypeStruct((rows, width), half),
            jax.ShapeDtypeStruct((rows, HEAD_DIM), full),
        ),
        in_specs=[anywhere] * 5,
        out_specs=(whole, whole, whole),
        scratch_shapes=[
            pltpu.VMEM((rows, depth), half),
            pltpu.VMEM((rows, depth), half),
            pltpu.VMEM((rows, 2 * width), full),
            pltpu.VMEM((depth, 3 * columns), half),
            pltpu.VMEM(out_weight.shape, half),
            pltpu.VMEM((rows, 2 * width), half),
            pltpu.VMEM((rows, 2 * width), half),
            pltpu.VMEM((local_heads, rows, HEAD_DIM), half),
            pltpu.VMEM((local_heads, rows, HEAD_DIM), half),
            pltpu.VMEM((local_heads, rows, HEAD_DIM), half),
            pltpu.VMEM((local_heads, rows, HEAD_DIM), half),
            pltpu.VMEM((local_heads, n, 1, HEAD_DIM), full),
            pltpu.VMEM((local_heads, n, 1, HEAD_DIM), full),
            pltpu.VMEM((rows, rows), half),
            pltpu.VMEM((rows, width), half),
            pltpu.VMEM((2, rows, width), half),
            pltpu.VMEM((2, 2, rows, width), half),
            pltpu.VMEM((rows, width), half),
            pltpu.VMEM((rows, width), half),
            pltpu.VMEM((rows // 2, width), half),
            pltpu.VMEM((2, rows, width), half),
            pltpu.VMEM((2, NEAR_WINDOW, width), half),
            pltpu.VMEM((rows // 2, width), half),
            pltpu.VMEM((rows // 2, width), half),
            pltpu.VMEM((1, width), full),
            pltpu.VMEM((rows // 2, width), half),
            pltpu.VMEM((1, width), full),
            pltpu.VMEM((2 * local_heads, n, 2, rows // (2 * n), 1), full),
            pltpu.VMEM((local_heads, rows, HEAD_DIM), half),
            pltpu.VMEM((local_heads, rows, HEAD_DIM), half),
            pltpu.VMEM((local_heads, rows, HEAD_DIM), half),
            pltpu.VMEM((local_heads, n, 2, rows // (2 * n), HEAD_DIM), full),
            dma((9,)), dma((2,)), dma((2, 2)),
            dma(()), dma((local_heads, planes)), dma(()), dma((local_heads, planes)),
            dma((7,)), dma((2, 2)), dma(()), dma((2,)), dma((2,)), dma((2,)),
            dma((2,)),
        ],
        compiler_params=pltpu.CompilerParams(
            collective_id=0, has_side_effects=True, vmem_limit_bytes=53000 * 1024
        ),
    )(tokens, query_weight, key_weight, value_weight, out_weight)
    return pl.pallas_call(
        mix,
        out_shape=(
            jax.ShapeDtypeStruct((rows, out_columns), half),
            jax.ShapeDtypeStruct((local_heads, rows), full),
        ),
        in_specs=[whole] * 4,
        out_specs=(whole, whole),
        compiler_params=pltpu.CompilerParams(vmem_limit_bytes=16000 * 1024),
    )(partial, peer, totals, out_weight)


def solution(mesh):
    n, n_tp = mesh.shape["sp"], mesh.shape["tp"]
    if n == FAR_DILATION and n_tp == 2:
        body = functools.partial(fused, n)
    else:
        body = local
    return jax.shard_map(
        body,
        mesh=mesh,
        in_specs=(P("sp", None), P(None, "tp"), P(None, "tp"), P(None, "tp"), P(None, "tp")),
        out_specs=(P("sp", "tp"), P("tp", "sp")),
        check_vma=False,
    )
```

```python
import functools
import jax
import jax.numpy as jnp
from jax import lax
from jax.experimental import pallas as pl
from jax.experimental.pallas import tpu as pltpu
from jax.sharding import PartitionSpec as P

HEADS = 4
HEAD_DIM = 128
NEAR_WINDOW = 128
MIDDLE_WINDOW = 512
MIDDLE_DILATION = 4
FAR_WINDOW = 2048
FAR_DILATION = 16


def from_behind(block, axis, distance):
    devices = range(lax.axis_size(axis))
    route = [(i - distance, i) for i in devices if i - distance in devices]
    return lax.ppermute(block, axis, route)


def window_table():
    return ((NEAR_WINDOW, 1), (MIDDLE_WINDOW, MIDDLE_DILATION), (FAR_WINDOW, FAR_DILATION))


def tail_counts(row_count, distance, held_rows):
    counts = []
    for entry, available in zip(window_table(), held_rows):
        counts.append(max(0, min(available, entry[0] - (distance - 1) * row_count)))
    return counts


def pack_tails(sources, counts):
    selected = [
        source[:, source.shape[1] - amount :]
        for source, amount in zip(sources, counts)
        if amount > 0
    ]
    return jnp.concatenate(selected, axis=1)


def unpack_rows(packed, counts):
    result = []
    cursor = 0
    for amount in counts:
        result.append(packed[:, cursor : cursor + amount])
        cursor = cursor + amount
    return result


def attend_group(group_queries, buffer, window, dilation, first_key, slopes_here):
    row_count = group_queries.shape[0]
    head_count = group_queries.shape[1]
    head_size = group_queries.shape[2]
    query_split = group_queries.reshape(row_count // dilation, dilation, head_count, head_size)
    key_split = buffer[0].reshape(-1, dilation, head_count, head_size)
    value_split = buffer[1].reshape(-1, dilation, head_count, head_size)
    scores = jnp.einsum(
        "mrhe,nrhe->rhmn", query_split, key_split, preferred_element_type=jnp.float32
    ) * head_size ** (-0.5)
    grid_shape = (row_count // dilation, key_split.shape[0])
    query_slot = lax.broadcasted_iota(jnp.int32, grid_shape, 0)
    key_slot = lax.broadcasted_iota(jnp.int32, grid_shape, 1)
    spacing = query_slot + window // dilation - key_slot
    residue = lax.broadcasted_iota(jnp.int32, (dilation, 1, 1), 0)
    key_place = first_key + residue + dilation * key_slot[None]
    valid = (spacing[None] >= 0) & (spacing[None] <= window // dilation) & (key_place >= 0)
    scores = (
        scores
        - slopes_here[None, :, None, None] * (dilation * spacing).astype(jnp.float32)[None, None]
    )
    masked = jnp.where(valid[:, None], scores, -jnp.inf)
    highest = jnp.max(masked, axis=-1, keepdims=True)
    log_sum = highest + jnp.log(jnp.sum(jnp.exp(masked - highest), axis=-1, keepdims=True))
    probs = jnp.exp(masked - log_sum).astype(jnp.bfloat16)
    attended = jnp.einsum("rhmn,nrhe->mrhe", probs, value_split, preferred_element_type=jnp.float32)
    attended = attended.reshape(row_count, head_count, head_size)
    log_rows = jnp.transpose(log_sum[..., 0], (1, 2, 0)).reshape(head_count, row_count)
    return (attended, log_rows)


def local(tokens, query_weight, key_weight, value_weight, out_weight):
    rows_here = tokens.shape[0]
    local_heads = query_weight.shape[1] // (3 * HEAD_DIM)

    def project(weight_matrix):
        product = jnp.dot(tokens, weight_matrix, preferred_element_type=jnp.float32)
        return product.astype(jnp.bfloat16).reshape(rows_here, local_heads, 3, HEAD_DIM)

    queries = project(query_weight)
    keys_all = project(key_weight)
    values_all = project(value_weight)
    table = window_table()
    own = [jnp.stack((keys_all[:, :, index], values_all[:, :, index])) for index in range(3)]
    held = list(own)
    span_now = 1
    while span_now * rows_here < FAR_WINDOW + rows_here:
        counts = tail_counts(rows_here, span_now, [item.shape[1] for item in held])
        packed = pack_tails(held, counts)
        arrived = from_behind(packed, "sp", span_now)
        pieces_in = unpack_rows(arrived, counts)
        for index in range(3):
            if counts[index] > 0:
                joined = jnp.concatenate((pieces_in[index], held[index]), axis=1)
                held[index] = joined
        span_now = span_now * 2
    priors = [held[index][:, : table[index][0]] for index in range(3)]
    position_start = lax.axis_index("sp") * rows_here
    head_ids = (
        lax.axis_index("tp") * local_heads + jnp.arange(local_heads, dtype=jnp.int32)
    ).astype(jnp.float32)
    outputs = []
    logs = []
    for index, (window, dilation) in enumerate(table):
        buffer = jnp.concatenate((priors[index], own[index]), axis=1)
        slopes_here = 2.0 ** (3.0 - 8.0 * (head_ids + 1.0) / HEADS) / window
        attended, log_rows = attend_group(
            queries[:, :, index], buffer, window, dilation, position_start - window, slopes_here
        )
        outputs.append(attended)
        logs.append(log_rows)
    stacked_logs = jnp.stack(logs)
    highest = jnp.max(stacked_logs, axis=0)
    total_log = highest + jnp.log(jnp.sum(jnp.exp(stacked_logs - highest), axis=0))
    mixing = jnp.exp(stacked_logs - total_log)
    merged = outputs[0] * jnp.transpose(mixing[0])[:, :, None]
    merged = merged + outputs[1] * jnp.transpose(mixing[1])[:, :, None]
    merged = merged + outputs[2] * jnp.transpose(mixing[2])[:, :, None]
    merged = merged.astype(jnp.bfloat16).reshape(rows_here, local_heads * HEAD_DIM)
    mixed = jnp.dot(
        lax.all_gather(merged, "tp", axis=1, tiled=True),
        out_weight,
        preferred_element_type=jnp.float32,
    ).astype(jnp.bfloat16)
    return (mixed, total_log)


MESH = pl.DeviceIdType.MESH
MASKED = -1e30


def scores_of(query, key):
    return lax.dot_general(
        query, key, (((1,), (1,)), ((), ())), preferred_element_type=jnp.float32
    ) * HEAD_DIM ** (-0.5)


def weigh(scores, slope, distance, valid):
    scores = jnp.where(valid, scores - slope * distance, MASKED)
    highest = jnp.max(scores, axis=-1, keepdims=True)
    weights = jnp.exp(scores - highest)
    return highest, weights, jnp.sum(weights, axis=-1, keepdims=True)


def apply(weights, value):
    return jnp.dot(weights.astype(jnp.bfloat16), value, preferred_element_type=jnp.float32)


def split_by(value, size):
    shift = size.bit_length() - 1
    return value >> shift, value & (size - 1)


def grid(row_count, key_count):
    row = lax.broadcasted_iota(jnp.int32, (row_count, 1), 0)
    column = lax.broadcasted_iota(jnp.int32, (row_count, key_count), 1)
    return row, column


def one_hot(rows, token_of_row):
    row, column = grid(rows, rows)
    return jnp.where(column == token_of_row(row), 1.0, 0.0).astype(jnp.bfloat16)


def kernel(
    n, local_heads,
    tok_hbm, wq_hbm, wk_hbm, wv_hbm, wo_hbm,
    partial_ref, peer_ref, totals_ref,
    tok, scattered, product, weight, wo, first_send, first_held, second_send, second_held, back_send, back_held, log_send, log_held, probs,
    mid_query, mid_own, mid_held, via_held, near_query, near_low, near_own, near_held, guest_query, guest_out, guest_log, guest_back, guest_back_log,
    stats, terms, merged_own, merged_held, near_sum,
    load_sem, first_sem, second_sem, back_ssem, back_rsem, log_ssem, log_rsem,
    mid_ssem, mid_rsem, via_rsem, near_ssem, near_rsem, guest_sem, merged_sem,
):
    me = lax.axis_index("sp")
    tp = lax.axis_index("tp")
    rows = tok.shape[0]
    width = local_heads * HEAD_DIM
    chunk = rows // n
    classes = MIDDLE_DILATION
    members = n // classes
    stretch = rows // classes
    part_rows = chunk // 2
    low_rows = rows // 2
    peer = 1 - tp
    sources = (wq_hbm, wk_hbm, wv_hbm)

    depth = tok.shape[1]
    halves = (pl.ds(0, depth // 2), pl.ds(depth // 2, depth // 2))
    tok_loads = [
        pltpu.make_async_copy(tok_hbm.at[:, part], tok.at[:, part], load_sem.at[side])
        for side, part in enumerate(halves)
    ]
    wo_load = pltpu.make_async_copy(wo_hbm, wo, load_sem.at[4])
    loads = []
    far_order = [(2, part, head) for head in range(local_heads) for part in range(3)]
    order = far_order[: 2 * local_heads]
    order += [(1, part, head) for part in (1, 2) for head in range(local_heads)]
    order += far_order[2 * local_heads :]
    for group, part in ((0, 0), (0, 1), (0, 2), (1, 0)):
        order += [(group, part, head) for head in range(local_heads)]
    first = 2 * local_heads
    early = 4 * local_heads
    for place, (group, part, head) in enumerate(order):
        source = sources[part].at[:, pl.ds((head * 3 + group) * HEAD_DIM, HEAD_DIM)]
        target = weight.at[:, pl.ds(place * HEAD_DIM, HEAD_DIM)]
        if place < first:
            loads.append([
                pltpu.make_async_copy(source.at[side], target.at[side], load_sem.at[2 + index])
                for index, side in enumerate(halves)
            ])
        else:
            loads.append(pltpu.make_async_copy(source, target, load_sem.at[4 + place // first]))
    for copy in tok_loads:
        copy.start()
    for side in range(2):
        for copy in loads[:first]:
            copy[side].start()

    barrier = pltpu.get_barrier_semaphore()

    upper = me // (n // 2)

    def target_of(k):
        rising = k - 1 + jnp.where(k - 1 >= me, 1, 0)
        falling = n - k - jnp.where(n - k <= me, 1, 0)
        return jnp.where(upper == 1, rising, falling)


    for k in range(1, n):
        pl.semaphore_signal(barrier, inc=1, device_id=(target_of(k), tp), device_id_type=MESH)
    pl.semaphore_signal(barrier, inc=1, device_id=(me, peer), device_id_type=MESH)
    for copy in loads[first:early]:
        copy.start()

    @pl.when(me < 2)
    def _():
        mid_held[0] = jnp.zeros((2, rows, width), jnp.bfloat16)

    @pl.when(me < 1)
    def _():
        mid_held[1] = jnp.zeros((2, rows, width), jnp.bfloat16)

    def project(source, first, last):
        part = weight.at[:, pl.ds(first * width, (last - first) * width)]
        pltpu.make_async_copy(part, part, load_sem.at[4 + first // 2]).wait()
        return jnp.dot(
            source[...], weight[:, first * width : last * width], preferred_element_type=jnp.float32
        ).astype(jnp.bfloat16)

    def at_rows(index):
        return pl.ds(pl.multiple_of(index * chunk, chunk), chunk)

    def scatter_token(row):
        group, index = split_by(row, chunk)
        high, low = split_by(group, members)
        return index * n + low * classes + high

    def gather_row(token):
        index, residue = split_by(token, n)
        high, low = split_by(residue, classes)
        side, inner = split_by(index, part_rows)
        return side * low_rows + (low * members + high) * part_rows + inner

    def low_row(row):
        group, inner = split_by(row, part_rows)
        return group * chunk + inner

    def class_token(row):
        group, index = split_by(row, stretch)
        return index * classes + group

    to_scattered = one_hot(rows, scatter_token)
    to_tokens = one_hot(rows, gather_row)
    to_classes = one_hot(rows, class_token)

    def moved(matrix, block):
        return jnp.dot(matrix, block, preferred_element_type=jnp.float32).astype(jnp.bfloat16)

    def each(action):
        for k in range(1, n):
            action(k)

    def far_copy(source, target, sem, k):
        to = target_of(k)
        return pltpu.make_async_remote_copy(
            src_ref=source.at[at_rows(to)],
            dst_ref=target.at[at_rows(me)],
            send_sem=sem.at[0],
            recv_sem=sem.at[1],
            device_id=(to, tp),
            device_id_type=MESH,
        )

    def far_whole(source, target, sem):
        others = pl.ds(0, rows - chunk)
        return pltpu.make_async_remote_copy(
            src_ref=source.at[others],
            dst_ref=target.at[others],
            send_sem=sem.at[0],
            recv_sem=sem.at[1],
            device_id=(lax.rem(me + 1, n), tp),
            device_id_type=MESH,
        )

    plane = me // members
    planes = n // members

    def back_copy(head, k):
        to = target_of(k)
        return pltpu.make_async_remote_copy(
            src_ref=back_send.at[head, at_rows(to)],
            dst_ref=back_held.at[head, at_rows(me)],
            send_sem=back_ssem,
            recv_sem=back_rsem.at[head, plane],
            device_id=(to, tp),
            device_id_type=MESH,
        )

    def back_some(head, count, group):
        some = pl.ds(0, count * chunk)
        return pltpu.make_async_remote_copy(
            src_ref=back_send.at[head, some],
            dst_ref=back_held.at[head, some],
            send_sem=back_ssem,
            recv_sem=back_rsem.at[head, group],
            device_id=(lax.rem(me + 1, n), tp),
            device_id_type=MESH,
        )

    def log_copy(head, k):
        to = target_of(k)
        return pltpu.make_async_remote_copy(
            src_ref=log_send.at[head, to],
            dst_ref=log_held.at[head, me],
            send_sem=log_ssem,
            recv_sem=log_rsem.at[head, plane],
            device_id=(to, tp),
            device_id_type=MESH,
        )

    def log_some(head, count, group):
        some = pl.ds(0, count)
        return pltpu.make_async_remote_copy(
            src_ref=log_send.at[head, some],
            dst_ref=log_held.at[head, some],
            send_sem=log_ssem,
            recv_sem=log_rsem.at[head, group],
            device_id=(lax.rem(me + 1, n), tp),
            device_id_type=MESH,
        )

    for copy, part in zip(tok_loads, halves):
        copy.wait()
        scattered[:, part] = moved(to_scattered, tok[:, part])
    for side, part in enumerate(halves):
        piece = weight.at[part, pl.ds(0, 2 * width)]
        pltpu.make_async_copy(piece, piece, load_sem.at[2 + side]).wait()
        term = jnp.dot(scattered[:, part], weight[part, : 2 * width], preferred_element_type=jnp.float32)
        if side == 0:
            product[...] = term
        else:
            first_send[...] = (product[...] + term).astype(jnp.bfloat16)
    for copy in loads[early:]:
        copy.start()
    pl.semaphore_wait(barrier, n)
    each(lambda k: far_copy(first_send, first_held, first_sem, k).start())
    first_held[at_rows(me), :] = first_send[at_rows(me), :]

    def mid_copy(slot, hop, source, part, sem):
        return pltpu.make_async_remote_copy(
            src_ref=source,
            dst_ref=mid_held.at[slot, part],
            send_sem=mid_ssem.at[min(2 * sem + part, 6)],
            recv_sem=mid_rsem.at[slot, part],
            device_id=(lax.rem(me + hop + n, n), tp),
            device_id_type=MESH,
        )

    def near_copy(hop, source, part, sem):
        return pltpu.make_async_remote_copy(
            src_ref=source,
            dst_ref=near_held.at[part],
            send_sem=near_ssem.at[sem],
            recv_sem=near_rsem.at[part],
            device_id=(lax.rem(me + hop, n), tp),
            device_id_type=MESH,
        )

    def via_copy(source, target):
        return pltpu.make_async_remote_copy(
            src_ref=source,
            dst_ref=target,
            send_sem=mid_ssem.at[1],
            recv_sem=via_rsem,
            device_id=(lax.rem(me + -2 + n, n), tp),
            device_id_type=MESH,
        )

    near_tail = pl.ds(rows - NEAR_WINDOW, NEAR_WINDOW)
    key_two = mid_copy(0, 2, mid_own.at[0], 0, 0)
    key_one = mid_copy(1, 1, mid_own.at[0], 0, 1)
    value_two = mid_copy(0, 2, mid_own.at[1], 1, 0)
    value_one = mid_copy(1, 1, mid_own.at[1], 1, 1)
    near_key = near_copy(1, near_own.at[0, near_tail], 0, 0)
    near_value = near_copy(1, near_own.at[1, near_tail], 1, 1)
    via_mid = via_copy(mid_own.at[1], via_held)
    onward_even = mid_copy(0, 4, via_held, 1, 3)
    onward_odd = mid_copy(1, 3, via_held, 1, 3)
    key_pass = mid_copy(0, 1, mid_held.at[1, 0], 0, 0)
    relay_key = mid_copy(0, 1, mid_held.at[1, 0], 0, 2)
    relay_value = mid_copy(0, 1, mid_held.at[1, 1], 1, 2)

    def guest_copy(hop, source, target, ssem, rsem):
        return pltpu.make_async_remote_copy(
            src_ref=source,
            dst_ref=target,
            send_sem=ssem,
            recv_sem=rsem,
            device_id=(lax.rem(me + hop + n, n), tp),
            device_id_type=MESH,
        )

    guest_ask = guest_copy(-1, near_low, guest_query, guest_sem.at[0], guest_sem.at[1])
    guest_tell = guest_copy(1, guest_out, guest_back, near_ssem.at[0], near_rsem.at[0])
    guest_tell_log = guest_copy(1, guest_log, guest_back_log, near_ssem.at[1], near_rsem.at[1])

    even = lax.rem(me, 2) == 0
    odd = jnp.logical_not(even)
    sends_one = me + 1 < n
    sends_two = even & (me + 2 < n)
    relays = even & (me >= 1)
    above = me + 4 - lax.rem(me, 4) < n
    crosses = (lax.rem(me, 4) >= 2) & above
    stays = jnp.logical_not(crosses)
    forwards = (lax.rem(me, 4) < 2) & above
    hosts = odd & sends_one
    guests = even & (me >= 1)
    direct = sends_one & jnp.logical_not(crosses & odd)

    pair = moved(to_classes, project(tok, 2, 4))
    mid_own[0] = pair[:, :width]
    mid_own[1] = pair[:, width:]

    @pl.when(crosses)
    def _():
        via_mid.start()

    pair = project(scattered, 4, 6)
    for head in range(local_heads):
        second_send[head] = pair[:, head * HEAD_DIM : (head + 1) * HEAD_DIM]
    near_query[...] = pair[:, width:]
    near_low[...] = moved(one_hot(rows, low_row)[:low_rows], pair[:, width:])

    def send_second(ks):
        for piece in range(2):
            for k in ks:
                far_copy(
                    second_send.at[piece], second_held.at[piece], second_sem.at[piece], k
                ).start()

    inner = (plane >= 1) & (plane < planes - 1)
    outward = range(1, n - members + 1)

    @pl.when(inner)
    def _():
        send_second(outward)

    send_second(range(n - members + 1, n))

    second_held[:, at_rows(me), :] = second_send[:, at_rows(me), :]
    wo_load.start()

    @pl.when(guests)
    def _():
        guest_ask.start()

    @pl.when(direct)
    def _():
        value_one.start()
        key_one.start()

    @pl.when(crosses & odd & inner)
    def _():
        key_one.start()

    pair = project(tok, 6, 8)
    near_own[0] = pair[:, :width]
    near_own[1] = pair[:, width:]

    @pl.when(even)
    def _():
        near_key.start()
        near_value.start()

    mid_query[...] = project(scattered, 8, 9)

    def slope_of(head, window):
        number = tp * local_heads + head
        slope = jnp.float32(0.0)
        for index in range(HEADS):
            value = 2.0 ** (3.0 - 8.0 * (index + 1.0) / HEADS) / window
            slope = jnp.where(number == index, jnp.float32(value), slope)
        return slope

    row, column = grid(rows, rows)
    apart = scatter_token(row) - column
    valid = (apart >= 0) & (apart <= NEAR_WINDOW)
    distance = apart.astype(jnp.float32)
    heads = [pl.ds(head * HEAD_DIM, HEAD_DIM) for head in range(local_heads)]

    def join(parts, side):
        held = [
            (
                stats[2 * head, :, side].reshape(-1, 1), stats[2 * head + 1, :, side].reshape(-1, 1),
                near_sum[head, :, side].reshape(-1, HEAD_DIM),
            )
            for head in range(local_heads)
        ]
        joined = []
        for (high, total, part), (held_high, held_total, held_part) in zip(parts, held):
            highest = jnp.maximum(held_high, high)
            held_share, share = jnp.exp(held_high - highest), jnp.exp(high - highest)
            joined.append((
                highest, held_total * held_share + total * share, held_part * held_share + part * share
            ))
        keep(joined, side)

    def keep(parts, side):
        shape = (n, -1, part_rows) if isinstance(side, slice) else (n, part_rows)
        for head, (high, total, part) in enumerate(parts):
            stats[2 * head, :, side] = high.reshape(*shape, 1)
            stats[2 * head + 1, :, side] = total.reshape(*shape, 1)
            near_sum[head, :, side] = part.reshape(*shape, HEAD_DIM)

    both = slice(0, 2)

    def partial_of(query, key_value, slopes, distance, valid):
        weighed = [
            weigh(scores_of(query[:, at], key_value[0, :, at]), slope, distance, valid)
            for at, slope in zip(heads, slopes)
        ]
        return [
            (high, total, apply(weights, key_value[1, :, at]))
            for at, (high, weights, total) in zip(heads, weighed)
        ]

    near_slopes = [slope_of(head, NEAR_WINDOW) for head in range(local_heads)]
    keep(partial_of(near_query, near_own, near_slopes, distance, valid), both)

    def class_slot(row):
        group, index = split_by(row, chunk)
        return index * members + split_by(group, members)[1]

    def own_rows(part, group, at):
        return mid_own[part, pl.ds(group * stretch, stretch), at]

    def held_rows(part, group, at):
        of_class = pl.ds(group * stretch, stretch)
        return jnp.concatenate((mid_held[0, part, of_class, at], mid_held[1, part, of_class, at]), axis=0)

    def middle_of(rows_of, apart, valid):
        distance = (apart * classes).astype(jnp.float32)
        weighed = []
        for head, at in enumerate(heads):
            scores = jnp.concatenate([
                scores_of(mid_query[group * stretch : (group + 1) * stretch, at], rows_of(0, group, at))
                for group in range(classes)
            ], axis=0)
            weighed.append(weigh(scores, slope_of(head, MIDDLE_WINDOW), distance, valid))
        return [
            (high, total, jnp.concatenate([
                apply(weights[group * stretch : (group + 1) * stretch], rows_of(1, group, at))
                for group in range(classes)
            ], axis=0))
            for at, (high, weights, total) in zip(heads, weighed)
        ]

    row, column = grid(rows, stretch)
    apart = class_slot(row) - column
    join(middle_of(own_rows, apart, apart >= 0), both)


    def near_rest():
        near_key.wait_recv()
        near_value.wait_recv()
        row, column = grid(low_rows, NEAR_WINDOW)
        apart = scatter_token(low_row(row)) + NEAR_WINDOW - column
        valid = (apart >= 0) & (apart <= NEAR_WINDOW)
        distance = apart.astype(jnp.float32)
        join(partial_of(near_low, near_held, near_slopes, distance, valid), 0)

    def near_join():
        guest_tell.wait_recv()
        guest_tell_log.wait_recv()
        row, column = grid(low_rows, HEAD_DIM)
        parts = []
        for at in heads:
            log = jnp.sum(
                jnp.where(row == column, jnp.broadcast_to(guest_back_log[:, at], (low_rows, HEAD_DIM)), 0.0),
                axis=-1, keepdims=True,
            )
            parts.append((log, jnp.ones_like(log), guest_back[:, at].astype(jnp.float32)))
        join(parts, 0)

    def near_host():
        guest_ask.wait_recv()
        row, column = grid(low_rows, NEAR_WINDOW)
        apart = scatter_token(low_row(row)) + NEAR_WINDOW - column
        valid = (apart >= 0) & (apart <= NEAR_WINDOW)
        distance = apart.astype(jnp.float32)
        weighed = [
            weigh(scores_of(guest_query[:, at], near_own[0, near_tail, at]), slope, distance, valid)
            for at, slope in zip(heads, near_slopes)
        ]
        row, column = grid(low_rows, HEAD_DIM)
        for at, (high, weights, total) in zip(heads, weighed):
            guest_out[:, at] = apply(weights * (1.0 / total), near_own[1, near_tail, at]).astype(jnp.bfloat16)
            guest_log[:, at] = jnp.sum(
                jnp.where(row == column, high + jnp.log(total), 0.0), axis=0, keepdims=True
            )
        guest_tell_log.start()
        guest_tell.start()

    @pl.when(jnp.logical_not(inner))
    def _():
        send_second(outward)

    @pl.when(crosses & odd & jnp.logical_not(inner))
    def _():
        key_one.start()

    @pl.when(odd)
    def _():
        near_rest()

    @pl.when(sends_two & stays)
    def _():
        value_two.start()
        key_two.start()

    @pl.when(crosses & odd)
    def _():
        key_one.wait_recv()
        key_pass.start()

    @pl.when(forwards)
    def _():
        via_mid.wait_recv()

    @pl.when(forwards & even)
    def _():
        onward_even.start()

    @pl.when(forwards & odd)
    def _():
        onward_odd.start()

    far_whole(first_send, first_held, first_sem).wait_recv()

    reach = FAR_WINDOW // FAR_DILATION
    lane = lax.broadcasted_iota(jnp.int32, (rows, HEAD_DIM), 1)
    slot = lax.broadcasted_iota(jnp.int32, (rows, HEAD_DIM), 0) & (chunk - 1)
    of_slot = lane == slot

    blocks = ((0, reach), (reach, rows))

    def far_part(head, part, first_row, last_row):
        place = head * 3 + part
        if place < 2 * local_heads:
            return first_held[first_row:last_row, place * HEAD_DIM : (place + 1) * HEAD_DIM]
        return second_held[place - 2 * local_heads, first_row:last_row]

    def second_arrives(piece):
        far_whole(second_send.at[piece], second_held.at[piece], second_sem.at[piece]).wait_recv()

    for head in range(local_heads):
        if head == local_heads - 1:
            second_arrives(0)
        parts = []
        for first_row, last_row in blocks:
            row, column = grid(last_row - first_row, last_row)
            apart = row + first_row - column
            high, weights, total = weigh(
                scores_of(far_part(head, 0, first_row, last_row), far_part(head, 1, 0, last_row)),
                slope_of(head, FAR_WINDOW), (apart * FAR_DILATION).astype(jnp.float32),
                (apart >= 0) & (apart <= reach),
            )
            parts.append((high + jnp.log(total), weights * (1.0 / total)))
        logs = jnp.concatenate([log for log, _ in parts], axis=0)
        log_send[head] = jnp.sum(
            jnp.where(of_slot, logs, 0.0).reshape(n, chunk, HEAD_DIM), axis=1, keepdims=True
        )
        for (first_row, last_row), (_, shares) in zip(blocks, parts):
            probs[first_row:last_row, :last_row] = shares.astype(jnp.bfloat16)
        each(lambda k: log_copy(head, k).start())
        log_held[head, me] = log_send[head, me]
        if head == local_heads - 1:
            second_arrives(1)
        for first_row, last_row in blocks:
            back_send[head, first_row:last_row] = jnp.dot(
                probs[first_row:last_row, :last_row], far_part(head, 2, 0, last_row),
                preferred_element_type=jnp.float32,
            ).astype(jnp.bfloat16)
        each(lambda k: back_copy(head, k).start())
        back_held[head, at_rows(me), :] = back_send[head, at_rows(me), :]

    @pl.when(hosts)
    def _():
        near_host()

    @pl.when(me >= 1)
    def _():
        value_one.wait_recv()

    @pl.when(relays)
    def _():
        relay_value.start()

    @pl.when((me >= 1) & jnp.logical_not(crosses & odd))
    def _():
        key_one.wait_recv()

    @pl.when(relays)
    def _():
        relay_key.start()

    @pl.when(me >= 2)
    def _():
        key_two.wait_recv()
        value_two.wait_recv()

    reach_slots = MIDDLE_WINDOW // classes
    row, column = grid(rows, reach_slots)
    apart = class_slot(row) + reach_slots - column
    valid = (apart >= 0) & (apart <= reach_slots) & (column + me * stretch >= reach_slots)
    join(middle_of(held_rows, apart, valid), both)

    block = members * part_rows

    def merged_copy(head, group, side):
        place = pl.ds(pl.multiple_of(side * low_rows + group * block, block), block)
        return pltpu.make_async_remote_copy(
            src_ref=merged_own.at[head, place],
            dst_ref=merged_held.at[head, place],
            send_sem=merged_sem.at[0],
            recv_sem=merged_sem.at[1],
            device_id=(me, peer),
            device_id_type=MESH,
        )

    lane = lax.broadcasted_iota(jnp.int32, (block, HEAD_DIM), 1)
    slot = lax.broadcasted_iota(jnp.int32, (block, HEAD_DIM), 0) & (part_rows - 1)

    def factors(head, group, side):
        some = pl.ds(group * members, members)
        spread = jnp.broadcast_to(
            log_held[head, some], (members, part_rows, HEAD_DIM)
        ).reshape(block, HEAD_DIM)
        far_log = jnp.sum(jnp.where(lane == slot + side * part_rows, spread, 0.0), axis=-1, keepdims=True)
        pair_log = stats[2 * head, some, side].reshape(block, 1)
        pair_sum = stats[2 * head + 1, some, side].reshape(block, 1)
        highest = jnp.maximum(pair_log, far_log)
        pair_part, far_share = jnp.exp(pair_log - highest), jnp.exp(far_log - highest)
        mass = pair_sum * pair_part + far_share
        inverse = 1.0 / mass
        pair_term = near_sum[head, some, side].reshape(block, HEAD_DIM) * (pair_part * inverse)
        rest = highest + jnp.log(mass)
        split = jnp.zeros((block, HEAD_DIM), jnp.float32)
        for term in range(3):
            piece = rest.astype(jnp.bfloat16).astype(jnp.float32)
            split = jnp.where(lane == 3 * head + term, piece, split)
            rest = rest - piece
        return pair_term, far_share * inverse, split

    def merge(head, group, side, pair_term, share, split):
        source = pl.ds(pl.multiple_of(group * members * chunk, members * chunk), members * chunk)
        place = pl.ds(pl.multiple_of(side * low_rows + group * block, block), block)
        far = back_held[head, source].astype(jnp.float32).reshape(members, 2, part_rows, HEAD_DIM)
        merged = pair_term + far[:, side].reshape(block, HEAD_DIM) * share
        merged_own[head, place] = merged.astype(jnp.bfloat16)
        merged_copy(head, group, side).start()
        terms[head, place] = split.astype(jnp.bfloat16)

    twin = plane + 1 - 2 * lax.rem(plane, 2)
    below = (1 - upper) * (planes // 2)
    soon = ((plane, members - 1), (twin, members), (below, members))
    late = below + 1
    def finish(heads_here, lot, sides, arrives):
        if arrives:
            for head in heads_here:
                for group, count in lot:
                    log_some(head, count, group).wait_recv()
        ready = [
            [(head, group, side, factors(head, group, side)) for head in heads_here for side in sides]
            for group, _ in lot
        ]
        for (group, count), held in zip(lot, ready):
            if arrives:
                for head in heads_here:
                    back_some(head, count, group).wait_recv()
            for head, group, side, values in held:
                merge(head, group, side, *values)

    late_lot = ((late, members),)
    every = range(local_heads)

    @pl.when(me < 2)
    def _():
        for head in every:
            for one in soon + late_lot:
                finish((head,), (one,), (0, 1), True)

    @pl.when((upper == 0) & odd & (me >= 2))
    def _():
        for head in every:
            finish((head,), soon + late_lot, (0, 1), True)

    @pl.when((upper == 1) & odd)
    def _():
        for head in every:
            finish((head,), soon, (0, 1), True)
            finish((head,), late_lot, (0, 1), True)

    @pl.when(guests)
    def _():
        finish(every, soon, (1,), True)
        near_join()
        finish(every, soon, (0,), False)
        finish(every, late_lot, (0, 1), True)

    lane = lax.broadcasted_iota(jnp.int32, (rows, HEAD_DIM), 1)
    split = terms[0]
    for head in range(1, local_heads):
        split = split + terms[head]
    totals = jnp.dot(to_tokens, split, preferred_element_type=jnp.float32)
    summed = jnp.zeros((rows, HEAD_DIM), jnp.float32)
    for head in range(local_heads):
        total = jnp.sum(
            jnp.where((lane >= 3 * head) & (lane < 3 * head + 3), totals, 0.0), axis=-1, keepdims=True
        )
        summed = jnp.where(lane == head, total, summed)
    totals_ref[...] = summed
    wo_load.wait()
    partial_ref[...] = jnp.dot(
        moved(to_tokens, jnp.concatenate([merged_own[head] for head in range(local_heads)], axis=1)), wo[pl.ds(pl.multiple_of(tp * width, width), width), :],
        preferred_element_type=jnp.float32,
    )

    far_whole(first_send, first_held, first_sem).wait_send()
    for piece in range(2):
        far_whole(second_send.at[piece], second_held.at[piece], second_sem.at[piece]).wait_send()
    sent_logs = log_send.at[:, pl.ds(0, n - 1)]
    pltpu.make_async_copy(sent_logs, sent_logs, log_ssem).wait()
    sent_back = back_send.at[:, pl.ds(0, rows - chunk)]
    pltpu.make_async_copy(sent_back, sent_back, back_ssem).wait()

    @pl.when(crosses)
    def _():
        via_mid.wait_send()

    @pl.when(crosses & odd)
    def _():
        key_pass.wait_send()

    @pl.when(sends_two & stays)
    def _():
        key_two.wait_send()

    @pl.when(sends_two & stays)
    def _():
        value_two.wait_send()

    @pl.when(sends_one)
    def _():
        key_one.wait_send()

    @pl.when(hosts)
    def _():
        guest_tell.wait_send()
        guest_tell_log.wait_send()

    @pl.when(guests)
    def _():
        guest_ask.wait_send()

    @pl.when(even)
    def _():
        near_key.wait_send()
        near_value.wait_send()

    @pl.when(direct)
    def _():
        value_one.wait_send()

    @pl.when(forwards & even)
    def _():
        onward_even.wait_send()

    @pl.when(forwards & odd)
    def _():
        onward_odd.wait_send()

    @pl.when(relays)
    def _():
        relay_key.wait_send()
        relay_value.wait_send()

    pltpu.make_async_copy(merged_held, merged_held, merged_sem.at[1]).wait()
    peer_ref[...] = moved(to_tokens, jnp.concatenate([merged_held[head] for head in range(local_heads)], axis=1))
    pltpu.make_async_copy(merged_own, merged_own, merged_sem.at[0]).wait()


def mix(partial_ref, peer_ref, totals_ref, wo_ref, mixed_ref, log_ref):
    width = peer_ref.shape[1]
    at = pl.ds(pl.multiple_of((1 - lax.axis_index("tp")) * width, width), width)
    product = jnp.dot(peer_ref[...], wo_ref[at], preferred_element_type=jnp.float32)
    mixed_ref[...] = (partial_ref[...] + product).astype(jnp.bfloat16)
    log_ref[...] = jnp.transpose(totals_ref[...])[: log_ref.shape[0]]


def fused(n, tokens, query_weight, key_weight, value_weight, out_weight):
    rows, depth = tokens.shape
    columns = query_weight.shape[1]
    out_columns = out_weight.shape[1]
    local_heads = columns // (3 * HEAD_DIM)
    width = local_heads * HEAD_DIM
    planes = MIDDLE_DILATION
    dma = pltpu.SemaphoreType.DMA
    half = jnp.bfloat16
    full = jnp.float32
    whole = pl.BlockSpec(memory_space=pltpu.VMEM)
    anywhere = pl.BlockSpec(memory_space=pl.ANY)
    partial, peer, totals = pl.pallas_call(
        functools.partial(kernel, n, local_heads),
        out_shape=(
            jax.ShapeDtypeStruct((rows, out_columns), full),
            jax.ShapeDtypeStruct((rows, width), half),
            jax.ShapeDtypeStruct((rows, HEAD_DIM), full),
        ),
        in_specs=[anywhere] * 5,
        out_specs=(whole, whole, whole),
        scratch_shapes=[
            pltpu.VMEM((rows, depth), half),
            pltpu.VMEM((rows, depth), half),
            pltpu.VMEM((rows, 2 * width), full),
            pltpu.VMEM((depth, 3 * columns), half),
            pltpu.VMEM(out_weight.shape, half),
            pltpu.VMEM((rows, 2 * width), half),
            pltpu.VMEM((rows, 2 * width), half),
            pltpu.VMEM((local_heads, rows, HEAD_DIM), half),
            pltpu.VMEM((local_heads, rows, HEAD_DIM), half),
            pltpu.VMEM((local_heads, rows, HEAD_DIM), half),
            pltpu.VMEM((local_heads, rows, HEAD_DIM), half),
            pltpu.VMEM((local_heads, n, 1, HEAD_DIM), full),
            pltpu.VMEM((local_heads, n, 1, HEAD_DIM), full),
            pltpu.VMEM((rows, rows), half),
            pltpu.VMEM((rows, width), half),
            pltpu.VMEM((2, rows, width), half),
            pltpu.VMEM((2, 2, rows, width), half),
            pltpu.VMEM((rows, width), half),
            pltpu.VMEM((rows, width), half),
            pltpu.VMEM((rows // 2, width), half),
            pltpu.VMEM((2, rows, width), half),
            pltpu.VMEM((2, NEAR_WINDOW, width), half),
            pltpu.VMEM((rows // 2, width), half),
            pltpu.VMEM((rows // 2, width), half),
            pltpu.VMEM((1, width), full),
            pltpu.VMEM((rows // 2, width), half),
            pltpu.VMEM((1, width), full),
            pltpu.VMEM((2 * local_heads, n, 2, rows // (2 * n), 1), full),
            pltpu.VMEM((local_heads, rows, HEAD_DIM), half),
            pltpu.VMEM((local_heads, rows, HEAD_DIM), half),
            pltpu.VMEM((local_heads, rows, HEAD_DIM), half),
            pltpu.VMEM((local_heads, n, 2, rows // (2 * n), HEAD_DIM), full),
            dma((9,)), dma((2,)), dma((2, 2)),
            dma(()), dma((local_heads, planes)), dma(()), dma((local_heads, planes)),
            dma((7,)), dma((2, 2)), dma(()), dma((2,)), dma((2,)), dma((2,)),
            dma((2,)),
        ],
        compiler_params=pltpu.CompilerParams(
            collective_id=0, has_side_effects=True, vmem_limit_bytes=53000 * 1024
        ),
    )(tokens, query_weight, key_weight, value_weight, out_weight)
    return pl.pallas_call(
        mix,
        out_shape=(
            jax.ShapeDtypeStruct((rows, out_columns), half),
            jax.ShapeDtypeStruct((local_heads, rows), full),
        ),
        in_specs=[whole] * 4,
        out_specs=(whole, whole),
        compiler_params=pltpu.CompilerParams(vmem_limit_bytes=16000 * 1024),
    )(partial, peer, totals, out_weight)


def solution(mesh):
    n, n_tp = mesh.shape["sp"], mesh.shape["tp"]
    if n == FAR_DILATION and n_tp == 2:
        body = functools.partial(fused, n)
    else:
        body = local
    return jax.shard_map(
        body,
        mesh=mesh,
        in_specs=(P("sp", None), P(None, "tp"), P(None, "tp"), P(None, "tp"), P(None, "tp")),
        out_specs=(P("sp", "tp"), P("tp", "sp")),
        check_vma=False,
    )
```

```python
import functools
import jax
import jax.numpy as jnp
from jax import lax
from jax.experimental import pallas as pl
from jax.experimental.pallas import tpu as pltpu
from jax.sharding import PartitionSpec as P

HEADS = 4
HEAD_DIM = 128
NEAR_WINDOW = 128
MIDDLE_WINDOW = 512
MIDDLE_DILATION = 4
FAR_WINDOW = 2048
FAR_DILATION = 16


def from_behind(block, axis, distance):
    devices = range(lax.axis_size(axis))
    route = [(i - distance, i) for i in devices if i - distance in devices]
    return lax.ppermute(block, axis, route)


def window_table():
    return ((NEAR_WINDOW, 1), (MIDDLE_WINDOW, MIDDLE_DILATION), (FAR_WINDOW, FAR_DILATION))


def tail_counts(row_count, distance, held_rows):
    counts = []
    for entry, available in zip(window_table(), held_rows):
        counts.append(max(0, min(available, entry[0] - (distance - 1) * row_count)))
    return counts


def pack_tails(sources, counts):
    selected = [
        source[:, source.shape[1] - amount :]
        for source, amount in zip(sources, counts)
        if amount > 0
    ]
    return jnp.concatenate(selected, axis=1)


def unpack_rows(packed, counts):
    result = []
    cursor = 0
    for amount in counts:
        result.append(packed[:, cursor : cursor + amount])
        cursor = cursor + amount
    return result


def attend_group(group_queries, buffer, window, dilation, first_key, slopes_here):
    row_count = group_queries.shape[0]
    head_count = group_queries.shape[1]
    head_size = group_queries.shape[2]
    query_split = group_queries.reshape(row_count // dilation, dilation, head_count, head_size)
    key_split = buffer[0].reshape(-1, dilation, head_count, head_size)
    value_split = buffer[1].reshape(-1, dilation, head_count, head_size)
    scores = jnp.einsum(
        "mrhe,nrhe->rhmn", query_split, key_split, preferred_element_type=jnp.float32
    ) * head_size ** (-0.5)
    grid_shape = (row_count // dilation, key_split.shape[0])
    query_slot = lax.broadcasted_iota(jnp.int32, grid_shape, 0)
    key_slot = lax.broadcasted_iota(jnp.int32, grid_shape, 1)
    spacing = query_slot + window // dilation - key_slot
    residue = lax.broadcasted_iota(jnp.int32, (dilation, 1, 1), 0)
    key_place = first_key + residue + dilation * key_slot[None]
    valid = (spacing[None] >= 0) & (spacing[None] <= window // dilation) & (key_place >= 0)
    scores = (
        scores
        - slopes_here[None, :, None, None] * (dilation * spacing).astype(jnp.float32)[None, None]
    )
    masked = jnp.where(valid[:, None], scores, -jnp.inf)
    highest = jnp.max(masked, axis=-1, keepdims=True)
    log_sum = highest + jnp.log(jnp.sum(jnp.exp(masked - highest), axis=-1, keepdims=True))
    probs = jnp.exp(masked - log_sum).astype(jnp.bfloat16)
    attended = jnp.einsum("rhmn,nrhe->mrhe", probs, value_split, preferred_element_type=jnp.float32)
    attended = attended.reshape(row_count, head_count, head_size)
    log_rows = jnp.transpose(log_sum[..., 0], (1, 2, 0)).reshape(head_count, row_count)
    return (attended, log_rows)


def local(tokens, query_weight, key_weight, value_weight, out_weight):
    rows_here = tokens.shape[0]
    local_heads = query_weight.shape[1] // (3 * HEAD_DIM)

    def project(weight_matrix):
        product = jnp.dot(tokens, weight_matrix, preferred_element_type=jnp.float32)
        return product.astype(jnp.bfloat16).reshape(rows_here, local_heads, 3, HEAD_DIM)

    queries = project(query_weight)
    keys_all = project(key_weight)
    values_all = project(value_weight)
    table = window_table()
    own = [jnp.stack((keys_all[:, :, index], values_all[:, :, index])) for index in range(3)]
    held = list(own)
    span_now = 1
    while span_now * rows_here < FAR_WINDOW + rows_here:
        counts = tail_counts(rows_here, span_now, [item.shape[1] for item in held])
        packed = pack_tails(held, counts)
        arrived = from_behind(packed, "sp", span_now)
        pieces_in = unpack_rows(arrived, counts)
        for index in range(3):
            if counts[index] > 0:
                joined = jnp.concatenate((pieces_in[index], held[index]), axis=1)
                held[index] = joined
        span_now = span_now * 2
    priors = [held[index][:, : table[index][0]] for index in range(3)]
    position_start = lax.axis_index("sp") * rows_here
    head_ids = (
        lax.axis_index("tp") * local_heads + jnp.arange(local_heads, dtype=jnp.int32)
    ).astype(jnp.float32)
    outputs = []
    logs = []
    for index, (window, dilation) in enumerate(table):
        buffer = jnp.concatenate((priors[index], own[index]), axis=1)
        slopes_here = 2.0 ** (3.0 - 8.0 * (head_ids + 1.0) / HEADS) / window
        attended, log_rows = attend_group(
            queries[:, :, index], buffer, window, dilation, position_start - window, slopes_here
        )
        outputs.append(attended)
        logs.append(log_rows)
    stacked_logs = jnp.stack(logs)
    highest = jnp.max(stacked_logs, axis=0)
    total_log = highest + jnp.log(jnp.sum(jnp.exp(stacked_logs - highest), axis=0))
    mixing = jnp.exp(stacked_logs - total_log)
    merged = outputs[0] * jnp.transpose(mixing[0])[:, :, None]
    merged = merged + outputs[1] * jnp.transpose(mixing[1])[:, :, None]
    merged = merged + outputs[2] * jnp.transpose(mixing[2])[:, :, None]
    merged = merged.astype(jnp.bfloat16).reshape(rows_here, local_heads * HEAD_DIM)
    mixed = jnp.dot(
        lax.all_gather(merged, "tp", axis=1, tiled=True),
        out_weight,
        preferred_element_type=jnp.float32,
    ).astype(jnp.bfloat16)
    return (mixed, total_log)


MESH = pl.DeviceIdType.MESH
MASKED = -1e30


def scores_of(query, key):
    return lax.dot_general(
        query, key, (((1,), (1,)), ((), ())), preferred_element_type=jnp.float32
    ) * HEAD_DIM ** (-0.5)


def weigh(scores, slope, distance, valid):
    scores = jnp.where(valid, scores - slope * distance, MASKED)
    highest = jnp.max(scores, axis=-1, keepdims=True)
    weights = jnp.exp(scores - highest)
    return highest, weights, jnp.sum(weights, axis=-1, keepdims=True)


def apply(weights, value):
    return jnp.dot(weights.astype(jnp.bfloat16), value, preferred_element_type=jnp.float32)


def split_by(value, size):
    shift = size.bit_length() - 1
    return value >> shift, value & (size - 1)


def grid(row_count, key_count):
    row = lax.broadcasted_iota(jnp.int32, (row_count, 1), 0)
    column = lax.broadcasted_iota(jnp.int32, (row_count, key_count), 1)
    return row, column


def one_hot(rows, token_of_row):
    row, column = grid(rows, rows)
    return jnp.where(column == token_of_row(row), 1.0, 0.0).astype(jnp.bfloat16)


def kernel(
    n, local_heads,
    tok_hbm, wq_hbm, wk_hbm, wv_hbm, wo_hbm,
    partial_ref, peer_ref, totals_ref,
    tok, scattered, product, weight, wo, first_send, first_held, second_send, second_held, back_send, back_held, log_send, log_held, probs,
    mid_query, mid_own, mid_held, via_held, near_query, near_low, near_own, near_held, guest_query, guest_out, guest_log, guest_back, guest_back_log,
    stats, terms, merged_own, merged_held, near_sum,
    load_sem, first_sem, second_sem, back_ssem, back_rsem, log_ssem, log_rsem,
    mid_ssem, mid_rsem, via_rsem, near_ssem, near_rsem, guest_sem, merged_sem,
):
    me = lax.axis_index("sp")
    tp = lax.axis_index("tp")
    rows = tok.shape[0]
    width = local_heads * HEAD_DIM
    chunk = rows // n
    classes = MIDDLE_DILATION
    members = n // classes
    stretch = rows // classes
    part_rows = chunk // 2
    low_rows = rows // 2
    peer = 1 - tp
    sources = (wq_hbm, wk_hbm, wv_hbm)

    depth = tok.shape[1]
    halves = (pl.ds(0, depth // 2), pl.ds(depth // 2, depth // 2))
    tok_loads = [
        pltpu.make_async_copy(tok_hbm.at[:, part], tok.at[:, part], load_sem.at[side])
        for side, part in enumerate(halves)
    ]
    wo_load = pltpu.make_async_copy(wo_hbm, wo, load_sem.at[4])
    loads = []
    far_order = [(2, part, head) for head in range(local_heads) for part in range(3)]
    order = far_order[: 2 * local_heads]
    order += [(1, part, head) for part in (1, 2) for head in range(local_heads)]
    order += far_order[2 * local_heads :]
    for group, part in ((0, 0), (0, 1), (0, 2), (1, 0)):
        order += [(group, part, head) for head in range(local_heads)]
    first = 2 * local_heads
    early = 4 * local_heads
    for place, (group, part, head) in enumerate(order):
        source = sources[part].at[:, pl.ds((head * 3 + group) * HEAD_DIM, HEAD_DIM)]
        target = weight.at[:, pl.ds(place * HEAD_DIM, HEAD_DIM)]
        if place < first:
            loads.append([
                pltpu.make_async_copy(source.at[side], target.at[side], load_sem.at[2 + index])
                for index, side in enumerate(halves)
            ])
        else:
            loads.append(pltpu.make_async_copy(source, target, load_sem.at[4 + place // first]))
    for copy in tok_loads:
        copy.start()
    for side in range(2):
        for copy in loads[:first]:
            copy[side].start()

    barrier = pltpu.get_barrier_semaphore()

    def greet(k, carry):
        pl.semaphore_signal(barrier, inc=1, device_id=(lax.rem(me + k, n), tp), device_id_type=MESH)
        return carry

    lax.fori_loop(1, n, greet, 0)
    pl.semaphore_signal(barrier, inc=1, device_id=(me, peer), device_id_type=MESH)
    for copy in loads[first:early]:
        copy.start()

    @pl.when(me < 2)
    def _():
        mid_held[0] = jnp.zeros((2, rows, width), jnp.bfloat16)

    @pl.when(me < 1)
    def _():
        mid_held[1] = jnp.zeros((2, rows, width), jnp.bfloat16)

    def project(source, first, last):
        part = weight.at[:, pl.ds(first * width, (last - first) * width)]
        pltpu.make_async_copy(part, part, load_sem.at[4 + first // 2]).wait()
        return jnp.dot(
            source[...], weight[:, first * width : last * width], preferred_element_type=jnp.float32
        ).astype(jnp.bfloat16)

    def at_rows(index):
        return pl.ds(pl.multiple_of(index * chunk, chunk), chunk)

    def scatter_token(row):
        group, index = split_by(row, chunk)
        high, low = split_by(group, members)
        return index * n + low * classes + high

    def gather_row(token):
        index, residue = split_by(token, n)
        high, low = split_by(residue, classes)
        side, inner = split_by(index, part_rows)
        return side * low_rows + (low * members + high) * part_rows + inner

    def low_row(row):
        group, inner = split_by(row, part_rows)
        return group * chunk + inner

    def class_token(row):
        group, index = split_by(row, stretch)
        return index * classes + group

    to_scattered = one_hot(rows, scatter_token)
    to_tokens = one_hot(rows, gather_row)
    to_classes = one_hot(rows, class_token)

    def moved(matrix, block):
        return jnp.dot(matrix, block, preferred_element_type=jnp.float32).astype(jnp.bfloat16)

    def each(action):
        for k in range(1, n):
            action(k)

    upper = me // (n // 2)

    def target_of(k):
        rising = k - 1 + jnp.where(k - 1 >= me, 1, 0)
        falling = n - k - jnp.where(n - k <= me, 1, 0)
        return jnp.where(upper == 1, rising, falling)


    def far_copy(source, target, sem, k):
        to = target_of(k)
        return pltpu.make_async_remote_copy(
            src_ref=source.at[at_rows(to)],
            dst_ref=target.at[at_rows(me)],
            send_sem=sem.at[0],
            recv_sem=sem.at[1],
            device_id=(to, tp),
            device_id_type=MESH,
        )

    def far_whole(source, target, sem):
        others = pl.ds(0, rows - chunk)
        return pltpu.make_async_remote_copy(
            src_ref=source.at[others],
            dst_ref=target.at[others],
            send_sem=sem.at[0],
            recv_sem=sem.at[1],
            device_id=(lax.rem(me + 1, n), tp),
            device_id_type=MESH,
        )

    plane = me // members
    planes = n // members

    def rising(k):
        return k - 1 + jnp.where(k - 1 >= me, 1, 0)

    def back_copy(head, k):
        to = rising(k)
        return pltpu.make_async_remote_copy(
            src_ref=back_send.at[head, at_rows(to)],
            dst_ref=back_held.at[head, at_rows(me)],
            send_sem=back_ssem,
            recv_sem=back_rsem.at[head, plane],
            device_id=(to, tp),
            device_id_type=MESH,
        )

    def back_some(head, count, group):
        some = pl.ds(0, count * chunk)
        return pltpu.make_async_remote_copy(
            src_ref=back_send.at[head, some],
            dst_ref=back_held.at[head, some],
            send_sem=back_ssem,
            recv_sem=back_rsem.at[head, group],
            device_id=(lax.rem(me + 1, n), tp),
            device_id_type=MESH,
        )

    def log_copy(head, k):
        to = rising(k)
        return pltpu.make_async_remote_copy(
            src_ref=log_send.at[head, to],
            dst_ref=log_held.at[head, me],
            send_sem=log_ssem,
            recv_sem=log_rsem.at[head, plane],
            device_id=(to, tp),
            device_id_type=MESH,
        )

    def log_some(head, count, group):
        some = pl.ds(0, count)
        return pltpu.make_async_remote_copy(
            src_ref=log_send.at[head, some],
            dst_ref=log_held.at[head, some],
            send_sem=log_ssem,
            recv_sem=log_rsem.at[head, group],
            device_id=(lax.rem(me + 1, n), tp),
            device_id_type=MESH,
        )

    for copy, part in zip(tok_loads, halves):
        copy.wait()
        scattered[:, part] = moved(to_scattered, tok[:, part])
    for side, part in enumerate(halves):
        piece = weight.at[part, pl.ds(0, 2 * width)]
        pltpu.make_async_copy(piece, piece, load_sem.at[2 + side]).wait()
        term = jnp.dot(scattered[:, part], weight[part, : 2 * width], preferred_element_type=jnp.float32)
        if side == 0:
            product[...] = term
        else:
            first_send[...] = (product[...] + term).astype(jnp.bfloat16)
    for copy in loads[early:]:
        copy.start()
    pl.semaphore_wait(barrier, n)
    each(lambda k: far_copy(first_send, first_held, first_sem, k).start())
    first_held[at_rows(me), :] = first_send[at_rows(me), :]

    def mid_copy(slot, hop, source, part, sem):
        return pltpu.make_async_remote_copy(
            src_ref=source,
            dst_ref=mid_held.at[slot, part],
            send_sem=mid_ssem.at[min(2 * sem + part, 6)],
            recv_sem=mid_rsem.at[slot, part],
            device_id=(lax.rem(me + hop + n, n), tp),
            device_id_type=MESH,
        )

    def near_copy(hop, source, part, sem):
        return pltpu.make_async_remote_copy(
            src_ref=source,
            dst_ref=near_held.at[part],
            send_sem=near_ssem.at[sem],
            recv_sem=near_rsem.at[part],
            device_id=(lax.rem(me + hop, n), tp),
            device_id_type=MESH,
        )

    def via_copy(source, target):
        return pltpu.make_async_remote_copy(
            src_ref=source,
            dst_ref=target,
            send_sem=mid_ssem.at[1],
            recv_sem=via_rsem,
            device_id=(lax.rem(me + -2 + n, n), tp),
            device_id_type=MESH,
        )

    near_tail = pl.ds(rows - NEAR_WINDOW, NEAR_WINDOW)
    key_two = mid_copy(0, 2, mid_own.at[0], 0, 0)
    key_one = mid_copy(1, 1, mid_own.at[0], 0, 1)
    value_two = mid_copy(0, 2, mid_own.at[1], 1, 0)
    value_one = mid_copy(1, 1, mid_own.at[1], 1, 1)
    near_key = near_copy(1, near_own.at[0, near_tail], 0, 0)
    near_value = near_copy(1, near_own.at[1, near_tail], 1, 1)
    via_mid = via_copy(mid_own.at[1], via_held)
    onward_even = mid_copy(0, 4, via_held, 1, 3)
    onward_odd = mid_copy(1, 3, via_held, 1, 3)
    key_pass = mid_copy(0, 1, mid_held.at[1, 0], 0, 0)
    relay_key = mid_copy(0, 1, mid_held.at[1, 0], 0, 2)
    relay_value = mid_copy(0, 1, mid_held.at[1, 1], 1, 2)

    def guest_copy(hop, source, target, ssem, rsem):
        return pltpu.make_async_remote_copy(
            src_ref=source,
            dst_ref=target,
            send_sem=ssem,
            recv_sem=rsem,
            device_id=(lax.rem(me + hop + n, n), tp),
            device_id_type=MESH,
        )

    guest_ask = guest_copy(-1, near_low, guest_query, guest_sem.at[0], guest_sem.at[1])
    guest_tell = guest_copy(1, guest_out, guest_back, near_ssem.at[0], near_rsem.at[0])
    guest_tell_log = guest_copy(1, guest_log, guest_back_log, near_ssem.at[1], near_rsem.at[1])

    even = lax.rem(me, 2) == 0
    odd = jnp.logical_not(even)
    sends_one = me + 1 < n
    sends_two = even & (me + 2 < n)
    relays = even & (me >= 1)
    above = me + 4 - lax.rem(me, 4) < n
    crosses = (lax.rem(me, 4) >= 2) & above
    stays = jnp.logical_not(crosses)
    forwards = (lax.rem(me, 4) < 2) & above
    hosts = odd & sends_one
    guests = even & (me >= 1)
    direct = sends_one & jnp.logical_not(crosses & odd)

    pair = moved(to_classes, project(tok, 2, 4))
    mid_own[0] = pair[:, :width]
    mid_own[1] = pair[:, width:]

    @pl.when(crosses)
    def _():
        via_mid.start()

    pair = project(scattered, 4, 6)
    for head in range(local_heads):
        second_send[head] = pair[:, head * HEAD_DIM : (head + 1) * HEAD_DIM]
    near_query[...] = pair[:, width:]
    near_low[...] = moved(one_hot(rows, low_row)[:low_rows], pair[:, width:])
    for piece in range(2):
        each(lambda k: far_copy(
            second_send.at[piece], second_held.at[piece], second_sem.at[piece], k
        ).start())
    second_held[:, at_rows(me), :] = second_send[:, at_rows(me), :]
    wo_load.start()

    @pl.when(guests)
    def _():
        guest_ask.start()

    @pl.when(direct)
    def _():
        value_one.start()
        key_one.start()

    @pl.when(crosses & odd)
    def _():
        key_one.start()

    pair = project(tok, 6, 8)
    near_own[0] = pair[:, :width]
    near_own[1] = pair[:, width:]

    @pl.when(even)
    def _():
        near_key.start()
        near_value.start()

    mid_query[...] = project(scattered, 8, 9)

    def slope_of(head, window):
        number = tp * local_heads + head
        slope = jnp.float32(0.0)
        for index in range(HEADS):
            value = 2.0 ** (3.0 - 8.0 * (index + 1.0) / HEADS) / window
            slope = jnp.where(number == index, jnp.float32(value), slope)
        return slope

    row, column = grid(rows, rows)
    apart = scatter_token(row) - column
    valid = (apart >= 0) & (apart <= NEAR_WINDOW)
    distance = apart.astype(jnp.float32)
    heads = [pl.ds(head * HEAD_DIM, HEAD_DIM) for head in range(local_heads)]

    def join(parts, side):
        held = [
            (
                stats[2 * head, :, side].reshape(-1, 1), stats[2 * head + 1, :, side].reshape(-1, 1),
                near_sum[head, :, side].reshape(-1, HEAD_DIM),
            )
            for head in range(local_heads)
        ]
        joined = []
        for (high, total, part), (held_high, held_total, held_part) in zip(parts, held):
            highest = jnp.maximum(held_high, high)
            held_share, share = jnp.exp(held_high - highest), jnp.exp(high - highest)
            joined.append((
                highest, held_total * held_share + total * share, held_part * held_share + part * share
            ))
        keep(joined, side)

    def keep(parts, side):
        shape = (n, -1, part_rows) if isinstance(side, slice) else (n, part_rows)
        for head, (high, total, part) in enumerate(parts):
            stats[2 * head, :, side] = high.reshape(*shape, 1)
            stats[2 * head + 1, :, side] = total.reshape(*shape, 1)
            near_sum[head, :, side] = part.reshape(*shape, HEAD_DIM)

    both = slice(0, 2)

    def partial_of(query, key_value, slopes, distance, valid):
        weighed = [
            weigh(scores_of(query[:, at], key_value[0, :, at]), slope, distance, valid)
            for at, slope in zip(heads, slopes)
        ]
        return [
            (high, total, apply(weights, key_value[1, :, at]))
            for at, (high, weights, total) in zip(heads, weighed)
        ]

    near_slopes = [slope_of(head, NEAR_WINDOW) for head in range(local_heads)]
    keep(partial_of(near_query, near_own, near_slopes, distance, valid), both)

    def class_slot(row):
        group, index = split_by(row, chunk)
        return index * members + split_by(group, members)[1]

    def own_rows(part, group, at):
        return mid_own[part, pl.ds(group * stretch, stretch), at]

    def held_rows(part, group, at):
        of_class = pl.ds(group * stretch, stretch)
        return jnp.concatenate((mid_held[0, part, of_class, at], mid_held[1, part, of_class, at]), axis=0)

    def middle_of(rows_of, apart, valid):
        distance = (apart * classes).astype(jnp.float32)
        weighed = []
        for head, at in enumerate(heads):
            scores = jnp.concatenate([
                scores_of(mid_query[group * stretch : (group + 1) * stretch, at], rows_of(0, group, at))
                for group in range(classes)
            ], axis=0)
            weighed.append(weigh(scores, slope_of(head, MIDDLE_WINDOW), distance, valid))
        return [
            (high, total, jnp.concatenate([
                apply(weights[group * stretch : (group + 1) * stretch], rows_of(1, group, at))
                for group in range(classes)
            ], axis=0))
            for at, (high, weights, total) in zip(heads, weighed)
        ]

    row, column = grid(rows, stretch)
    apart = class_slot(row) - column
    join(middle_of(own_rows, apart, apart >= 0), both)


    def near_rest():
        near_key.wait_recv()
        near_value.wait_recv()
        row, column = grid(low_rows, NEAR_WINDOW)
        apart = scatter_token(low_row(row)) + NEAR_WINDOW - column
        valid = (apart >= 0) & (apart <= NEAR_WINDOW)
        distance = apart.astype(jnp.float32)
        join(partial_of(near_low, near_held, near_slopes, distance, valid), 0)

    def near_join():
        guest_tell.wait_recv()
        guest_tell_log.wait_recv()
        row, column = grid(low_rows, HEAD_DIM)
        parts = []
        for at in heads:
            log = jnp.sum(
                jnp.where(row == column, jnp.broadcast_to(guest_back_log[:, at], (low_rows, HEAD_DIM)), 0.0),
                axis=-1, keepdims=True,
            )
            parts.append((log, jnp.ones_like(log), guest_back[:, at].astype(jnp.float32)))
        join(parts, 0)

    def near_host():
        guest_ask.wait_recv()
        row, column = grid(low_rows, NEAR_WINDOW)
        apart = scatter_token(low_row(row)) + NEAR_WINDOW - column
        valid = (apart >= 0) & (apart <= NEAR_WINDOW)
        distance = apart.astype(jnp.float32)
        weighed = [
            weigh(scores_of(guest_query[:, at], near_own[0, near_tail, at]), slope, distance, valid)
            for at, slope in zip(heads, near_slopes)
        ]
        row, column = grid(low_rows, HEAD_DIM)
        for at, (high, weights, total) in zip(heads, weighed):
            guest_out[:, at] = apply(weights * (1.0 / total), near_own[1, near_tail, at]).astype(jnp.bfloat16)
            guest_log[:, at] = jnp.sum(
                jnp.where(row == column, high + jnp.log(total), 0.0), axis=0, keepdims=True
            )
        guest_tell_log.start()
        guest_tell.start()

    @pl.when(odd)
    def _():
        near_rest()

    @pl.when(sends_two & stays)
    def _():
        value_two.start()
        key_two.start()

    @pl.when(crosses & odd)
    def _():
        key_one.wait_recv()
        key_pass.start()

    @pl.when(forwards)
    def _():
        via_mid.wait_recv()

    @pl.when(forwards & even)
    def _():
        onward_even.start()

    @pl.when(forwards & odd)
    def _():
        onward_odd.start()

    far_whole(first_send, first_held, first_sem).wait_recv()

    reach = FAR_WINDOW // FAR_DILATION
    lane = lax.broadcasted_iota(jnp.int32, (rows, HEAD_DIM), 1)
    slot = lax.broadcasted_iota(jnp.int32, (rows, HEAD_DIM), 0) & (chunk - 1)
    of_slot = lane == slot

    blocks = ((0, reach), (reach, rows))

    def far_part(head, part, first_row, last_row):
        place = head * 3 + part
        if place < 2 * local_heads:
            return first_held[first_row:last_row, place * HEAD_DIM : (place + 1) * HEAD_DIM]
        return second_held[place - 2 * local_heads, first_row:last_row]

    def second_arrives(piece):
        far_whole(second_send.at[piece], second_held.at[piece], second_sem.at[piece]).wait_recv()

    for head in range(local_heads):
        if head == local_heads - 1:
            second_arrives(0)
        parts = []
        for first_row, last_row in blocks:
            row, column = grid(last_row - first_row, last_row)
            apart = row + first_row - column
            high, weights, total = weigh(
                scores_of(far_part(head, 0, first_row, last_row), far_part(head, 1, 0, last_row)),
                slope_of(head, FAR_WINDOW), (apart * FAR_DILATION).astype(jnp.float32),
                (apart >= 0) & (apart <= reach),
            )
            parts.append((high + jnp.log(total), weights * (1.0 / total)))
        logs = jnp.concatenate([log for log, _ in parts], axis=0)
        log_send[head] = jnp.sum(
            jnp.where(of_slot, logs, 0.0).reshape(n, chunk, HEAD_DIM), axis=1, keepdims=True
        )
        for (first_row, last_row), (_, shares) in zip(blocks, parts):
            probs[first_row:last_row, :last_row] = shares.astype(jnp.bfloat16)
        each(lambda k: log_copy(head, k).start())
        log_held[head, me] = log_send[head, me]
        if head == local_heads - 1:
            second_arrives(1)
        for first_row, last_row in blocks:
            back_send[head, first_row:last_row] = jnp.dot(
                probs[first_row:last_row, :last_row], far_part(head, 2, 0, last_row),
                preferred_element_type=jnp.float32,
            ).astype(jnp.bfloat16)
        each(lambda k: back_copy(head, k).start())
        back_held[head, at_rows(me), :] = back_send[head, at_rows(me), :]

    @pl.when(hosts)
    def _():
        near_host()

    @pl.when(me >= 1)
    def _():
        value_one.wait_recv()

    @pl.when(relays)
    def _():
        relay_value.start()

    @pl.when((me >= 1) & jnp.logical_not(crosses & odd))
    def _():
        key_one.wait_recv()

    @pl.when(relays)
    def _():
        relay_key.start()

    @pl.when(me >= 2)
    def _():
        key_two.wait_recv()
        value_two.wait_recv()

    reach_slots = MIDDLE_WINDOW // classes
    row, column = grid(rows, reach_slots)
    apart = class_slot(row) + reach_slots - column
    valid = (apart >= 0) & (apart <= reach_slots) & (column + me * stretch >= reach_slots)
    join(middle_of(held_rows, apart, valid), both)

    block = members * part_rows

    def merged_copy(head, group, side):
        place = pl.ds(pl.multiple_of(side * low_rows + group * block, block), block)
        return pltpu.make_async_remote_copy(
            src_ref=merged_own.at[head, place],
            dst_ref=merged_held.at[head, place],
            send_sem=merged_sem.at[0],
            recv_sem=merged_sem.at[1],
            device_id=(me, peer),
            device_id_type=MESH,
        )

    lane = lax.broadcasted_iota(jnp.int32, (block, HEAD_DIM), 1)
    slot = lax.broadcasted_iota(jnp.int32, (block, HEAD_DIM), 0) & (part_rows - 1)

    def factors(head, group, side):
        some = pl.ds(group * members, members)
        spread = jnp.broadcast_to(
            log_held[head, some], (members, part_rows, HEAD_DIM)
        ).reshape(block, HEAD_DIM)
        far_log = jnp.sum(jnp.where(lane == slot + side * part_rows, spread, 0.0), axis=-1, keepdims=True)
        pair_log = stats[2 * head, some, side].reshape(block, 1)
        pair_sum = stats[2 * head + 1, some, side].reshape(block, 1)
        highest = jnp.maximum(pair_log, far_log)
        pair_part, far_share = jnp.exp(pair_log - highest), jnp.exp(far_log - highest)
        mass = pair_sum * pair_part + far_share
        inverse = 1.0 / mass
        pair_term = near_sum[head, some, side].reshape(block, HEAD_DIM) * (pair_part * inverse)
        rest = highest + jnp.log(mass)
        split = jnp.zeros((block, HEAD_DIM), jnp.float32)
        for term in range(3):
            piece = rest.astype(jnp.bfloat16).astype(jnp.float32)
            split = jnp.where(lane == 3 * head + term, piece, split)
            rest = rest - piece
        return pair_term, far_share * inverse, split

    def merge(head, group, side, pair_term, share, split):
        source = pl.ds(pl.multiple_of(group * members * chunk, members * chunk), members * chunk)
        place = pl.ds(pl.multiple_of(side * low_rows + group * block, block), block)
        far = back_held[head, source].astype(jnp.float32).reshape(members, 2, part_rows, HEAD_DIM)
        merged = pair_term + far[:, side].reshape(block, HEAD_DIM) * share
        merged_own[head, place] = merged.astype(jnp.bfloat16)
        merged_copy(head, group, side).start()
        terms[head, place] = split.astype(jnp.bfloat16)

    twin = plane + 1 - 2 * lax.rem(plane, 2)
    below = (1 - upper) * (planes // 2)
    soon = ((plane, members - 1), (twin, members), (below, members))
    late = below + 1
    def finish(heads_here, lot, sides, arrives):
        if arrives:
            for head in heads_here:
                for group, count in lot:
                    log_some(head, count, group).wait_recv()
        ready = [
            [(head, group, side, factors(head, group, side)) for head in heads_here for side in sides]
            for group, _ in lot
        ]
        for (group, count), held in zip(lot, ready):
            if arrives:
                for head in heads_here:
                    back_some(head, count, group).wait_recv()
            for head, group, side, values in held:
                merge(head, group, side, *values)

    late_lot = ((late, members),)
    every = range(local_heads)

    @pl.when(me < 2)
    def _():
        for head in every:
            for one in soon + late_lot:
                finish((head,), (one,), (0, 1), True)

    @pl.when((upper == 0) & odd & (me >= 2))
    def _():
        for head in every:
            finish((head,), soon + late_lot, (0, 1), True)

    @pl.when((upper == 1) & odd)
    def _():
        for head in every:
            finish((head,), soon, (0, 1), True)
            finish((head,), late_lot, (0, 1), True)

    @pl.when(guests)
    def _():
        finish(every, soon, (1,), True)
        near_join()
        finish(every, soon, (0,), False)
        finish(every, late_lot, (0, 1), True)

    lane = lax.broadcasted_iota(jnp.int32, (rows, HEAD_DIM), 1)
    split = terms[0]
    for head in range(1, local_heads):
        split = split + terms[head]
    totals = jnp.dot(to_tokens, split, preferred_element_type=jnp.float32)
    summed = jnp.zeros((rows, HEAD_DIM), jnp.float32)
    for head in range(local_heads):
        total = jnp.sum(
            jnp.where((lane >= 3 * head) & (lane < 3 * head + 3), totals, 0.0), axis=-1, keepdims=True
        )
        summed = jnp.where(lane == head, total, summed)
    totals_ref[...] = summed
    wo_load.wait()
    partial_ref[...] = jnp.dot(
        moved(to_tokens, jnp.concatenate([merged_own[head] for head in range(local_heads)], axis=1)), wo[pl.ds(pl.multiple_of(tp * width, width), width), :],
        preferred_element_type=jnp.float32,
    )

    far_whole(first_send, first_held, first_sem).wait_send()
    for piece in range(2):
        far_whole(second_send.at[piece], second_held.at[piece], second_sem.at[piece]).wait_send()
    sent_logs = log_send.at[:, pl.ds(0, n - 1)]
    pltpu.make_async_copy(sent_logs, sent_logs, log_ssem).wait()
    sent_back = back_send.at[:, pl.ds(0, rows - chunk)]
    pltpu.make_async_copy(sent_back, sent_back, back_ssem).wait()

    @pl.when(crosses)
    def _():
        via_mid.wait_send()

    @pl.when(crosses & odd)
    def _():
        key_pass.wait_send()

    @pl.when(sends_two & stays)
    def _():
        key_two.wait_send()

    @pl.when(sends_two & stays)
    def _():
        value_two.wait_send()

    @pl.when(sends_one)
    def _():
        key_one.wait_send()

    @pl.when(hosts)
    def _():
        guest_tell.wait_send()
        guest_tell_log.wait_send()

    @pl.when(guests)
    def _():
        guest_ask.wait_send()

    @pl.when(even)
    def _():
        near_key.wait_send()
        near_value.wait_send()

    @pl.when(direct)
    def _():
        value_one.wait_send()

    @pl.when(forwards & even)
    def _():
        onward_even.wait_send()

    @pl.when(forwards & odd)
    def _():
        onward_odd.wait_send()

    @pl.when(relays)
    def _():
        relay_key.wait_send()
        relay_value.wait_send()

    pltpu.make_async_copy(merged_held, merged_held, merged_sem.at[1]).wait()
    peer_ref[...] = moved(to_tokens, jnp.concatenate([merged_held[head] for head in range(local_heads)], axis=1))
    pltpu.make_async_copy(merged_own, merged_own, merged_sem.at[0]).wait()


def mix(partial_ref, peer_ref, totals_ref, wo_ref, mixed_ref, log_ref):
    width = peer_ref.shape[1]
    at = pl.ds(pl.multiple_of((1 - lax.axis_index("tp")) * width, width), width)
    product = jnp.dot(peer_ref[...], wo_ref[at], preferred_element_type=jnp.float32)
    mixed_ref[...] = (partial_ref[...] + product).astype(jnp.bfloat16)
    log_ref[...] = jnp.transpose(totals_ref[...])[: log_ref.shape[0]]


def fused(n, tokens, query_weight, key_weight, value_weight, out_weight):
    rows, depth = tokens.shape
    columns = query_weight.shape[1]
    out_columns = out_weight.shape[1]
    local_heads = columns // (3 * HEAD_DIM)
    width = local_heads * HEAD_DIM
    planes = MIDDLE_DILATION
    dma = pltpu.SemaphoreType.DMA
    half = jnp.bfloat16
    full = jnp.float32
    whole = pl.BlockSpec(memory_space=pltpu.VMEM)
    anywhere = pl.BlockSpec(memory_space=pl.ANY)
    partial, peer, totals = pl.pallas_call(
        functools.partial(kernel, n, local_heads),
        out_shape=(
            jax.ShapeDtypeStruct((rows, out_columns), full),
            jax.ShapeDtypeStruct((rows, width), half),
            jax.ShapeDtypeStruct((rows, HEAD_DIM), full),
        ),
        in_specs=[anywhere] * 5,
        out_specs=(whole, whole, whole),
        scratch_shapes=[
            pltpu.VMEM((rows, depth), half),
            pltpu.VMEM((rows, depth), half),
            pltpu.VMEM((rows, 2 * width), full),
            pltpu.VMEM((depth, 3 * columns), half),
            pltpu.VMEM(out_weight.shape, half),
            pltpu.VMEM((rows, 2 * width), half),
            pltpu.VMEM((rows, 2 * width), half),
            pltpu.VMEM((local_heads, rows, HEAD_DIM), half),
            pltpu.VMEM((local_heads, rows, HEAD_DIM), half),
            pltpu.VMEM((local_heads, rows, HEAD_DIM), half),
            pltpu.VMEM((local_heads, rows, HEAD_DIM), half),
            pltpu.VMEM((local_heads, n, 1, HEAD_DIM), full),
            pltpu.VMEM((local_heads, n, 1, HEAD_DIM), full),
            pltpu.VMEM((rows, rows), half),
            pltpu.VMEM((rows, width), half),
            pltpu.VMEM((2, rows, width), half),
            pltpu.VMEM((2, 2, rows, width), half),
            pltpu.VMEM((rows, width), half),
            pltpu.VMEM((rows, width), half),
            pltpu.VMEM((rows // 2, width), half),
            pltpu.VMEM((2, rows, width), half),
            pltpu.VMEM((2, NEAR_WINDOW, width), half),
            pltpu.VMEM((rows // 2, width), half),
            pltpu.VMEM((rows // 2, width), half),
            pltpu.VMEM((1, width), full),
            pltpu.VMEM((rows // 2, width), half),
            pltpu.VMEM((1, width), full),
            pltpu.VMEM((2 * local_heads, n, 2, rows // (2 * n), 1), full),
            pltpu.VMEM((local_heads, rows, HEAD_DIM), half),
            pltpu.VMEM((local_heads, rows, HEAD_DIM), half),
            pltpu.VMEM((local_heads, rows, HEAD_DIM), half),
            pltpu.VMEM((local_heads, n, 2, rows // (2 * n), HEAD_DIM), full),
            dma((9,)), dma((2,)), dma((2, 2)),
            dma(()), dma((local_heads, planes)), dma(()), dma((local_heads, planes)),
            dma((7,)), dma((2, 2)), dma(()), dma((2,)), dma((2,)), dma((2,)),
            dma((2,)),
        ],
        compiler_params=pltpu.CompilerParams(
            collective_id=0, has_side_effects=True, vmem_limit_bytes=53000 * 1024
        ),
    )(tokens, query_weight, key_weight, value_weight, out_weight)
    return pl.pallas_call(
        mix,
        out_shape=(
            jax.ShapeDtypeStruct((rows, out_columns), half),
            jax.ShapeDtypeStruct((local_heads, rows), full),
        ),
        in_specs=[whole] * 4,
        out_specs=(whole, whole),
        compiler_params=pltpu.CompilerParams(vmem_limit_bytes=16000 * 1024),
    )(partial, peer, totals, out_weight)


def solution(mesh):
    n, n_tp = mesh.shape["sp"], mesh.shape["tp"]
    if n == FAR_DILATION and n_tp == 2:
        body = functools.partial(fused, n)
    else:
        body = local
    return jax.shard_map(
        body,
        mesh=mesh,
        in_specs=(P("sp", None), P(None, "tp"), P(None, "tp"), P(None, "tp"), P(None, "tp")),
        out_specs=(P("sp", "tp"), P("tp", "sp")),
        check_vma=False,
    )
```
